512 devices in a mesh: sp: 32 (over z, x), dp: 16 (over y, core).
Axes of the slice: x: 4, y: 8, z: 8, core: 2. Of those that a mesh axis runs over, the one named last changes fastest.
Arguments:
- layer_activity: bfloat16 [16, 4096, 2048], P('dp', 'sp'), may hold values from -6 to 6
- writer_matrix: bfloat16 [2048, 256], P('dp'), may hold values from -0.125 to 0.125
- reader_matrix: bfloat16 [2048, 256], P('dp'), may hold values from -0.125 to 0.125
- source_unfiltered: bfloat16 [16, 4096, 2048], P('dp', 'sp'), may hold values from -6 to 6
- switch_raw_signal: bfloat16 [16, 4096, 2048], P('dp', 'sp'), may hold values from -6 to 6
- saved_result: bfloat16 [16, 4096, 2048], P('dp', 'sp'), may hold values from -6 to 6
- final_adjoint: bfloat16 [16, 4096, 2048], P('dp', 'sp'), may hold values from -6 to 6
- delta_raw: bfloat16 [16, 4096, 32], P('dp', 'sp'), may hold values from -4 to 4
- extra_logdrop: float32 [16, 4096, 32], P('dp', None, 'sp'), may hold values from 0 to 2.1
- source_filter_coefs: float32 [5, 2048], P(None, 'sp'), may hold values from -2.5 to 2.5
- writer_filter_coefs: float32 [5, 256], replicated, may hold values from -2.5 to 2.5
- reader_filter_coefs: float32 [5, 256], replicated, may hold values from -2.5 to 2.5
- delta_offset: float32 [32], P('sp'), may hold values from -7.5 to -6
- fading_exponents: float32 [32], P('sp'), may hold values from -6 to 3.4
- direct_factor: float32 [32], P('sp'), may hold values from 0.1 to 1.9
- rescale_factor: float32 [2048], replicated, may hold values from 0.1 to 1.9
Outputs:
- d_hidden: bfloat16 [16, 4096, 2048], P('dp', 'sp')
- d_x_raw: bfloat16 [16, 4096, 2048], P('dp', 'sp')
- d_gate: bfloat16 [16, 4096, 2048], P('dp', 'sp')
- d_dt_raw: bfloat16 [16, 4096, 32], P('dp', 'sp')
- d_w_b: float32 [2048, 256], P('dp')
- d_w_c: float32 [2048, 256], P('dp')
The draws below stay inside these ranges and needn't reach their ends.
All inputs are finite; a program needn't handle non-finite values.
Results may differ from the reference program's by a relative error of at most 0.012.
Values may be sent and summed in bfloat16 or wider, within the bound.
A program may use at most 128 MiB of HBM per device.

```python
import jax
import jax.numpy as jnp
from jax import lax

D = 2048
HEADS = 32
HEAD_DIM = 64
STATE = 128
GROUPS = 2
NORM_GROUPS = 8
CONV_K = 5
BLOCK = 128
TOK_DEV = 128
INNER = 2048
TOKEN_TOTAL = 4096
BATCH_TOTAL = 16


def draw_delta_raw(key, part):
    key_base, key_shift = jax.random.split(key)
    baseline = jnp.clip(0.7 * jax.random.normal(key_base, (BATCH_TOTAL, TOKEN_TOTAL, HEADS), jnp.float32), -2.8, 2.8)
    blocks = TOKEN_TOTAL // TOK_DEV
    shifts = jax.random.uniform(key_shift, (BATCH_TOTAL, blocks, 1, 1), jnp.float32, -1.0, 1.0)
    shifts = jnp.broadcast_to(shifts, (BATCH_TOTAL, blocks, TOK_DEV, 1)).reshape(BATCH_TOTAL, TOKEN_TOTAL, 1)
    return (baseline + shifts).astype(jnp.bfloat16)


def draw_extra_logdrop(key, part):
    key_where, key_size = jax.random.split(key)
    places = jax.random.randint(key_where, (3, BATCH_TOTAL, 1, HEADS), 0, TOKEN_TOTAL)
    amounts = jax.random.uniform(key_size, (3, BATCH_TOTAL, 1, HEADS), jnp.float32, 0.22, 0.69)
    positions = jnp.arange(TOKEN_TOTAL, dtype=jnp.int32)[None, None, :, None]
    return jnp.sum(jnp.where(positions == places, amounts, 0.0), axis=0)


def draw_fading_exponents(key, part):
    key_pick, key_fast, key_slow = jax.random.split(key, 3)
    fraction = 0.5
    picked = jax.random.uniform(key_pick, (HEADS,), jnp.float32) < fraction
    fast_rate = jax.random.uniform(key_fast, (HEADS,), jnp.float32, 2.3, 3.0)
    slow_rate = jnp.log(jax.random.uniform(key_slow, (HEADS,), jnp.float32, 0.2, 0.8) / (TOKEN_TOTAL * 0.0018))
    return jnp.where(picked, fast_rate, slow_rate)


def strengthened(result, key, source, target, blocks, factor):
    owner, partner = [(jnp.arange(result.shape[position]) // (result.shape[position] // blocks)).reshape([-1 if axis == position else 1 for axis in range(result.ndim)]) for position in (source, target)]
    chosen = jax.random.permutation(key, blocks)[partner]
    strong = (owner == chosen) | (owner == (partner + blocks // 2) % blocks)
    return jnp.where(strong, factor * result, result)


def level_of(stream_key, extent, cuts, smallest, high):
    factor_of = 1.0
    for axis_at, shards_of in cuts:
        heights = jax.random.uniform(jax.random.fold_in(jax.random.fold_in(stream_key, 6), axis_at), (shards_of,), jnp.float32, smallest / len(cuts), high / len(cuts))
        factor_of = factor_of * jnp.repeat(jnp.exp(heights), extent[axis_at] // shards_of).reshape((-1,) + (1,) * (len(extent) - 1 - axis_at))
    return factor_of


def gaussian(key, extent, spread, most, pieces=(), held_as=jnp.bfloat16):
    values = jax.random.normal(key, extent, jnp.float32) * spread
    if len(pieces) > 0:
        values = level_of(key, extent, pieces, -0.22, 0.18) * values
    return jnp.clip(values, min=-most, max=most).astype(held_as)


def bell_draw_with(rng, dims, scale, bound, shards, heavy, kind=jnp.bfloat16):
    entries = scale * jax.random.normal(rng, dims, jnp.float32)
    if shards:
        entries = entries * level_of(rng, dims, shards, -0.22, 0.18)
    return jnp.clip(strengthened(entries, jax.random.fold_in(rng, 3), *heavy), -bound, bound).astype(kind)


def setup_inputs(seed: int = 0) -> dict:
    seeds = jax.random.split(jax.random.key(seed), 17)
    return {
        "layer_activity": bell_draw_with(seeds[0], (BATCH_TOTAL, TOKEN_TOTAL, D), 1.0, 6.0, ((0, 16), (1, 32)), (1, 2, 32, 2.75)),
        "writer_matrix": gaussian(seeds[1], (D, GROUPS * STATE), D ** -0.5, 0.125, ((0, 16),)),
        "reader_matrix": gaussian(seeds[2], (D, GROUPS * STATE), D ** -0.5, 0.125, ((0, 16),)),
        "source_unfiltered": gaussian(seeds[3], (BATCH_TOTAL, TOKEN_TOTAL, INNER), 1.0, 6.0, ((0, 16), (1, 32))),
        "switch_raw_signal": gaussian(seeds[4], (BATCH_TOTAL, TOKEN_TOTAL, INNER), 1.0, 6.0, ((0, 16), (1, 32))),
        "saved_result": gaussian(seeds[5], (BATCH_TOTAL, TOKEN_TOTAL, INNER), 1.0, 6.0, ((0, 16), (1, 32))),
        "final_adjoint": gaussian(seeds[6], (BATCH_TOTAL, TOKEN_TOTAL, INNER), 1.0, 6.0, ((0, 16), (1, 32))),
        "delta_raw": draw_delta_raw(jax.random.fold_in(seeds[16], 71), 0),
        "extra_logdrop": draw_extra_logdrop(jax.random.fold_in(seeds[16], 71), 0),
        "source_filter_coefs": gaussian(seeds[9], (CONV_K, INNER), CONV_K ** -0.5, 2.5, ((1, 32),), jnp.float32),
        "writer_filter_coefs": gaussian(seeds[10], (CONV_K, GROUPS * STATE), CONV_K ** -0.5, 2.5, (), jnp.float32),
        "reader_filter_coefs": gaussian(seeds[11], (CONV_K, GROUPS * STATE), CONV_K ** -0.5, 2.5, (), jnp.float32),
        "delta_offset": jnp.clip(-7.5 + 1.5 * jax.random.uniform(seeds[12], (HEADS,), jnp.float32) ** level_of(seeds[12], (HEADS,), ((0, 32),), -0.2, 0.2), -7.5, -6.0),
        "fading_exponents": draw_fading_exponents(jax.random.fold_in(seeds[16], 71), 0),
        "direct_factor": jnp.clip(1.0 + 0.18 * jax.random.normal(seeds[14], (HEADS,), jnp.float32), 0.1, 1.9),
        "rescale_factor": jnp.clip(1.0 + 0.18 * jax.random.normal(seeds[15], (INNER,), jnp.float32), 0.1, 1.9),
    }


EPSILON = 1e-06
highest = lax.Precision.HIGHEST

def centred_conv(values, tap_weights):
    sample_window = values.shape[0]
    reach_side = (tap_weights.shape[0] - 1) // 2
    padded = jnp.pad(values, ((reach_side, reach_side), (0, 0)))
    summed = jnp.zeros_like(values)
    for offset in range(tap_weights.shape[0]):
        summed = summed + tap_weights[offset][None, :] * padded[offset:offset + sample_window]
    return summed

def one_channel_scan(source_unfiltered, writer_unfiltered, reader_unfiltered, delta_raw, extra_logdrop, source_filter_coefs, writer_filter_coefs, reader_filter_coefs, delta_offset, fading_exponents, direct_factor):
    inputs = jax.nn.silu(centred_conv(source_unfiltered, source_filter_coefs))
    keys_b = jax.nn.silu(centred_conv(writer_unfiltered, writer_filter_coefs))
    reads_c = jax.nn.silu(centred_conv(reader_unfiltered, reader_filter_coefs))
    smooth_delta = jax.nn.softplus(delta_raw + delta_offset)
    channel_fading = smooth_delta * jnp.exp(fading_exponents) + extra_logdrop
    cumulative = jnp.cumsum(channel_fading)
    sample_window = source_unfiltered.shape[0]
    blocks = sample_window // BLOCK
    driven = (inputs * smooth_delta[:, None]).reshape(blocks, BLOCK, -1)
    keyed = keys_b.reshape(blocks, BLOCK, -1)
    reading = reads_c.reshape(blocks, BLOCK, -1)
    levels = cumulative.reshape(blocks, BLOCK)
    within = jnp.exp(-jnp.abs(levels[:, :, None] - levels[:, None, :]))
    scores = jnp.einsum('ktn,ksn->kts', reading, keyed, precision=highest) * within
    output = jnp.einsum('kts,ksp->ktp', scores, driven, precision=highest)
    block_ends = levels[:, -1]
    block_starts = levels[:, 0]
    block_order = jnp.arange(blocks, dtype=jnp.int32)
    prev_end = jnp.concatenate([cumulative[:1], block_ends[:-1]])
    next_start = jnp.concatenate([block_starts[1:], cumulative[-1:]])
    weight_fwd = jnp.exp(levels - block_ends[:, None])
    state_fwd = jnp.einsum('ksn,ksp->knp', keyed * weight_fwd[:, :, None], driven, precision=highest)
    mask_fwd = (block_order[None, :] < block_order[:, None]).astype(cumulative.dtype)
    link_fwd = jnp.exp(-jnp.abs(prev_end[:, None] - block_ends[None, :])) * mask_fwd
    carry_fwd = jnp.einsum('kj,jnp->knp', link_fwd, state_fwd, precision=highest)
    read_fwd = reading * jnp.exp(prev_end[:, None] - levels)[:, :, None]
    weight_bwd = jnp.exp(block_starts[:, None] - levels)
    state_bwd = jnp.einsum('ksn,ksp->knp', keyed * weight_bwd[:, :, None], driven, precision=highest)
    mask_bwd = (block_order[None, :] > block_order[:, None]).astype(cumulative.dtype)
    link_bwd = jnp.exp(-jnp.abs(next_start[:, None] - block_starts[None, :])) * mask_bwd
    carry_bwd = jnp.einsum('kj,jnp->knp', link_bwd, state_bwd, precision=highest)
    read_bwd = reading * jnp.exp(levels - next_start[:, None])[:, :, None]
    output = output + jnp.einsum('ktn,knp->ktp', read_fwd, carry_fwd, precision=highest)
    output = output + jnp.einsum('ktn,knp->ktp', read_bwd, carry_bwd, precision=highest)
    return output.reshape(sample_window, -1) + direct_factor * inputs

def channelwise_derivs(source_unfiltered, writer_unfiltered, reader_unfiltered, delta_raw, extra_logdrop, source_filter_coefs, writer_filter_coefs, reader_filter_coefs, delta_offset, fading_exponents, direct_factor, result_adjoint):

    def forward(source_filtered, writer_filtered, reader_filtered, delta_argument):
        return one_channel_scan(source_filtered, writer_filtered, reader_filtered, delta_argument, extra_logdrop, source_filter_coefs, writer_filter_coefs, reader_filter_coefs, delta_offset, fading_exponents, direct_factor)
    primal, pullback = jax.vjp(forward, source_unfiltered.astype(jnp.float32), writer_unfiltered.astype(jnp.float32), reader_unfiltered.astype(jnp.float32), delta_raw.astype(jnp.float32))
    source_derivative, writer_derivative, reader_derivative, delta_derivative = pullback(result_adjoint.astype(jnp.float32))
    return (source_derivative.astype(jnp.bfloat16), writer_derivative.astype(jnp.bfloat16), reader_derivative.astype(jnp.bfloat16), delta_derivative.astype(jnp.bfloat16))

def gated_norm(values, gating, rescale_factor):
    mixed = values * jax.nn.silu(gating)
    grouped = mixed.reshape(mixed.shape[0], NORM_GROUPS, -1)
    scaled = grouped * lax.rsqrt(lax.optimization_barrier(jnp.mean(grouped * grouped, axis=-1, keepdims=True)) + EPSILON)
    return scaled.reshape(mixed.shape) * rescale_factor

def norm_backward(saved_result, switch_raw_signal, final_adjoint, rescale_factor):
    primal, pullback = jax.vjp(lambda values, gating: gated_norm(values, gating, rescale_factor), saved_result.astype(jnp.float32), switch_raw_signal.astype(jnp.float32))
    d_values, d_gates = pullback(final_adjoint.astype(jnp.float32))
    return (d_values.astype(jnp.bfloat16), d_gates.astype(jnp.bfloat16))

def reference(layer_activity, writer_matrix, reader_matrix, source_unfiltered, switch_raw_signal, saved_result, final_adjoint, delta_raw, extra_logdrop, source_filter_coefs, writer_filter_coefs, reader_filter_coefs, delta_offset, fading_exponents, direct_factor, rescale_factor):
    latent_dimension = GROUPS * STATE
    per_group = HEADS // GROUPS
    group_of = jnp.arange(HEADS, dtype=jnp.int32) // per_group
    token_rows = layer_activity.reshape(BATCH_TOTAL * TOKEN_TOTAL, D)
    writer_linear = jnp.dot(token_rows, writer_matrix, preferred_element_type=jnp.float32).astype(jnp.bfloat16)
    reader_linear = jnp.dot(token_rows, reader_matrix, preferred_element_type=jnp.float32).astype(jnp.bfloat16)
    source_filter_fn = jnp.transpose(source_filter_coefs.reshape(CONV_K, HEADS, HEAD_DIM), (1, 0, 2))
    writer_filter_fn = jnp.transpose(writer_filter_coefs.reshape(CONV_K, GROUPS, STATE)[:, group_of], (1, 0, 2))
    reader_filter_fn = jnp.transpose(reader_filter_coefs.reshape(CONV_K, GROUPS, STATE)[:, group_of], (1, 0, 2))

    def one_sample_pass(collected_parts):
        sample_source, sample_writer, sample_reader, sample_delta, sample_logdrop_lines, sample_result, sample_switch, sample_final = collected_parts
        result_adjoint, d_gate = norm_backward(sample_result, sample_switch, sample_final, rescale_factor)
        channelwise_source = jnp.transpose(sample_source.reshape(TOKEN_TOTAL, HEADS, HEAD_DIM), (1, 0, 2))
        channelwise_writer = jnp.transpose(sample_writer.reshape(TOKEN_TOTAL, GROUPS, STATE)[:, group_of], (1, 0, 2))
        channelwise_reader = jnp.transpose(sample_reader.reshape(TOKEN_TOTAL, GROUPS, STATE)[:, group_of], (1, 0, 2))
        channelwise_adjoint = jnp.transpose(result_adjoint.reshape(TOKEN_TOTAL, HEADS, HEAD_DIM), (1, 0, 2))
        source_derivative, writer_derivative, reader_derivative, delta_derivative = lax.map(lambda collected_items: channelwise_derivs(*collected_items), (channelwise_source, channelwise_writer, channelwise_reader, sample_delta.T, sample_logdrop_lines.T, source_filter_fn, writer_filter_fn, reader_filter_fn, delta_offset, fading_exponents, direct_factor, channelwise_adjoint))
        summed_b = lax.optimization_barrier(jnp.sum(writer_derivative.astype(jnp.float32).reshape(GROUPS, per_group, TOKEN_TOTAL, STATE), axis=1))
        summed_c = lax.optimization_barrier(jnp.sum(reader_derivative.astype(jnp.float32).reshape(GROUPS, per_group, TOKEN_TOTAL, STATE), axis=1))
        summed_b = jnp.transpose(summed_b, (1, 0, 2)).reshape(TOKEN_TOTAL, latent_dimension).astype(jnp.bfloat16)
        summed_c = jnp.transpose(summed_c, (1, 0, 2)).reshape(TOKEN_TOTAL, latent_dimension).astype(jnp.bfloat16)
        return (jnp.transpose(source_derivative, (1, 0, 2)).reshape(TOKEN_TOTAL, INNER), summed_b, summed_c, delta_derivative.T, d_gate)
    whole_batch_source, whole_batch_writer, whole_batch_reader, whole_batch_delta, whole_batch_switch = lax.map(one_sample_pass, (source_unfiltered, writer_linear.reshape(BATCH_TOTAL, TOKEN_TOTAL, latent_dimension), reader_linear.reshape(BATCH_TOTAL, TOKEN_TOTAL, latent_dimension), delta_raw, extra_logdrop, saved_result, switch_raw_signal, final_adjoint))
    grad_rows_b = whole_batch_writer.reshape(BATCH_TOTAL * TOKEN_TOTAL, latent_dimension)
    grad_rows_c = whole_batch_reader.reshape(BATCH_TOTAL * TOKEN_TOTAL, latent_dimension)
    d_hidden = (jnp.dot(grad_rows_b, writer_matrix.T, preferred_element_type=jnp.float32) + jnp.dot(grad_rows_c, reader_matrix.T, preferred_element_type=jnp.float32)).astype(jnp.bfloat16)
    d_w_b = jnp.dot(token_rows.T, grad_rows_b, preferred_element_type=jnp.float32)
    d_w_c = jnp.dot(token_rows.T, grad_rows_c, preferred_element_type=jnp.float32)
    return (d_hidden.reshape(BATCH_TOTAL, TOKEN_TOTAL, D), whole_batch_source, whole_batch_switch, whole_batch_delta, d_w_b, d_w_c)
```

```python
import functools

import jax
import jax.numpy as jnp
from jax import lax
from jax.experimental import pallas as pl
from jax.experimental.pallas import tpu as pltpu
from jax.sharding import Mesh
from jax.sharding import PartitionSpec as P

HEADS = 32
HEAD_DIM = 64
STATE = 128
GROUPS = 2
NORM_GROUPS = 8
CONV_K = 5
BLOCK = 128
INNER = 2048
NZ, NX, NY, NC = 8, 4, 8, 2
LH = HEADS // NX
LW = LH * HEAD_DIM
CHUNK = NX * BLOCK
EDGE = 16
EPSILON = 1e-06
VMEM_LIMIT = 60 * 1024 * 1024

f32 = jnp.float32
bf16 = jnp.bfloat16
highest = lax.Precision.HIGHEST
MESH = pl.DeviceIdType.MESH
DMA = pltpu.SemaphoreType.DMA


def vmem():
    return pl.BlockSpec(memory_space=pltpu.VMEM)


def remote(src, dst, send, recv, device):
    return pltpu.make_async_remote_copy(
        src_ref=src, dst_ref=dst, send_sem=send, recv_sem=recv, device_id=device, device_id_type=MESH
    )


def greet(barrier, device):
    pl.semaphore_signal(barrier, inc=1, device_id=device, device_id_type=MESH)


def columns(start, size):
    return pl.ds(pl.multiple_of(start * size, size), size)


def norm_kernel(saved_ref, switch_ref, final_ref, gain_ref, dy_ref, dgate_ref):
    width = INNER // NORM_GROUPS
    for group in range(NORM_GROUPS):
        cols = slice(group * width, (group + 1) * width)
        saved = saved_ref[:, cols].astype(f32)
        switch = switch_ref[:, cols].astype(f32)
        final = final_ref[:, cols].astype(f32)
        gate = 1.0 / (1.0 + jnp.exp(-switch))
        act = switch * gate
        mixed = saved * act
        scale = lax.rsqrt(jnp.mean(mixed * mixed, axis=-1, keepdims=True) + EPSILON)
        d_normed = final * gain_ref[:, cols]
        inner = jnp.mean(d_normed * mixed, axis=-1, keepdims=True)
        d_mixed = d_normed * scale - mixed * (scale * scale * scale * inner)
        dy_ref[:, cols] = (d_mixed * act).astype(bf16)
        slope = gate * (1.0 + switch * (1.0 - gate))
        dgate_ref[:, cols] = (d_mixed * saved * slope).astype(bf16)


def norm_backward(saved, switch, final, gain):
    out = jax.ShapeDtypeStruct(saved.shape, bf16)
    return pl.pallas_call(
        norm_kernel,
        out_shape=(out, out),
        in_specs=[vmem()] * 4,
        out_specs=(vmem(), vmem()),
        compiler_params=pltpu.CompilerParams(vmem_limit_bytes=VMEM_LIMIT),
        name="norm_backward",
    )(saved, switch, final, gain)


def exchange_in_kernel(
    w_ref, x_ref, dy_ref, dt_ref, msg_ref,
    wf_ref, xh_ref, dyh_ref, dth_ref, prm_ref, xp_ref, xn_ref,
    own_sem, xs, xr, ys, yr, ts, tr, ms, mr, hs, hr, rs, rr, ls, lr, ps, pr,
):
    z, x, y, c = (lax.axis_index(name) for name in ("z", "x", "y", "c"))
    half = BLOCK // 2
    up, down = lax.rem(z + 1, NZ), lax.rem(z + NZ - 1, NZ)
    right, left = lax.rem(y + 1, NY), lax.rem(y + NY - 1, NY)
    other = 1 - c
    head = z * NX + x
    dest = z // 2
    slot = lax.rem(head, LH)
    mine = dest == x

    barrier = pltpu.get_barrier_semaphore()
    for d in range(1, NX):
        greet(barrier, {"x": lax.rem(x + d, NX)})
    greet(barrier, {"z": up})
    greet(barrier, {"z": down})
    greet(barrier, {"y": right})
    greet(barrier, {"y": left})
    greet(barrier, {"c": other})
    for i in range(LH):
        sz, sx = 2 * x + i // NX, i % NX

        @pl.when(jnp.logical_not(jnp.logical_and(sz == z, sx == x)))
        def _():
            greet(barrier, {"z": sz, "x": sx})

    pl.semaphore_wait(barrier, NX - 1 + 5 + NZ - mine.astype(jnp.int32))

    def rows(h):
        return pl.ds(h * half, half)

    def ring_right(s, h):
        block = lax.rem(y - s + NY, NY) * NC + c
        src = w_ref.at[rows(h)] if s == 0 else wf_ref.at[block, rows(h)]
        return remote(src, wf_ref.at[block, rows(h)], rs.at[s, h], rr.at[s, h], {"y": right})

    def ring_left(s, h):
        block = lax.rem(y + s, NY) * NC + c
        src = w_ref.at[rows(h)] if s == 0 else wf_ref.at[block, rows(h)]
        return remote(src, wf_ref.at[block, rows(h)], ls.at[s, h], lr.at[s, h], {"y": left})

    def across(n, h):
        offset = 0 if n == 0 else (-n if n < 5 else n - 4)
        block = lax.rem(y + offset + NY, NY) * NC + c
        src = w_ref.at[rows(h)] if n == 0 else wf_ref.at[block, rows(h)]
        return remote(src, wf_ref.at[block, rows(h)], ps.at[n, h], pr.at[n, h], {"c": other})

    for h in range(2):
        ring_right(0, h).start()
        ring_left(0, h).start()

    own = [
        pltpu.make_async_copy(w_ref, wf_ref.at[y * NC + c], own_sem.at[0]),
        pltpu.make_async_copy(x_ref.at[:, columns(x, LW)], xh_ref.at[x], own_sem.at[1]),
        pltpu.make_async_copy(dy_ref.at[:, columns(x, LW)], dyh_ref.at[x], own_sem.at[2]),
        pltpu.make_async_copy(dt_ref.at[columns(x, LH)], dth_ref.at[x], own_sem.at[3]),
    ]
    for copy in own:
        copy.start()

    def to_x(d):
        peer = lax.rem(x + d, NX)
        device = {"x": peer}
        return (
            remote(x_ref.at[:, columns(peer, LW)], xh_ref.at[x], xs.at[d - 1], xr.at[d - 1], device),
            remote(dt_ref.at[columns(peer, LH)], dth_ref.at[x], ts.at[d - 1], tr.at[d - 1], device),
            remote(dy_ref.at[:, columns(peer, LW)], dyh_ref.at[x], ys.at[d - 1], yr.at[d - 1], device),
        )

    for d in range(1, NX):
        for copy in to_x(d):
            copy.start()

    def message(i):
        return remote(
            msg_ref.at[i], prm_ref.at[slot], ms.at[i], mr.at[slot], {"z": jnp.int32(i), "x": dest}
        )

    keep = pltpu.make_async_copy(msg_ref.at[z], prm_ref.at[slot], own_sem.at[4])
    for i in range(NZ):

        @pl.when(jnp.logical_not(jnp.logical_and(mine, z == i)))
        def _():
            message(i).start()

    @pl.when(mine)
    def _():
        keep.start()

    for h in range(2):
        across(0, h).start()

    for d in range(1, NX):
        to_x(d)[0].wait_recv()
    own[1].wait()
    edge_up = remote(xh_ref.at[NX - 1, pl.ds(BLOCK - EDGE, EDGE)], xp_ref, hs.at[0], hr.at[0], {"z": up})
    edge_down = remote(xh_ref.at[0, pl.ds(0, EDGE)], xn_ref, hs.at[1], hr.at[1], {"z": down})
    edge_up.start()
    edge_down.start()

    for s in range(4):
        for h in range(2):
            ring_right(s, h).wait_recv()
            if s < 3:
                ring_right(s + 1, h).start()
            across(1 + s, h).start()
            if s < 3:
                ring_left(s, h).wait_recv()
                if s < 2:
                    ring_left(s + 1, h).start()
                across(5 + s, h).start()

    for d in range(1, NX):
        copies = to_x(d)
        copies[0].wait_send()
        copies[1].wait()
        copies[2].wait()
    edge_up.wait()
    edge_down.wait()
    for i in range(LH):
        sz, sx = 2 * x + i // NX, i % NX

        @pl.when(jnp.logical_not(jnp.logical_and(sz == z, sx == x)))
        def _():
            remote(msg_ref.at[i], prm_ref.at[i], ms.at[i], mr.at[i], {"z": sz, "x": sx}).wait_recv()

    for i in range(NZ):

        @pl.when(jnp.logical_not(jnp.logical_and(mine, z == i)))
        def _():
            message(i).wait_send()

    @pl.when(mine)
    def _():
        keep.wait()

    for n in (0, 2, 3):
        own[n].wait()
    for h in range(2):
        for s in range(4):
            ring_right(s, h).wait_send()
        for s in range(3):
            ring_left(s, h).wait_send()
        for n in range(8):
            across(n, h).wait()


def exchange_in(w, x, dy, dt, msg):
    shapes = (
        jax.ShapeDtypeStruct((NY * NC, BLOCK, 2 * GROUPS * STATE), bf16),
        jax.ShapeDtypeStruct((NX, BLOCK, LW), bf16),
        jax.ShapeDtypeStruct((NX, BLOCK, LW), bf16),
        jax.ShapeDtypeStruct((NX, LH, BLOCK), f32),
        jax.ShapeDtypeStruct((LH, 16, BLOCK), f32),
        jax.ShapeDtypeStruct((EDGE, LW), bf16),
        jax.ShapeDtypeStruct((EDGE, LW), bf16),
    )
    return pl.pallas_call(
        exchange_in_kernel,
        out_shape=shapes,
        in_specs=[vmem()] * 5,
        out_specs=tuple(vmem() for _ in shapes),
        scratch_shapes=[
            DMA((5,)), DMA((3,)), DMA((3,)), DMA((3,)), DMA((3,)), DMA((3,)), DMA((3,)),
            DMA((8,)), DMA((8,)), DMA((2,)), DMA((2,)),
            DMA((4, 2)), DMA((4, 2)), DMA((3, 2)), DMA((3, 2)), DMA((8, 2)), DMA((8, 2)),
        ],
        compiler_params=pltpu.CompilerParams(
            collective_id=0, has_side_effects=True, vmem_limit_bytes=VMEM_LIMIT
        ),
        name="exchange_in",
    )(w, x, dy, dt, msg)


def maps_in_kernel(bc_ref, out_ref, prev_ref, next_ref, own_sem, send, recv, hs, hr):
    z, x = lax.axis_index("z"), lax.axis_index("x")
    up, down = lax.rem(z + 1, NZ), lax.rem(z + NZ - 1, NZ)
    barrier = pltpu.get_barrier_semaphore()
    for d in range(1, NX):
        greet(barrier, {"x": lax.rem(x + d, NX)})
    greet(barrier, {"z": up})
    greet(barrier, {"z": down})
    pl.semaphore_wait(barrier, NX + 1)

    def to_x(d):
        peer = lax.rem(x + d, NX)
        return remote(
            bc_ref.at[:, columns(peer // 2, 2 * STATE)], out_ref.at[x], send.at[d - 1], recv.at[d - 1], {"x": peer}
        )

    for d in range(1, NX):
        to_x(d).start()
    own = pltpu.make_async_copy(bc_ref.at[:, columns(x // 2, 2 * STATE)], out_ref.at[x], own_sem.at[0])
    own.start()
    own.wait()
    for d in range(1, NX):
        to_x(d).wait_recv()
    edge_up = remote(out_ref.at[NX - 1, pl.ds(BLOCK - EDGE, EDGE)], prev_ref, hs.at[0], hr.at[0], {"z": up})
    edge_down = remote(out_ref.at[0, pl.ds(0, EDGE)], next_ref, hs.at[1], hr.at[1], {"z": down})
    edge_up.start()
    edge_down.start()
    for d in range(1, NX):
        to_x(d).wait_send()
    edge_up.wait()
    edge_down.wait()


def maps_in(bc):
    shapes = (
        jax.ShapeDtypeStruct((NX, BLOCK, 2 * STATE), bf16),
        jax.ShapeDtypeStruct((EDGE, 2 * STATE), bf16),
        jax.ShapeDtypeStruct((EDGE, 2 * STATE), bf16),
    )
    return pl.pallas_call(
        maps_in_kernel,
        out_shape=shapes,
        in_specs=[vmem()],
        out_specs=tuple(vmem() for _ in shapes),
        scratch_shapes=[DMA((1,)), DMA((3,)), DMA((3,)), DMA((2,)), DMA((2,))],
        compiler_params=pltpu.CompilerParams(
            collective_id=1, has_side_effects=True, vmem_limit_bytes=VMEM_LIMIT
        ),
        name="maps_in",
    )(bc)


def scan_kernel(sr_ref, sl_ref, decay_ref, cr_ref, cl_ref, outr, outl, rs, rr, ls, lr):
    z = lax.axis_index("z")
    up, down = lax.rem(z + 1, NZ), lax.rem(z + NZ - 1, NZ)
    first, last = z == 0, z == NZ - 1
    barrier = pltpu.get_barrier_semaphore()

    @pl.when(jnp.logical_not(first))
    def _():
        greet(barrier, {"z": down})

    @pl.when(jnp.logical_not(last))
    def _():
        greet(barrier, {"z": up})

    @pl.when(first)
    def _():
        cr_ref[...] = jnp.zeros_like(cr_ref)

    @pl.when(last)
    def _():
        cl_ref[...] = jnp.zeros_like(cl_ref)

    pl.semaphore_wait(barrier, 2 - first.astype(jnp.int32) - last.astype(jnp.int32))
    count = 2 * LW // 128

    def piece(n):
        return n // (LW // 128), slice(None), columns(lax.rem(n, LW // 128), 128)

    def going_up(n):
        return remote(outr.at[piece(n)], cr_ref.at[piece(n)], rs.at[n], rr.at[n], {"z": up})

    def going_down(n):
        return remote(outl.at[piece(n)], cl_ref.at[piece(n)], ls.at[n], lr.at[n], {"z": down})

    def step(t, carry):
        n = t - z

        @pl.when(jnp.logical_and(n >= 0, n < count))
        def _():
            @pl.when(jnp.logical_not(first))
            def _():
                going_up(n).wait_recv()

            @pl.when(jnp.logical_not(last))
            def _():
                at = piece(n)
                outr[at] = (cr_ref[at].astype(f32) * decay_ref[0:1, at[2]] + sr_ref[at]).astype(bf16)
                going_up(n).start()

        m = t - (NZ - 1 - z)

        @pl.when(jnp.logical_and(m >= 0, m < count))
        def _():
            @pl.when(jnp.logical_not(last))
            def _():
                going_down(m).wait_recv()

            @pl.when(jnp.logical_not(first))
            def _():
                at = piece(m)
                outl[at] = (cl_ref[at].astype(f32) * decay_ref[0:1, at[2]] + sl_ref[at]).astype(bf16)
                going_down(m).start()

        return carry

    lax.fori_loop(0, NZ - 1 + count, step, 0)
    for n in range(count):

        @pl.when(jnp.logical_not(last))
        def _():
            going_up(jnp.int32(n)).wait_send()

        @pl.when(jnp.logical_not(first))
        def _():
            going_down(jnp.int32(n)).wait_send()


def scan_states(sr, sl, decay):
    out = jax.ShapeDtypeStruct((2, STATE, LW), bf16)
    return pl.pallas_call(
        scan_kernel,
        out_shape=(out, out),
        in_specs=[vmem()] * 3,
        out_specs=(vmem(), vmem()),
        scratch_shapes=[
            pltpu.VMEM((2, STATE, LW), bf16),
            pltpu.VMEM((2, STATE, LW), bf16),
            DMA((8,)), DMA((8,)), DMA((8,)), DMA((8,)),
        ],
        compiler_params=pltpu.CompilerParams(
            collective_id=2, has_side_effects=True, vmem_limit_bytes=VMEM_LIMIT
        ),
        name="scan_states",
    )(sr, sl, decay)


def dot(a, b):
    return jnp.dot(a, b, preferred_element_type=f32)


def dot_nt(a, b):
    return lax.dot_general(a, b, (((1,), (1,)), ((), ())), preferred_element_type=f32)


def dot_tn(a, b):
    return lax.dot_general(a, b, (((0,), (0,)), ((), ())), preferred_element_type=f32)


def iota2(shape, dim):
    return lax.broadcasted_iota(jnp.int32, shape, dim)


def parts_of(value, count):
    out = []
    for _ in range(count):
        top = value.astype(bf16).astype(f32)
        out.append(top)
        value = value - top
    return out


def spreaders():
    r, cc = iota2((48, 3 * LW), 0), iota2((48, 3 * LW), 1)
    three = jnp.logical_and(r // 16 == cc // LW, lax.rem(r, 8) == lax.rem(cc, LW) // HEAD_DIM)
    r, cc = iota2((24, LH * BLOCK), 0), iota2((24, LH * BLOCK), 1)
    wide = lax.rem(r, 8) == cc // BLOCK
    r, cc = iota2((LH, 2 * LW), 0), iota2((LH, 2 * LW), 1)
    gather = lax.rem(cc, LW) // HEAD_DIM == r
    return three.astype(bf16), wide.astype(bf16), gather.astype(bf16)


def per_head_sum(gather_ref, value):
    return dot_nt(gather_ref[...], jnp.concatenate(parts_of(value, 2), axis=1).astype(bf16))


def silu_parts(pre):
    gate = 1.0 / (1.0 + jnp.exp(-pre))
    return pre * gate, gate * (1.0 + pre * (1.0 - gate))


def pair_row(prm_ref, row, j):
    lane = iota2((1, 128), 1)
    return jnp.where(lane < HEAD_DIM, prm_ref[row, 2 * j : 2 * j + 1, :], prm_ref[row, 2 * j + 1 : 2 * j + 2, :])


def fill_padded(pad_ref, body_ref, prev_ref, next_ref, z):
    pad_ref[pl.ds(0, EDGE)] = jnp.where(z == 0, 0.0, prev_ref[...].astype(f32))
    for k in range(NX):
        pad_ref[pl.ds(EDGE + k * BLOCK, BLOCK)] = body_ref[k].astype(f32)
    pad_ref[pl.ds(EDGE + CHUNK, EDGE)] = jnp.where(z == NZ - 1, 0.0, next_ref[...].astype(f32))


def maps_of(bcp_ref, taps_ref, rows, which):
    lanes = slice(which * STATE, (which + 1) * STATE)
    pre = jnp.zeros((rows.size, STATE), f32)
    for tap in range(CONV_K):
        pre = pre + taps_ref[tap : tap + 1, lanes] * bcp_ref[pl.ds(rows.start + EDGE - 2 + tap, rows.size), lanes]
    return silu_parts(pre)


def block_scalars(prm_ref, dth_ref, k, upper):
    raw = dth_ref[k] + prm_ref[9]
    dt = jax.nn.softplus(raw)
    rate = dt * jnp.exp(prm_ref[10]) + prm_ref[k]
    level = jnp.dot(rate, upper, precision=highest, preferred_element_type=f32)
    total = level[:, BLOCK - 1 : BLOCK]
    return raw, dt, level, jnp.exp(-level), jnp.exp(level - total)


def prepare(
    k, prm_ref, dth_ref, dyh_ref, bcp_ref, taps_ref, xpad_ref, three_ref,
    v16, pv16, qv16, pdy16, qdy16, b16, c16, gamma, u_ref, slope_ref, spread_ref, bs_ref, cs_ref, level_ref,
):
    row, col = iota2((BLOCK, BLOCK), 0), iota2((BLOCK, BLOCK), 1)
    upper = (row <= col).astype(f32)
    raw, dt, level, p, q = block_scalars(prm_ref, dth_ref, k, upper)
    stack = jnp.concatenate(parts_of(dt, 2) + parts_of(p, 2) + parts_of(q, 2), axis=0)
    spread = dot_tn(stack.astype(bf16), three_ref[...])
    rows = pl.ds(k * BLOCK, BLOCK)
    keys, key_slope = maps_of(bcp_ref, taps_ref, rows, 0)
    reads, read_slope = maps_of(bcp_ref, taps_ref, rows, 1)
    b16[rows], c16[rows] = keys.astype(bf16), reads.astype(bf16)
    if level_ref is not None:
        level_ref[k] = level
        spread_ref[rows] = spread
        bs_ref[rows], cs_ref[rows] = key_slope, read_slope
    gamma[k] = jnp.broadcast_to(spread[BLOCK - 1 : BLOCK, LW : 2 * LW], (8, LW))
    for j in range(LH // 2):
        lanes = slice(128 * j, 128 * (j + 1))
        pre = jnp.zeros((BLOCK, 128), f32)
        for tap in range(CONV_K):
            pre = pre + pair_row(prm_ref, 4 + tap, j) * xpad_ref[pl.ds(k * BLOCK + EDGE - 2 + tap, BLOCK), lanes]
        u, slope = silu_parts(pre)
        if u_ref is not None:
            u_ref[rows, lanes], slope_ref[rows, lanes] = u, slope
        pe = spread[:, LW + 128 * j : LW + 128 * (j + 1)]
        qe = spread[:, 2 * LW + 128 * j : 2 * LW + 128 * (j + 1)]
        v = u * spread[:, lanes]
        dy = dyh_ref[k, :, lanes].astype(f32)
        if v16 is not None:
            v16[rows, lanes] = v.astype(bf16)
        pv16[rows, lanes], qv16[rows, lanes] = (pe * v).astype(bf16), (qe * v).astype(bf16)
        pdy16[rows, lanes], qdy16[rows, lanes] = (pe * dy).astype(bf16), (qe * dy).astype(bf16)


def block_states(k, b16, c16, pv16, qv16, pdy16, qdy16):
    rows = pl.ds(k * BLOCK, BLOCK)
    b, c = b16[rows], c16[rows]
    return (
        dot_tn(b, qv16[rows]), dot_tn(c, qdy16[rows]),
        dot_tn(b, pv16[rows]), dot_tn(c, pdy16[rows]),
    )


def states_kernel(
    xh_ref, xp_ref, xn_ref, dyh_ref, bch_ref, bp_ref, bn_ref, dth_ref, prm_ref, taps_ref, three_ref,
    sr_ref, sl_ref, decay_ref,
    xpad, bcpad, pv16, qv16, pdy16, qdy16, b16, c16, gamma,
):
    z = lax.axis_index("z")
    fill_padded(xpad, xh_ref, xp_ref, xn_ref, z)
    fill_padded(bcpad, bch_ref, bp_ref, bn_ref, z)
    decay_ref[...] = jnp.ones_like(decay_ref)
    for k in range(NX):
        prepare(
            k, prm_ref, dth_ref, dyh_ref, bcpad, taps_ref, xpad, three_ref,
            None, pv16, qv16, pdy16, qdy16, b16, c16, gamma, None, None, None, None, None, None,
        )
        kvr, cdr, kvl, cdl = block_states(k, b16, c16, pv16, qv16, pdy16, qdy16)
        g = gamma[k, 0:1]
        if k == 0:
            sr_ref[0], sr_ref[1], sl_ref[0], sl_ref[1] = kvr, cdr, kvl, cdl
        else:
            before = decay_ref[0:1]
            sr_ref[0] = sr_ref[0] * g + kvr
            sr_ref[1] = sr_ref[1] * g + cdr
            sl_ref[0] = sl_ref[0] + before * kvl
            sl_ref[1] = sl_ref[1] + before * cdl
        decay_ref[...] = decay_ref[...] * gamma[k]


def chunk_states(xh, xp, xn, dyh, bch, bp, bn, dth, prm, taps, three):
    state = jax.ShapeDtypeStruct((2, STATE, LW), f32)
    wide16 = pltpu.VMEM((CHUNK, LW), bf16)
    return pl.pallas_call(
        states_kernel,
        out_shape=(state, state, jax.ShapeDtypeStruct((8, LW), f32)),
        in_specs=[vmem()] * 11,
        out_specs=(vmem(),) * 3,
        scratch_shapes=[
            pltpu.VMEM((CHUNK + 2 * EDGE, LW), f32),
            pltpu.VMEM((CHUNK + 2 * EDGE, 2 * STATE), f32),
            wide16, wide16, wide16, wide16,
            pltpu.VMEM((CHUNK, STATE), bf16),
            pltpu.VMEM((CHUNK, STATE), bf16),
            pltpu.VMEM((NX, 8, LW), f32),
        ],
        compiler_params=pltpu.CompilerParams(vmem_limit_bytes=VMEM_LIMIT),
        name="chunk_states",
    )(xh, xp, xn, dyh, bch, bp, bn, dth, prm, taps, three)


def unconvolved(pad_ref, start, size, lanes, tap_of):
    total = jnp.zeros((size, 128), f32)
    for tap in range(CONV_K):
        total = total + tap_of(tap) * pad_ref[pl.ds(start + 2 * EDGE + 2 - tap, size), lanes]
    return total


def gradients_kernel(
    xh_ref, xp_ref, xn_ref, dyh_ref, bch_ref, bp_ref, bn_ref, dth_ref, prm_ref, taps_ref,
    three_ref, wide_ref, gather_ref, cr_ref, cl_ref,
    dx_ref, dxp_ref, dxn_ref, dbc_ref, dbp_ref, dbn_ref, ddt_ref,
    xpad, bcpad, v16, pv16, qv16, pdy16, qdy16, b16, c16, gamma, u_scr, slope_scr, spread_scr,
    bs_scr, cs_scr, level_scr, right, left, dxpad, dbcpad, dl_scr, dvu_scr,
):
    z = lax.axis_index("z")
    fill_padded(xpad, xh_ref, xp_ref, xn_ref, z)
    fill_padded(bcpad, bch_ref, bp_ref, bn_ref, z)
    for pad in (dxpad, dbcpad):
        pad[pl.ds(0, 2 * EDGE)] = jnp.zeros((2 * EDGE, pad.shape[1]), f32)
        pad[pl.ds(2 * EDGE + CHUNK, 2 * EDGE)] = jnp.zeros((2 * EDGE, pad.shape[1]), f32)
    row, col = iota2((BLOCK, BLOCK), 0), iota2((BLOCK, BLOCK), 1)
    sign = (row > col).astype(f32) - (row < col).astype(f32)
    lower = (row >= col).astype(f32)
    lane = iota2((BLOCK, 128), 1)
    low_half = lane < HEAD_DIM
    head_row = iota2((8, BLOCK), 0)

    right[0, 0], right[0, 1] = cr_ref[0].astype(f32), cr_ref[1].astype(f32)
    left[NX - 1, 0], left[NX - 1, 1] = cl_ref[0].astype(f32), cl_ref[1].astype(f32)
    for k in range(NX):
        prepare(
            k, prm_ref, dth_ref, dyh_ref, bcpad, taps_ref, xpad, three_ref,
            v16, pv16, qv16, pdy16, qdy16, b16, c16, gamma, u_scr, slope_scr, spread_scr, bs_scr, cs_scr, level_scr,
        )
        kvr, cdr, kvl, cdl = block_states(k, b16, c16, pv16, qv16, pdy16, qdy16)
        g = gamma[k, 0:1]
        right[k + 1, 0] = right[k, 0] * g + kvr
        right[k + 1, 1] = right[k, 1] * g + cdr
        if k > 0:
            left[k - 1, 0], left[k - 1, 1] = kvl, cdl
    for k in range(NX - 2, -1, -1):
        g = gamma[k + 1, 0:1]
        left[k, 0] = left[k, 0] + g * left[k + 1, 0]
        left[k, 1] = left[k, 1] + g * left[k + 1, 1]

    def block(k, carry):
        rows = pl.ds(pl.multiple_of(k * BLOCK, BLOCK), BLOCK)
        b, c = b16[rows], c16[rows]
        grid = dot_nt(c, b)
        grid_t = dot_nt(b, c)
        signed = grid * sign
        level = level_scr[k]
        level_cols = dot_tn(jnp.concatenate(parts_of(level, 3), axis=0).astype(bf16), wide_ref[...])
        weights = jnp.zeros((BLOCK, BLOCK), f32)
        dl = jnp.zeros((8, BLOCK), f32)
        dc = jnp.zeros((BLOCK, STATE), f32)
        db = jnp.zeros((BLOCK, STATE), f32)
        dvu = jnp.zeros((8, BLOCK), f32)
        for j in range(LH // 2):
            lanes = slice(128 * j, 128 * (j + 1))
            vj = v16[rows, lanes]
            dyj = dyh_ref[k, :, lanes]
            halves = []
            for i in range(2):
                h = 2 * j + i
                near = jnp.exp(-jnp.abs(level_cols[:, 128 * h : 128 * (h + 1)] - level[h : h + 1, :]))
                keep = low_half if i == 0 else jnp.logical_not(low_half)
                shared = dot_nt(jnp.where(keep, dyj, jnp.zeros_like(dyj)), vj) * near
                weights = weights + shared
                crossing = (shared * signed).astype(bf16)
                pick = (head_row == h).astype(bf16)
                dl = dl + dot(pick, crossing) - dot_nt(pick, crossing)
                halves.append(dot((grid_t * near).astype(bf16), dyj))
            kvr, cdr = right[k, 0, :, lanes].astype(bf16), right[k, 1, :, lanes].astype(bf16)
            kvl, cdl = left[k, 0, :, lanes].astype(bf16), left[k, 1, :, lanes].astype(bf16)
            pe = spread_scr[rows, LW + 128 * j : LW + 128 * (j + 1)]
            qe = spread_scr[rows, 2 * LW + 128 * j : 2 * LW + 128 * (j + 1)]
            from_later, from_earlier = dot(b, cdl), dot(b, cdr)
            pv, qv, pdy, qdy = pv16[rows, lanes], qv16[rows, lanes], pdy16[rows, lanes], qdy16[rows, lanes]
            dv = jnp.where(low_half, halves[0], halves[1]) + qe * from_later + pe * from_earlier
            cross = (
                qv.astype(f32) * from_later - pv.astype(f32) * from_earlier
                + qdy.astype(f32) * dot(c, kvl) - pdy.astype(f32) * dot(c, kvr)
            )
            dc = dc + dot_nt(pdy, kvr) + dot_nt(qdy, kvl)
            db = db + dot_nt(qv, cdl) + dot_nt(pv, cdr)
            picks = jnp.concatenate([gather_ref[:, lanes]] * 2, axis=1)
            dl = dl + dot_nt(picks, jnp.concatenate(parts_of(cross, 2), axis=1).astype(bf16))
            u = u_scr[rows, lanes]
            dvu = dvu + dot_nt(picks, jnp.concatenate(parts_of(dv * u, 2), axis=1).astype(bf16))
            skip = pair_row(prm_ref, 11, j)
            du = dv * spread_scr[rows, lanes] + skip * dyj.astype(f32)
            dxpad[pl.ds(pl.multiple_of(2 * EDGE + k * BLOCK, EDGE), BLOCK), lanes] = du * slope_scr[rows, lanes]
        weights = weights.astype(bf16)
        dc = dc + dot(weights, b)
        db = db + dot_tn(weights, c)
        out_rows = pl.ds(pl.multiple_of(2 * EDGE + k * BLOCK, EDGE), BLOCK)
        dbcpad[out_rows, 0:STATE] = db * bs_scr[rows]
        dbcpad[out_rows, STATE : 2 * STATE] = dc * cs_scr[rows]
        dl_scr[k], dvu_scr[k] = dl, dvu
        return carry

    lax.fori_loop(0, NX, block, 0)

    met = right[NX, 0] * left[NX - 1, 1] + right[NX, 1] * left[NX - 1, 0]
    after = -jnp.sum(per_head_sum(gather_ref, met), axis=1, keepdims=True)
    for k in range(NX - 1, -1, -1):
        d_rate = jnp.dot(dl_scr[k], lower, precision=highest, preferred_element_type=f32) + after
        after = d_rate[:, 0:1]
        raw = dth_ref[k] + prm_ref[9]
        d_dt = d_rate * jnp.exp(prm_ref[10]) + dvu_scr[k]
        ddt_ref[k] = d_dt / (1.0 + jnp.exp(-raw))

    pieces = [(k * BLOCK, BLOCK) for k in range(NX)]
    for j in range(LH // 2):
        lanes = slice(128 * j, 128 * (j + 1))
        tap_of = lambda tap, j=j: pair_row(prm_ref, 4 + tap, j)
        for k, (start, size) in enumerate(pieces):
            dx_ref[k, :, lanes] = unconvolved(dxpad, start, size, lanes, tap_of).astype(bf16)
        before = unconvolved(dxpad, -EDGE, EDGE, lanes, tap_of)
        behind = unconvolved(dxpad, CHUNK, EDGE, lanes, tap_of)
        dxp_ref[:, lanes] = jnp.where(z == 0, 0.0, before).astype(bf16)
        dxn_ref[:, lanes] = jnp.where(z == NZ - 1, 0.0, behind).astype(bf16)
    for w in range(2):
        lanes = slice(STATE * w, STATE * (w + 1))
        tap_of = lambda tap, lanes=lanes: taps_ref[tap : tap + 1, lanes]
        for k, (start, size) in enumerate(pieces):
            dbc_ref[k, :, lanes] = unconvolved(dbcpad, start, size, lanes, tap_of).astype(bf16)
        before = unconvolved(dbcpad, -EDGE, EDGE, lanes, tap_of)
        behind = unconvolved(dbcpad, CHUNK, EDGE, lanes, tap_of)
        dbp_ref[:, lanes] = jnp.where(z == 0, 0.0, before).astype(bf16)
        dbn_ref[:, lanes] = jnp.where(z == NZ - 1, 0.0, behind).astype(bf16)


def chunk_gradients(xh, xp, xn, dyh, bch, bp, bn, dth, prm, taps, three, wide, gather, cr, cl):
    shapes = (
        jax.ShapeDtypeStruct((NX, BLOCK, LW), bf16),
        jax.ShapeDtypeStruct((EDGE, LW), bf16),
        jax.ShapeDtypeStruct((EDGE, LW), bf16),
        jax.ShapeDtypeStruct((NX, BLOCK, 2 * STATE), bf16),
        jax.ShapeDtypeStruct((EDGE, 2 * STATE), bf16),
        jax.ShapeDtypeStruct((EDGE, 2 * STATE), bf16),
        jax.ShapeDtypeStruct((NX, LH, BLOCK), f32),
    )
    wide16 = pltpu.VMEM((CHUNK, LW), bf16)
    return pl.pallas_call(
        gradients_kernel,
        out_shape=shapes,
        in_specs=[vmem()] * 15,
        out_specs=tuple(vmem() for _ in shapes),
        scratch_shapes=[
            pltpu.VMEM((CHUNK + 2 * EDGE, LW), f32),
            pltpu.VMEM((CHUNK + 2 * EDGE, 2 * STATE), f32),
            wide16, wide16, wide16, wide16, wide16,
            pltpu.VMEM((CHUNK, STATE), bf16),
            pltpu.VMEM((CHUNK, STATE), bf16),
            pltpu.VMEM((NX, 8, LW), f32),
            pltpu.VMEM((CHUNK, LW), f32),
            pltpu.VMEM((CHUNK, LW), f32),
            pltpu.VMEM((CHUNK, 3 * LW), f32),
            pltpu.VMEM((CHUNK, STATE), f32),
            pltpu.VMEM((CHUNK, STATE), f32),
            pltpu.VMEM((NX, 8, BLOCK), f32),
            pltpu.VMEM((NX + 1, 2, STATE, LW), f32),
            pltpu.VMEM((NX, 2, STATE, LW), f32),
            pltpu.VMEM((CHUNK + 4 * EDGE, LW), f32),
            pltpu.VMEM((CHUNK + 4 * EDGE, 2 * STATE), f32),
            pltpu.VMEM((NX, 8, BLOCK), f32),
            pltpu.VMEM((NX, 8, BLOCK), f32),
        ],
        compiler_params=pltpu.CompilerParams(vmem_limit_bytes=VMEM_LIMIT),
        name="chunk_gradients",
    )(xh, xp, xn, dyh, bch, bp, bn, dth, prm, taps, three, wide, gather, cr, cl)


def exchange_out_kernel(
    dx_ref, dxp_ref, dxn_ref, dbc_ref, dbp_ref, dbn_ref, ddt_ref,
    dxo_ref, exp_ref, exn_ref, bco_ref, ebp_ref, ebn_ref, dto_ref,
    own_sem, xs, xr, bs, br, ts, tr, es, er,
):
    z, x = lax.axis_index("z"), lax.axis_index("x")
    up, down = lax.rem(z + 1, NZ), lax.rem(z + NZ - 1, NZ)
    first, last = x == 0, x == NX - 1

    @pl.when(jnp.logical_not(first))
    def _():
        exp_ref[...] = jnp.zeros_like(exp_ref)
        ebp_ref[...] = jnp.zeros_like(ebp_ref)

    @pl.when(jnp.logical_not(last))
    def _():
        exn_ref[...] = jnp.zeros_like(exn_ref)
        ebn_ref[...] = jnp.zeros_like(ebn_ref)

    barrier = pltpu.get_barrier_semaphore()
    for d in range(1, NX):
        greet(barrier, {"x": lax.rem(x + d, NX)})

    @pl.when(first)
    def _():
        for n in range(NX):
            greet(barrier, {"z": down, "x": jnp.int32(n)})

    @pl.when(last)
    def _():
        for n in range(NX):
            greet(barrier, {"z": up, "x": jnp.int32(n)})

    pl.semaphore_wait(barrier, NX - 1 + 2)

    def to_x(d):
        peer = lax.rem(x + d, NX)
        device = {"x": peer}
        return (
            remote(dbc_ref.at[peer], bco_ref.at[x], bs.at[d - 1], br.at[d - 1], device),
            remote(ddt_ref.at[peer], dto_ref.at[x], ts.at[d - 1], tr.at[d - 1], device),
            remote(dx_ref.at[peer], dxo_ref.at[:, columns(x, LW)], xs.at[d - 1], xr.at[d - 1], device),
        )

    def edges(n):
        before, behind = {"z": down, "x": jnp.int32(NX - 1)}, {"z": up, "x": jnp.int32(0)}
        return (
            remote(dbp_ref, ebn_ref.at[n], es.at[0], er.at[0, n], before),
            remote(dxp_ref, exn_ref.at[:, columns(n, LW)], es.at[1], er.at[1, n], before),
            remote(dbn_ref, ebp_ref.at[n], es.at[2], er.at[2, n], behind),
            remote(dxn_ref, exp_ref.at[:, columns(n, LW)], es.at[3], er.at[3, n], behind),
        )

    for copy in edges(x):
        copy.start()
    for d in range(1, NX):
        for copy in to_x(d):
            copy.start()
    own = [
        pltpu.make_async_copy(dx_ref.at[x], dxo_ref.at[:, columns(x, LW)], own_sem.at[0]),
        pltpu.make_async_copy(dbc_ref.at[x], bco_ref.at[x], own_sem.at[1]),
        pltpu.make_async_copy(ddt_ref.at[x], dto_ref.at[x], own_sem.at[2]),
    ]
    for copy in own:
        copy.start()
    for copy in own:
        copy.wait()
    for d in range(1, NX):
        for copy in to_x(d):
            copy.wait()
    for copy in edges(x):
        copy.wait_send()

    @pl.when(last)
    def _():
        for n in range(NX):
            for copy in edges(n)[:2]:
                copy.wait_recv()

    @pl.when(first)
    def _():
        for n in range(NX):
            for copy in edges(n)[2:]:
                copy.wait_recv()


def exchange_out(dx, dxp, dxn, dbc, dbp, dbn, ddt):
    shapes = (
        jax.ShapeDtypeStruct((BLOCK, INNER), bf16),
        jax.ShapeDtypeStruct((EDGE, INNER), bf16),
        jax.ShapeDtypeStruct((EDGE, INNER), bf16),
        jax.ShapeDtypeStruct((NX, BLOCK, 2 * STATE), bf16),
        jax.ShapeDtypeStruct((NX, EDGE, 2 * STATE), bf16),
        jax.ShapeDtypeStruct((NX, EDGE, 2 * STATE), bf16),
        jax.ShapeDtypeStruct((NX, LH, BLOCK), f32),
    )
    return pl.pallas_call(
        exchange_out_kernel,
        out_shape=shapes,
        in_specs=[vmem()] * 7,
        out_specs=tuple(vmem() for _ in shapes),
        scratch_shapes=[DMA((3,))] + [DMA((3,))] * 6 + [DMA((4,)), DMA((4, NX))],
        compiler_params=pltpu.CompilerParams(
            collective_id=3, has_side_effects=True, vmem_limit_bytes=VMEM_LIMIT
        ),
        name="exchange_out",
    )(dx, dxp, dxn, dbc, dbp, dbn, ddt)


def weight_sum_kernel(
    part_ref, out_ref,
    pair, inr, inl, outr, outl, quarter, piece, xin, zin, held,
    cs, cr, rs, rr, ls, lr, xs, xr, zs, zr, gs, gr, fs, fr,
):
    z, x, y, c = (lax.axis_index(name) for name in ("z", "x", "y", "c"))
    right, left = lax.rem(y + 1, NY), lax.rem(y + NY - 1, NY)
    other = 1 - c
    half = BLOCK // 2
    barrier = pltpu.get_barrier_semaphore()
    for d in range(1, NX):
        greet(barrier, {"x": lax.rem(x + d, NX)})
    for d in range(1, NZ):
        greet(barrier, {"z": lax.rem(z + d, NZ)})
    greet(barrier, {"y": right})
    greet(barrier, {"y": left})
    greet(barrier, {"c": other})
    pl.semaphore_wait(barrier, NX + NZ + 1)

    order = [4, 5, 3, 6, 2, 7, 1, 0]

    def swap(n):
        block = lax.rem(y + order[n], NY)
        return remote(part_ref.at[block, other], pair.at[block], cs.at[n], cr.at[n], {"c": other})

    for n in range(NY):
        swap(n).start()

    def both(block, rows):
        return part_ref[block, c, rows].astype(f32) + pair[block, rows].astype(f32)

    def going_right(s, h):
        rows = pl.ds(h * half, half)
        return remote(outr.at[s, rows], inr.at[s, rows], rs.at[s, h], rr.at[s, h], {"y": right})

    def going_left(s, h):
        rows = pl.ds(h * half, half)
        return remote(outl.at[s, rows], inl.at[s, rows], ls.at[s, h], lr.at[s, h], {"y": left})

    arrived = 0
    for s in range(4):
        need = 2 * s + 2 if s < 3 else 7
        while arrived < need:
            swap(arrived).wait_recv()
            arrived += 1
        for h in range(2):
            rows = pl.ds(h * half, half)
            value = both(lax.rem(y + 4 - s, NY), rows)
            if s > 0:
                going_right(s - 1, h).wait_recv()
                value = value + inr[s - 1, rows].astype(f32)
            outr[s, rows] = value.astype(bf16)
            going_right(s, h).start()
            if s < 3:
                value = both(lax.rem(y + NY - 3 + s, NY), rows)
                if s > 0:
                    going_left(s - 1, h).wait_recv()
                    value = value + inl[s - 1, rows].astype(f32)
                outl[s, rows] = value.astype(bf16)
                going_left(s, h).start()
    swap(7).wait_recv()
    for h in range(2):
        rows = pl.ds(h * half, half)
        value = both(y, rows)
        going_left(2, h).wait_recv()
        value = value + inl[2, rows].astype(f32)
        going_right(3, h).wait_recv()
        quarter[rows] = value + inr[3, rows].astype(f32)

    strip = BLOCK // NX

    def to_x(d):
        peer = lax.rem(x + d, NX)
        return remote(
            quarter.at[columns(peer, strip)], xin.at[d - 1], xs.at[d - 1], xr.at[d - 1], {"x": peer}
        )

    for d in range(1, NX):
        to_x(d).start()
    total = quarter[columns(x, strip)]
    for d in range(1, NX):
        to_x(d).wait_recv()
        total = total + xin[d - 1]
    for i in range(NZ):
        piece[i] = total[8 * (i // 2) : 8 * (i // 2) + 8, 256 * (i % 2) : 256 * (i % 2) + 256]

    def to_z(d):
        peer = lax.rem(z + d, NZ)
        return remote(piece.at[peer], zin.at[d - 1], zs.at[d - 1], zr.at[d - 1], {"z": peer})

    for d in range(1, NZ):
        to_z(d).start()
    value = piece[z]
    for d in range(1, NZ):
        to_z(d).wait_recv()
        value = value + zin[d - 1]
    held[z] = value

    def back_z(d):
        peer = lax.rem(z + d, NZ)
        return remote(held.at[z], held.at[z], gs.at[d - 1], gr.at[d - 1], {"z": peer})

    for d in range(1, NZ):
        back_z(d).start()
    for d in range(1, NZ):
        source = lax.rem(z - d + NZ, NZ)
        remote(held.at[z], held.at[source], gs.at[d - 1], gr.at[d - 1], {"z": source}).wait_recv()
    mine = columns(x, strip)
    rows_out = [
        jnp.concatenate([held[2 * i], held[2 * i + 1]], axis=1) for i in range(NZ // 2)
    ]
    out_ref[mine] = jnp.concatenate(rows_out, axis=0)

    def back_x(d):
        peer = lax.rem(x + d, NX)
        return remote(out_ref.at[mine], out_ref.at[mine], fs.at[d - 1], fr.at[d - 1], {"x": peer})

    for d in range(1, NX):
        back_x(d).start()
    for d in range(1, NX):
        source = lax.rem(x - d + NX, NX)
        theirs = out_ref.at[columns(source, strip)]
        remote(theirs, theirs, fs.at[d - 1], fr.at[d - 1], {"x": source}).wait_recv()
    for d in range(1, NX):
        to_x(d).wait_send()
        back_x(d).wait_send()
    for d in range(1, NZ):
        to_z(d).wait_send()
        back_z(d).wait_send()
    for n in range(NY):
        swap(n).wait_send()
    for h in range(2):
        for s in range(4):
            going_right(s, h).wait_send()
        for s in range(3):
            going_left(s, h).wait_send()


def weight_sum(part):
    width = part.shape[-1]
    strip = BLOCK // NX
    block16 = lambda n: pltpu.VMEM((n, BLOCK, width), bf16)
    return pl.pallas_call(
        weight_sum_kernel,
        out_shape=jax.ShapeDtypeStruct((BLOCK, width), f32),
        in_specs=[vmem()],
        out_specs=vmem(),
        scratch_shapes=[
            block16(NY), block16(4), block16(3), block16(4), block16(3),
            pltpu.VMEM((BLOCK, width), f32),
            pltpu.VMEM((NZ, 8, 256), f32),
            pltpu.VMEM((NX - 1, strip, width), f32),
            pltpu.VMEM((NZ - 1, 8, 256), f32),
            pltpu.VMEM((NZ, 8, 256), f32),
            DMA((8,)), DMA((8,)), DMA((4, 2)), DMA((4, 2)), DMA((3, 2)), DMA((3, 2)),
            DMA((3,)), DMA((3,)), DMA((7,)), DMA((7,)), DMA((7,)), DMA((7,)), DMA((3,)), DMA((3,)),
        ],
        compiler_params=pltpu.CompilerParams(
            collective_id=4, has_side_effects=True, vmem_limit_bytes=VMEM_LIMIT
        ),
        name="weight_sum",
    )(part)


def interleaved(first, second):
    return jnp.concatenate(
        [first[..., :STATE], second[..., :STATE], first[..., STATE:], second[..., STATE:]], axis=-1
    )


def local(
    layer_activity, writer_matrix, reader_matrix, source_unfiltered, switch_raw_signal, saved_result,
    final_adjoint, delta_raw, extra_logdrop, source_filter_coefs, writer_filter_coefs, reader_filter_coefs,
    delta_offset, fading_exponents, direct_factor, rescale_factor,
):
    tokens = layer_activity.shape[1]
    rows = layer_activity.reshape(tokens, -1)
    dy, d_gate = norm_backward(
        saved_result.reshape(tokens, INNER),
        switch_raw_signal.reshape(tokens, INNER),
        final_adjoint.reshape(tokens, INNER),
        rescale_factor.reshape(1, INNER),
    )
    shard = interleaved(writer_matrix, reader_matrix)
    taps = jnp.concatenate([source_filter_coefs, source_filter_coefs], axis=1)
    scalars = jnp.broadcast_to(
        jnp.concatenate([delta_offset, fading_exponents, direct_factor])[:, None], (3, BLOCK)
    )
    params = jnp.concatenate([taps, scalars, jnp.zeros((4, BLOCK), f32)], axis=0)
    drops = extra_logdrop.reshape(NZ, NX, BLOCK)
    message = jnp.concatenate([drops, jnp.broadcast_to(params[None], (NZ, 12, BLOCK))], axis=1)
    delta = delta_raw.reshape(tokens, HEADS).T.astype(f32)
    weights, xh, dyh, dth, prm, xp, xn = exchange_in(
        shard, source_unfiltered.reshape(tokens, INNER), dy, delta, message
    )
    weights = weights.reshape(-1, shard.shape[1])
    projected = jnp.dot(rows, weights, preferred_element_type=f32).astype(bf16)
    bch, bp, bn = maps_in(projected)
    prm = jnp.transpose(prm, (1, 0, 2))
    group = lax.axis_index("x") // 2
    all_taps = interleaved(writer_filter_coefs, reader_filter_coefs)
    map_taps = jnp.where(group == 0, all_taps[:, : 2 * STATE], all_taps[:, 2 * STATE :])
    three, wide, gather = spreaders()
    base = (xh, xp, xn, dyh, bch, bp, bn, dth, prm, map_taps, three)
    sr, sl, decay = chunk_states(*base)
    cr, cl = scan_states(sr, sl, decay)
    grads = chunk_gradients(*base, wide, gather, cr, cl)
    dx, exp, exn, bco, ebp, ebn, ddt = exchange_out(*grads)

    gap = tokens - 2 * EDGE
    edge = jnp.concatenate([exp, jnp.zeros((gap, INNER), bf16), exn], axis=0)
    d_x = (dx.astype(f32) + edge.astype(f32)).astype(bf16)
    maps = bco.astype(f32) + jnp.concatenate(
        [ebp.astype(f32), jnp.zeros((NX, gap, 2 * STATE), f32), ebn.astype(f32)], axis=1
    )
    d_maps = jnp.concatenate([maps[0] + maps[1], maps[2] + maps[3]], axis=1).astype(bf16)
    d_hidden = lax.dot_general(
        d_maps, weights, (((1,), (1,)), ((), ())), preferred_element_type=f32
    ).astype(bf16)
    part = lax.dot_general(
        rows, d_maps, (((0,), (0,)), ((), ())), preferred_element_type=f32
    ).astype(bf16)
    total = weight_sum(part.reshape(NY, NC, BLOCK, -1))
    d_dt = ddt.reshape(HEADS, tokens).T.astype(bf16)
    return (
        d_hidden.reshape(1, tokens, -1),
        d_x.reshape(1, tokens, INNER),
        d_gate.reshape(1, tokens, INNER),
        d_dt.reshape(1, tokens, HEADS),
        jnp.concatenate([total[:, :STATE], total[:, 2 * STATE : 3 * STATE]], axis=1),
        jnp.concatenate([total[:, STATE : 2 * STATE], total[:, 3 * STATE :]], axis=1),
    )


def solution(mesh):
    split = Mesh(mesh.devices.reshape(NZ, NX, NY, NC), ("z", "x", "y", "c"))
    sp, dp = ("z", "x"), ("y", "c")
    in_specs = (
        P(dp, sp, None),
        P(dp, None),
        P(dp, None),
        P(dp, sp, None),
        P(dp, sp, None),
        P(dp, sp, None),
        P(dp, sp, None),
        P(dp, sp, None),
        P(dp, None, sp),
        P(None, sp),
        P(),
        P(),
        P(sp),
        P(sp),
        P(sp),
        P(),
    )
    out_specs = (
        P(dp, sp, None),
        P(dp, sp, None),
        P(dp, sp, None),
        P(dp, sp, None),
        P(dp, None),
        P(dp, None),
    )
    return jax.shard_map(local, mesh=split, in_specs=in_specs, out_specs=out_specs, check_vma=False)
```

```python
import functools

import jax
import jax.numpy as jnp
from jax import lax
from jax.experimental import pallas as pl
from jax.experimental.pallas import tpu as pltpu
from jax.sharding import Mesh
from jax.sharding import PartitionSpec as P

HEADS = 32
HEAD_DIM = 64
STATE = 128
GROUPS = 2
NORM_GROUPS = 8
CONV_K = 5
BLOCK = 128
INNER = 2048
NZ, NX, NY, NC = 8, 4, 8, 2
LH = HEADS // NX
LW = LH * HEAD_DIM
CHUNK = NX * BLOCK
EDGE = 16
EPSILON = 1e-06
VMEM_LIMIT = 60 * 1024 * 1024

f32 = jnp.float32
bf16 = jnp.bfloat16
highest = lax.Precision.HIGHEST
MESH = pl.DeviceIdType.MESH
DMA = pltpu.SemaphoreType.DMA


def vmem():
    return pl.BlockSpec(memory_space=pltpu.VMEM)


def remote(src, dst, send, recv, device):
    return pltpu.make_async_remote_copy(
        src_ref=src, dst_ref=dst, send_sem=send, recv_sem=recv, device_id=device, device_id_type=MESH
    )


def greet(barrier, device):
    pl.semaphore_signal(barrier, inc=1, device_id=device, device_id_type=MESH)


def columns(start, size):
    return pl.ds(pl.multiple_of(start * size, size), size)


def dot(a, b):
    return jnp.dot(a, b, preferred_element_type=f32)


def dot_nt(a, b):
    return lax.dot_general(a, b, (((1,), (1,)), ((), ())), preferred_element_type=f32)


def dot_tn(a, b):
    return lax.dot_general(a, b, (((0,), (0,)), ((), ())), preferred_element_type=f32)


def iota2(shape, dim):
    return lax.broadcasted_iota(jnp.int32, shape, dim)


def parts_of(value, count):
    out = []
    for _ in range(count):
        top = value.astype(bf16).astype(f32)
        out.append(top)
        value = value - top
    return out


def silu_parts(pre):
    gate = 1.0 / (1.0 + jnp.exp(-pre))
    return pre * gate, gate * (1.0 + pre * (1.0 - gate))


def norm_group(group, saved_ref, switch_ref, final_ref, gain_ref, dy_ref, dgate_ref):
    width = INNER // NORM_GROUPS
    cols = slice(group * width, (group + 1) * width)
    saved = saved_ref[:, cols].astype(f32)
    switch = switch_ref[:, cols].astype(f32)
    final = final_ref[:, cols].astype(f32)
    gate = 1.0 / (1.0 + jnp.exp(-switch))
    act = switch * gate
    mixed = saved * act
    scale = lax.rsqrt(jnp.mean(mixed * mixed, axis=-1, keepdims=True) + EPSILON)
    d_normed = final * gain_ref[:, cols]
    inner = jnp.mean(d_normed * mixed, axis=-1, keepdims=True)
    d_mixed = d_normed * scale - mixed * (scale * scale * scale * inner)
    dy_ref[:, cols] = (d_mixed * act).astype(bf16)
    slope = gate * (1.0 + switch * (1.0 - gate))
    dgate_ref[:, cols] = (d_mixed * saved * slope).astype(bf16)


def pair_row(prm_ref, row, j):
    lane = iota2((1, 128), 1)
    return jnp.where(lane < HEAD_DIM, prm_ref[2 * j, row : row + 1, :], prm_ref[2 * j + 1, row : row + 1, :])


def fill_padded(pad_ref, body_ref, prev_ref, next_ref, z):
    pad_ref[pl.ds(0, EDGE)] = jnp.where(z == 0, 0.0, prev_ref[...].astype(f32))
    for k in range(NX):
        pad_ref[pl.ds(EDGE + k * BLOCK, BLOCK)] = body_ref[k].astype(f32)
    pad_ref[pl.ds(EDGE + CHUNK, EDGE)] = jnp.where(z == NZ - 1, 0.0, next_ref[...].astype(f32))


def unconvolved(pad_ref, start, size, lanes, tap_of):
    total = jnp.zeros((size, 128), f32)
    for tap in range(CONV_K):
        total = total + tap_of(tap) * pad_ref[pl.ds(start + 2 * EDGE + 2 - tap, size), lanes]
    return total


BUFFERS = dict(
    dy=((BLOCK, INNER), bf16),
    xh=((NX, BLOCK, LW), bf16),
    dyh=((NX, BLOCK, LW), bf16),
    dth=((NX, LH, BLOCK), f32),
    prm=((LH, 16, BLOCK), f32),
    xp=((EDGE, LW), bf16),
    xn=((EDGE, LW), bf16),
    wf=((NY * NC, BLOCK, 2 * GROUPS * STATE), bf16),
    bc=((BLOCK, 2 * GROUPS * STATE), bf16),
    bch=((NX, BLOCK, 2 * STATE), bf16),
    bp=((EDGE, 2 * STATE), bf16),
    bn=((EDGE, 2 * STATE), bf16),
    three=((48, 3 * LW), bf16),
    wide=((24, LH * BLOCK), bf16),
    gather=((LH, LW), bf16),
    xpad=((CHUNK + 2 * EDGE, LW), f32),
    bcpad=((CHUNK + 2 * EDGE, 2 * STATE), f32),
    v16=((CHUNK, LW), bf16),
    pv16=((CHUNK, LW), bf16),
    qv16=((CHUNK, LW), bf16),
    pdy16=((CHUNK, LW), bf16),
    qdy16=((CHUNK, LW), bf16),
    b16=((CHUNK, STATE), bf16),
    c16=((CHUNK, STATE), bf16),
    u=((CHUNK, LW), f32),
    slope=((CHUNK, LW), f32),
    spread=((CHUNK, 3 * LW), f32),
    bs=((CHUNK, STATE), f32),
    cs=((CHUNK, STATE), f32),
    level=((NX, LH, BLOCK), f32),
    gamma=((NX, 8, LW), f32),
    signed=((NX, BLOCK, BLOCK), f32),
    grid_t=((NX, BLOCK, BLOCK), f32),
    weights=((NX, BLOCK, BLOCK), f32),
    right=((NX + 1, 2, STATE, LW), f32),
    left=((NX, 2, STATE, LW), f32),
    sr=((2, STATE, LW), f32),
    sl=((2, STATE, LW), f32),
    decay=((8, LW), f32),
    outr=((2, STATE, LW), bf16),
    outl=((2, STATE, LW), bf16),
    cr=((2, STATE, LW), bf16),
    cl=((2, STATE, LW), bf16),
    dv=((CHUNK, LW), f32),
    dl=((NX, LH, BLOCK), f32),
    dvu=((NX, LH, BLOCK), f32),
    dxpad=((CHUNK + 4 * EDGE, LW), f32),
    dbcpad=((CHUNK + 4 * EDGE, 2 * STATE), f32),
    dx=((NX, BLOCK, LW), bf16),
    dxp=((EDGE, LW), bf16),
    dxn=((EDGE, LW), bf16),
    dbc=((NX, BLOCK, 2 * STATE), bf16),
    dbp=((EDGE, 2 * STATE), bf16),
    dbn=((EDGE, 2 * STATE), bf16),
    ddt=((NX, LH, BLOCK), f32),
    dto=((NX, LH, BLOCK), f32),
    exp=((EDGE, INNER), bf16),
    exn=((EDGE, INNER), bf16),
    bco=((NX, BLOCK, 2 * STATE), bf16),
    ebp=((NX, EDGE, 2 * STATE), bf16),
    ebn=((NX, EDGE, 2 * STATE), bf16),
    dmaps=((BLOCK, 2 * GROUPS * STATE), bf16),
    part=((NY, BLOCK, 2 * GROUPS * STATE), bf16),
    kept=((NY, BLOCK, 2 * GROUPS * STATE), f32),
    pair=((NY, BLOCK, 2 * GROUPS * STATE), bf16),
    inr=((4, BLOCK, 2 * GROUPS * STATE), bf16),
    inl=((4, BLOCK, 2 * GROUPS * STATE), bf16),
    outwr=((4, BLOCK, 2 * GROUPS * STATE), bf16),
    outwl=((4, BLOCK, 2 * GROUPS * STATE), bf16),
    quarter=((BLOCK, 2 * GROUPS * STATE), f32),
    piece=((NZ, 8, 256), f32),
    xin=((NX - 1, BLOCK // NX, 2 * GROUPS * STATE), f32),
    zin=((NZ - 1, 8, 256), f32),
    held=((NZ, 8, 256), f32),
)
PIECES = 16
SEMAPHORES = dict(
    own=(12,), x_s=(3,), x_r=(3,), y_s=(3,), y_r=(3,), t_s=(3,), t_r=(3,), m_s=(8,), m_r=(8,),
    h_s=(4,), h_r=(4,), wr_s=(4, 2), wr_r=(4, 2), wl_s=(4, 2), wl_r=(4, 2), wp_s=(8, 2), wp_r=(8, 2),
    b_s=(3,), b_r=(3,), up_s=(PIECES,), up_r=(PIECES,), dn_s=(PIECES,), dn_r=(PIECES,),
    ox_s=(3,), ox_r=(3,), ob_s=(3,), ob_r=(3,), ot_s=(3,), ot_r=(3,), e_s=(4,), e_r=(4, NX),
    sw_s=(8,), sw_r=(8,), rr_s=(4, 2), rr_r=(4, 2), rl_s=(4, 2), rl_r=(4, 2),
    qx_s=(3,), qx_r=(3,), qz_s=(7,), qz_r=(7,), gz_s=(7,), gz_r=(7,), gx_s=(3,), gx_r=(3,),
)


class Named:
    def __init__(self, names, refs):
        for name, ref in zip(names, refs, strict=True):
            setattr(self, name, ref)


INPUTS = ("w", "act", "x", "switch", "saved", "final", "gain", "dt", "msg", "taps")
OUTPUTS = ("dgate", "dxo", "dhid", "dts", "total")


def kernel(*refs):
    n_in, n_out, n_buf = len(INPUTS), len(OUTPUTS), len(BUFFERS)
    a = Named(INPUTS, refs[:n_in])
    o = Named(OUTPUTS, refs[n_in : n_in + n_out])
    s = Named(BUFFERS, refs[n_in + n_out : n_in + n_out + n_buf])
    m = Named(SEMAPHORES, refs[n_in + n_out + n_buf :])
    z, x, y, c = (lax.axis_index(name) for name in ("z", "x", "y", "c"))
    half = BLOCK // 2
    up, down = lax.rem(z + 1, NZ), lax.rem(z + NZ - 1, NZ)
    north, south = lax.rem(y + 1, NY), lax.rem(y + NY - 1, NY)
    other = 1 - c
    head = z * NX + x
    dest = z // 2
    slot = lax.rem(head, LH)
    mine = dest == x
    first, last = z == 0, z == NZ - 1
    x_first, x_last = x == 0, x == NX - 1

    def when(condition):
        return pl.when(condition)

    def unless(condition):
        return pl.when(jnp.logical_not(condition))

    def sender_of(i):
        return 2 * x + i // NX, i % NX

    def is_me(i):
        sz, sx = sender_of(i)
        return jnp.logical_and(sz == z, sx == x)

    @when(first)
    def _():
        s.cr[...] = jnp.zeros_like(s.cr)

    @when(last)
    def _():
        s.cl[...] = jnp.zeros_like(s.cl)

    @unless(x_first)
    def _():
        s.exp[...] = jnp.zeros_like(s.exp)
        s.ebp[...] = jnp.zeros_like(s.ebp)

    @unless(x_last)
    def _():
        s.exn[...] = jnp.zeros_like(s.exn)
        s.ebn[...] = jnp.zeros_like(s.ebn)

    barrier = pltpu.get_barrier_semaphore()
    for d in range(1, NX):
        greet(barrier, {"x": lax.rem(x + d, NX)})
    for d in range(1, NZ):
        greet(barrier, {"z": lax.rem(z + d, NZ)})
    greet(barrier, {"y": north})
    greet(barrier, {"y": south})
    greet(barrier, {"c": other})
    for i in range(LH):

        @unless(is_me(i))
        def _():
            sz, sx = sender_of(i)
            greet(barrier, {"z": sz, "x": sx})

    @when(x_first)
    def _():
        for n in range(NX):
            greet(barrier, {"z": down, "x": jnp.int32(n)})

    @when(x_last)
    def _():
        for n in range(NX):
            greet(barrier, {"z": up, "x": jnp.int32(n)})

    pl.semaphore_wait(barrier, NX - 1 + NZ - 1 + 3 + NZ - mine.astype(jnp.int32) + 2)

    def rows(h):
        return pl.ds(h * half, half)

    def w_ring(step, h, way):
        block = lax.rem(y - way * step + NY, NY) * NC + c
        src = a.w.at[rows(h)] if step == 0 else s.wf.at[block, rows(h)]
        send, recv, to = (m.wr_s, m.wr_r, north) if way > 0 else (m.wl_s, m.wl_r, south)
        return remote(src, s.wf.at[block, rows(h)], send.at[step, h], recv.at[step, h], {"y": to})

    def w_offset(n):
        return 0 if n == 0 else (-n if n < 5 else n - 4)

    def w_across(n, h):
        block = lax.rem(y + w_offset(n) + NY, NY) * NC + c
        src = a.w.at[rows(h)] if n == 0 else s.wf.at[block, rows(h)]
        return remote(src, s.wf.at[block, rows(h)], m.wp_s.at[n, h], m.wp_r.at[n, h], {"c": other})

    w_steps = [(step, h, way) for step in range(3) for h in range(2) for way in (1, -1)]
    w_steps += [(3, 0, 1), (3, 1, -1)]
    for step, h, way in w_steps[:4]:
        w_ring(step, h, way).start()
    own = [
        pltpu.make_async_copy(a.w, s.wf.at[y * NC + c], m.own.at[0]),
        pltpu.make_async_copy(a.x.at[:, columns(x, LW)], s.xh.at[x], m.own.at[1]),
        pltpu.make_async_copy(a.dt.at[columns(x, LH)], s.dth.at[x], m.own.at[2]),
    ]
    for copy in own:
        copy.start()
    for h in range(2):
        w_across(0, h).start()

    def x_to(d):
        peer = lax.rem(x + d, NX)
        return remote(
            a.x.at[:, columns(peer, LW)], s.xh.at[x], m.x_s.at[d - 1], m.x_r.at[d - 1], {"x": peer}
        )

    def dt_to(d):
        peer = lax.rem(x + d, NX)
        return remote(
            a.dt.at[columns(peer, LH)], s.dth.at[x], m.t_s.at[d - 1], m.t_r.at[d - 1], {"x": peer}
        )

    def dy_to(d):
        peer = lax.rem(x + d, NX)
        return remote(
            s.dy.at[:, columns(peer, LW)], s.dyh.at[x], m.y_s.at[d - 1], m.y_r.at[d - 1], {"x": peer}
        )

    def message(i):
        return remote(
            a.msg.at[i], s.prm.at[slot], m.m_s.at[i], m.m_r.at[slot], {"z": jnp.int32(i), "x": dest}
        )

    for d in range(1, NX):
        x_to(d).start()
        dt_to(d).start()
    keep = pltpu.make_async_copy(a.msg.at[z], s.prm.at[slot], m.own.at[3])
    for i in range(NZ):

        @unless(jnp.logical_and(mine, z == i))
        def _():
            message(i).start()

    @when(mine)
    def _():
        keep.start()

    for group in range(NORM_GROUPS):
        norm_group(group, a.saved, a.switch, a.final, a.gain, s.dy, o.dgate)
    for d in range(1, NX):
        dy_to(d).start()
    own_dy = pltpu.make_async_copy(s.dy.at[:, columns(x, LW)], s.dyh.at[x], m.own.at[4])
    own_dy.start()

    def projected(n, core):
        block = lax.rem(y + w_offset(n) + NY, NY) * NC + core
        return dot(a.act[:, columns(block, BLOCK)], s.wf[block])

    own[0].wait()
    maps = projected(0, c)
    for step in range(4):
        for h in range(2):
            for way in (1, -1):
                if step == 3 and (h == 0) != (way == 1):
                    continue
                w_ring(step, h, way).wait_recv()
                following = (step + 1, h, way)
                if following in w_steps:
                    w_ring(*following).start()
                w_across(1 + step if way == 1 or step == 3 else 5 + step, h).start()
        maps = maps + projected(1 + step, c)
        if step < 3:
            maps = maps + projected(5 + step, c)
        for n in ((0,), (1, 5), (2, 6), (3, 7))[step]:
            for h in range(2):
                w_across(n, h).wait_recv()
            maps = maps + projected(n, other)
    for h in range(2):
        w_across(4, h).wait_recv()
    maps = maps + projected(4, other)
    s.bc[...] = maps.astype(bf16)

    def bc_to(d):
        peer = lax.rem(x + d, NX)
        return remote(
            s.bc.at[:, columns(peer // 2, 2 * STATE)], s.bch.at[x], m.b_s.at[d - 1], m.b_r.at[d - 1], {"x": peer}
        )

    for d in range(1, NX):
        bc_to(d).start()
    own_bc = pltpu.make_async_copy(s.bc.at[:, columns(x // 2, 2 * STATE)], s.bch.at[x], m.own.at[5])
    own_bc.start()

    for d in range(1, NX):
        x_to(d).wait_recv()
    own[1].wait()
    tail_rows, head_rows = pl.ds(BLOCK - EDGE, EDGE), pl.ds(0, EDGE)
    edges_in = [
        remote(s.xh.at[NX - 1, tail_rows], s.xp, m.h_s.at[0], m.h_r.at[0], {"z": up}),
        remote(s.xh.at[0, head_rows], s.xn, m.h_s.at[1], m.h_r.at[1], {"z": down}),
        remote(s.bch.at[NX - 1, tail_rows], s.bp, m.h_s.at[2], m.h_r.at[2], {"z": up}),
        remote(s.bch.at[0, head_rows], s.bn, m.h_s.at[3], m.h_r.at[3], {"z": down}),
    ]
    edges_in[0].start()
    edges_in[1].start()

    r, cc = iota2((48, 3 * LW), 0), iota2((48, 3 * LW), 1)
    s.three[...] = jnp.logical_and(
        r // 16 == cc // LW, jnp.bitwise_and(r, 7) == jnp.bitwise_and(cc, LW - 1) // HEAD_DIM
    ).astype(bf16)
    r, cc = iota2((24, LH * BLOCK), 0), iota2((24, LH * BLOCK), 1)
    s.wide[...] = (jnp.bitwise_and(r, 7) == cc // BLOCK).astype(bf16)
    s.gather[...] = (iota2((LH, LW), 1) // HEAD_DIM == iota2((LH, LW), 0)).astype(bf16)
    for pad in (s.dxpad, s.dbcpad):
        pad[pl.ds(0, 2 * EDGE)] = jnp.zeros((2 * EDGE, pad.shape[1]), f32)
        pad[pl.ds(2 * EDGE + CHUNK, 2 * EDGE)] = jnp.zeros((2 * EDGE, pad.shape[1]), f32)

    for d in range(1, NX):
        dt_to(d).wait_recv()
        dy_to(d).wait_recv()
    own[2].wait()
    own_dy.wait()
    for i in range(LH):

        @unless(is_me(i))
        def _():
            sz, sx = sender_of(i)
            remote(a.msg.at[i], s.prm.at[i], m.m_s.at[i], m.m_r.at[i], {"z": sz, "x": sx}).wait_recv()

    @when(mine)
    def _():
        keep.wait()

    row, col = iota2((BLOCK, BLOCK), 0), iota2((BLOCK, BLOCK), 1)
    upper = (row <= col).astype(f32)
    lower = (row >= col).astype(f32)
    sign = (row > col).astype(f32) - (row < col).astype(f32)
    low_half = iota2((BLOCK, 128), 1) < HEAD_DIM
    head_row = iota2((8, BLOCK), 0)

    edges_in[0].wait()
    edges_in[1].wait()
    fill_padded(s.xpad, s.xh, s.xp, s.xn, z)
    for k in range(NX):
        at = pl.ds(k * BLOCK, BLOCK)
        dt = jax.nn.softplus(s.dth[k] + s.prm[:, 9, :])
        rate = dt * jnp.exp(s.prm[:, 10, :]) + s.prm[:, k, :]
        level = jnp.dot(rate, upper, precision=highest, preferred_element_type=f32)
        total = level[:, BLOCK - 1 : BLOCK]
        s.level[k] = level
        stack = jnp.concatenate(
            parts_of(dt, 2) + parts_of(jnp.exp(-level), 2) + parts_of(jnp.exp(level - total), 2), axis=0
        )
        spread = dot_tn(stack.astype(bf16), s.three[...])
        s.spread[at] = spread
        s.gamma[k] = jnp.broadcast_to(spread[BLOCK - 1 : BLOCK, LW : 2 * LW], (8, LW))
        for j in range(LH // 2):
            lanes = slice(128 * j, 128 * (j + 1))
            pre = jnp.zeros((BLOCK, 128), f32)
            for tap in range(CONV_K):
                pre = pre + pair_row(s.prm, 4 + tap, j) * s.xpad[pl.ds(k * BLOCK + EDGE - 2 + tap, BLOCK), lanes]
            u, slope = silu_parts(pre)
            s.u[at, lanes], s.slope[at, lanes] = u, slope
            pe = spread[:, LW + 128 * j : LW + 128 * (j + 1)]
            qe = spread[:, 2 * LW + 128 * j : 2 * LW + 128 * (j + 1)]
            v = u * spread[:, lanes]
            dy = s.dyh[k, :, lanes].astype(f32)
            s.v16[at, lanes] = v.astype(bf16)
            s.pv16[at, lanes], s.qv16[at, lanes] = (pe * v).astype(bf16), (qe * v).astype(bf16)
            s.pdy16[at, lanes], s.qdy16[at, lanes] = (pe * dy).astype(bf16), (qe * dy).astype(bf16)

    own_bc.wait()
    for d in range(1, NX):
        bc_to(d).wait_recv()
    edges_in[2].start()
    edges_in[3].start()
    edges_in[2].wait()
    edges_in[3].wait()
    fill_padded(s.bcpad, s.bch, s.bp, s.bn, z)
    s.decay[...] = jnp.ones_like(s.decay)
    for k in range(NX):
        at = pl.ds(k * BLOCK, BLOCK)
        for which, held, slopes in ((0, s.b16, s.bs), (1, s.c16, s.cs)):
            lanes = slice(which * STATE, (which + 1) * STATE)
            pre = jnp.zeros((BLOCK, STATE), f32)
            for tap in range(CONV_K):
                pre = pre + a.taps[tap : tap + 1, lanes] * s.bcpad[pl.ds(k * BLOCK + EDGE - 2 + tap, BLOCK), lanes]
            value, slopes[at] = silu_parts(pre)
            held[at] = value.astype(bf16)
        b, cc = s.b16[at], s.c16[at]
        kvr, cdr = dot_tn(b, s.qv16[at]), dot_tn(cc, s.qdy16[at])
        kvl, cdl = dot_tn(b, s.pv16[at]), dot_tn(cc, s.pdy16[at])
        s.right[k + 1, 0], s.right[k + 1, 1] = kvr, cdr
        if k > 0:
            s.left[k - 1, 0], s.left[k - 1, 1] = kvl, cdl
        if k == 0:
            s.sr[0], s.sr[1], s.sl[0], s.sl[1] = kvr, cdr, kvl, cdl
        else:
            g, before = s.gamma[k, 0:1], s.decay[0:1]
            s.sr[0] = s.sr[0] * g + kvr
            s.sr[1] = s.sr[1] * g + cdr
            s.sl[0] = s.sl[0] + before * kvl
            s.sl[1] = s.sl[1] + before * cdl
        s.decay[...] = s.decay[...] * s.gamma[k]

    def piece(n):
        return n // 8, pl.ds(pl.multiple_of(lax.rem(n // 4, 2) * 64, 64), 64), columns(lax.rem(n, 4), 128)

    def going_up(n):
        return remote(s.outr.at[piece(n)], s.cr.at[piece(n)], m.up_s.at[n], m.up_r.at[n], {"z": up})

    def going_down(n):
        return remote(s.outl.at[piece(n)], s.cl.at[piece(n)], m.dn_s.at[n], m.dn_r.at[n], {"z": down})

    def scan_step(t):
        n = t - z

        @when(jnp.logical_and(n >= 0, n < PIECES))
        def _():
            @unless(first)
            def _():
                going_up(n).wait_recv()

            @unless(last)
            def _():
                at = piece(n)
                s.outr[at] = (s.cr[at].astype(f32) * s.decay[0:1, at[2]] + s.sr[at]).astype(bf16)
                going_up(n).start()

        i = t - (NZ - 1 - z)

        @when(jnp.logical_and(i >= 0, i < PIECES))
        def _():
            @unless(last)
            def _():
                going_down(i).wait_recv()

            @unless(first)
            def _():
                at = piece(i)
                s.outl[at] = (s.cl[at].astype(f32) * s.decay[0:1, at[2]] + s.sl[at]).astype(bf16)
                going_down(i).start()

    def within(k, j):
        at = pl.ds(pl.multiple_of(k * BLOCK, BLOCK), BLOCK)
        lanes = columns(j, 128)
        parts = jnp.concatenate(parts_of(s.level[k], 3), axis=0).astype(bf16)
        level_cols = dot_tn(parts, s.wide[:, columns(j, 256)])
        vj, dyj = s.v16[at, lanes], s.dyh[k, :, lanes]
        signed, grid_t = s.signed[k], s.grid_t[k]
        halves = []
        weights = s.weights[k]
        dl = s.dl[k]
        for i in range(2):
            h = 2 * j + i
            near = jnp.exp(-jnp.abs(level_cols[:, 128 * i : 128 * (i + 1)] - s.level[k, pl.ds(h, 1), :]))
            keep_half = low_half if i == 0 else jnp.logical_not(low_half)
            shared = dot_nt(jnp.where(keep_half, dyj, jnp.zeros_like(dyj)), vj) * near
            weights = weights + shared
            crossing = (shared * signed).astype(bf16)
            pick = (head_row == h).astype(bf16)
            dl = dl + dot(pick, crossing) - dot_nt(pick, crossing)
            halves.append(dot((grid_t * near).astype(bf16), dyj))
        s.weights[k] = weights
        s.dl[k] = dl
        s.dv[at, lanes] = jnp.where(low_half, halves[0], halves[1])

    s.weights[...] = jnp.zeros_like(s.weights)
    s.dl[...] = jnp.zeros_like(s.dl)
    for t in range(2):
        scan_step(jnp.int32(t))
    for k in range(NX):
        at = pl.ds(k * BLOCK, BLOCK)
        b, cc = s.b16[at], s.c16[at]
        s.signed[k] = dot_nt(cc, b) * sign
        s.grid_t[k] = dot_nt(b, cc)

    def steps(t, carry):
        scan_step(t + 2)

        @when(t < NX * LH // 2)
        def _():
            within(t // (LH // 2), lax.rem(t, LH // 2))

        return carry

    lax.fori_loop(0, NZ - 1 + PIECES - 2, steps, 0)

    s.right[0, 0], s.right[0, 1] = s.cr[0].astype(f32), s.cr[1].astype(f32)
    s.left[NX - 1, 0], s.left[NX - 1, 1] = s.cl[0].astype(f32), s.cl[1].astype(f32)
    for k in range(NX):
        g = s.gamma[k, 0:1]
        s.right[k + 1, 0] = s.right[k + 1, 0] + s.right[k, 0] * g
        s.right[k + 1, 1] = s.right[k + 1, 1] + s.right[k, 1] * g
    for k in range(NX - 2, -1, -1):
        g = s.gamma[k + 1, 0:1]
        s.left[k, 0] = s.left[k, 0] + g * s.left[k + 1, 0]
        s.left[k, 1] = s.left[k, 1] + g * s.left[k + 1, 1]

    def through(k, carry):
        at = pl.ds(pl.multiple_of(k * BLOCK, BLOCK), BLOCK)
        padded = pl.ds(pl.multiple_of(2 * EDGE + k * BLOCK, EDGE), BLOCK)
        b, cc = s.b16[at], s.c16[at]
        weights = s.weights[k].astype(bf16)
        dc = dot(weights, b)
        db = dot_tn(weights, cc)
        dl = s.dl[k]
        dvu = jnp.zeros((8, BLOCK), f32)
        for j in range(LH // 2):
            lanes = slice(128 * j, 128 * (j + 1))
            kvr, cdr = s.right[k, 0, :, lanes].astype(bf16), s.right[k, 1, :, lanes].astype(bf16)
            kvl, cdl = s.left[k, 0, :, lanes].astype(bf16), s.left[k, 1, :, lanes].astype(bf16)
            pe = s.spread[at, LW + 128 * j : LW + 128 * (j + 1)]
            qe = s.spread[at, 2 * LW + 128 * j : 2 * LW + 128 * (j + 1)]
            from_later, from_earlier = dot(b, cdl), dot(b, cdr)
            pv, qv, pdy, qdy = s.pv16[at, lanes], s.qv16[at, lanes], s.pdy16[at, lanes], s.qdy16[at, lanes]
            dv = s.dv[at, lanes] + qe * from_later + pe * from_earlier
            cross = (
                qv.astype(f32) * from_later - pv.astype(f32) * from_earlier
                + qdy.astype(f32) * dot(cc, kvl) - pdy.astype(f32) * dot(cc, kvr)
            )
            dc = dc + dot_nt(pdy, kvr) + dot_nt(qdy, kvl)
            db = db + dot_nt(qv, cdl) + dot_nt(pv, cdr)
            picks = jnp.concatenate([s.gather[:, lanes]] * 2, axis=1)
            dl = dl + dot_nt(picks, jnp.concatenate(parts_of(cross, 2), axis=1).astype(bf16))
            dvu = dvu + dot_nt(picks, jnp.concatenate(parts_of(dv * s.u[at, lanes], 2), axis=1).astype(bf16))
            du = dv * s.spread[at, lanes] + pair_row(s.prm, 11, j) * s.dyh[k, :, lanes].astype(f32)
            s.dxpad[padded, lanes] = du * s.slope[at, lanes]
        s.dbcpad[padded, 0:STATE] = db * s.bs[at]
        s.dbcpad[padded, STATE : 2 * STATE] = dc * s.cs[at]
        s.dl[k], s.dvu[k] = dl, dvu
        return carry

    lax.fori_loop(0, NX, through, 0)

    def masked_edges(pad, width, tap_for, before_ref, behind_ref):
        for w in range(width // 128):
            lanes = slice(128 * w, 128 * (w + 1))
            before = unconvolved(pad, -EDGE, EDGE, lanes, tap_for(w))
            behind = unconvolved(pad, CHUNK, EDGE, lanes, tap_for(w))
            before_ref[:, lanes] = jnp.where(first, 0.0, before).astype(bf16)
            behind_ref[:, lanes] = jnp.where(last, 0.0, behind).astype(bf16)

    def map_tap(w):
        return lambda tap: a.taps[tap : tap + 1, 128 * w : 128 * (w + 1)]

    def input_tap(j):
        return lambda tap: pair_row(s.prm, 4 + tap, j)

    def bco_to(d):
        peer = lax.rem(x + d, NX)
        return remote(s.dbc.at[peer], s.bco.at[x], m.ob_s.at[d - 1], m.ob_r.at[d - 1], {"x": peer})

    def dto_to(d):
        peer = lax.rem(x + d, NX)
        return remote(s.ddt.at[peer], s.dto.at[x], m.ot_s.at[d - 1], m.ot_r.at[d - 1], {"x": peer})

    def dxo_to(d):
        peer = lax.rem(x + d, NX)
        return remote(
            s.dx.at[peer], o.dxo.at[:, columns(x, LW)], m.ox_s.at[d - 1], m.ox_r.at[d - 1], {"x": peer}
        )

    def edges_out(n):
        before, behind = {"z": down, "x": jnp.int32(NX - 1)}, {"z": up, "x": jnp.int32(0)}
        return (
            remote(s.dbp, s.ebn.at[n], m.e_s.at[0], m.e_r.at[0, n], before),
            remote(s.dbn, s.ebp.at[n], m.e_s.at[1], m.e_r.at[1, n], behind),
            remote(s.dxp, s.exn.at[:, columns(n, LW)], m.e_s.at[2], m.e_r.at[2, n], before),
            remote(s.dxn, s.exp.at[:, columns(n, LW)], m.e_s.at[3], m.e_r.at[3, n], behind),
        )

    masked_edges(s.dbcpad, 2 * STATE, map_tap, s.dbp, s.dbn)
    for copy in edges_out(x)[:2]:
        copy.start()
    for k in range(NX):
        for w in range(2):
            lanes = slice(STATE * w, STATE * (w + 1))
            s.dbc[k, :, lanes] = unconvolved(s.dbcpad, k * BLOCK, BLOCK, lanes, map_tap(w)).astype(bf16)
    for d in (2, 1, 3):
        bco_to(d).start()
    own_bco = pltpu.make_async_copy(s.dbc.at[x], s.bco.at[x], m.own.at[6])
    own_bco.start()

    masked_edges(s.dxpad, LW, input_tap, s.dxp, s.dxn)
    for copy in edges_out(x)[2:]:
        copy.start()
    for k in range(NX):
        for j in range(LH // 2):
            lanes = slice(128 * j, 128 * (j + 1))
            s.dx[k, :, lanes] = unconvolved(s.dxpad, k * BLOCK, BLOCK, lanes, input_tap(j)).astype(bf16)
    for d in (2, 1, 3):
        dxo_to(d).start()
    own_dx = pltpu.make_async_copy(s.dx.at[x], o.dxo.at[:, columns(x, LW)], m.own.at[7])
    own_dx.start()

    own_bco.wait()
    for d in range(1, NX):
        bco_to(d).wait_recv()

    @when(x_last)
    def _():
        for n in range(NX):
            edges_out(n)[0].wait_recv()

    @when(x_first)
    def _():
        for n in range(NX):
            edges_out(n)[1].wait_recv()

    for g in range(GROUPS):
        lanes = slice(2 * STATE * g, 2 * STATE * (g + 1))
        both = s.bco[2 * g].astype(f32) + s.bco[2 * g + 1].astype(f32)
        edge = s.ebp[2 * g].astype(f32) + s.ebp[2 * g + 1].astype(f32)
        s.dmaps[0:EDGE, lanes] = (both[0:EDGE] + edge).astype(bf16)
        s.dmaps[EDGE : BLOCK - EDGE, lanes] = both[EDGE : BLOCK - EDGE].astype(bf16)
        edge = s.ebn[2 * g].astype(f32) + s.ebn[2 * g + 1].astype(f32)
        s.dmaps[BLOCK - EDGE :, lanes] = (both[BLOCK - EDGE :] + edge).astype(bf16)

    order = [4, 3, 5, 2, 6, 1, 7, 0]

    def weight_part(n, core):
        block = lax.rem(y + order[n], NY) * NC + core
        return dot_tn(a.act[:, columns(block, BLOCK)], s.dmaps[...])

    def swap(n):
        return remote(s.part.at[n], s.pair.at[n], m.sw_s.at[n], m.sw_r.at[n], {"c": other})

    for n in range(NY):
        s.part[n] = weight_part(n, other).astype(bf16)
        swap(n).start()
    for n in range(NY):
        s.kept[n] = weight_part(n, c)

    def reduced(step, h, way):
        send, recv, to = (m.rr_s, m.rr_r, north) if way > 0 else (m.rl_s, m.rl_r, south)
        out, into = (s.outwr, s.inr) if way > 0 else (s.outwl, s.inl)
        return remote(out.at[step, rows(h)], into.at[step, rows(h)], send.at[step, h], recv.at[step, h], {"y": to})

    def both_cores(n, h):
        return s.kept[n, rows(h)] + s.pair[n, rows(h)].astype(f32)

    def hidden_part(n):
        s_block = n
        o.dhid[:, 128 * n : 128 * (n + 1)] = dot_nt(s.dmaps[...], s.wf[s_block]).astype(bf16)

    for step in range(4):
        for n in ((0,), (1, 2), (3, 4), (5, 6))[step]:
            swap(n).wait_recv()
        for h in range(2):
            for way in (1, -1):
                if step == 0 and (h == 0) != (way == 1):
                    continue
                n = order.index((way * (4 - step)) % NY)
                value = both_cores(n, h)
                if step > 1 or (step == 1 and (h == 0) == (way == 1)):
                    reduced(step - 1, h, way).wait_recv()
                    value = value + (s.inr if way > 0 else s.inl)[step - 1, rows(h)].astype(f32)
                (s.outwr if way > 0 else s.outwl)[step, rows(h)] = value.astype(bf16)
                reduced(step, h, way).start()
        for n in range(4 * step, 4 * step + 4):
            hidden_part(n)
    swap(7).wait_recv()
    for h in range(2):
        value = both_cores(7, h)
        reduced(3, h, 1).wait_recv()
        value = value + s.inr[3, rows(h)].astype(f32)
        reduced(3, h, -1).wait_recv()
        s.quarter[rows(h)] = value + s.inl[3, rows(h)].astype(f32)

    strip = BLOCK // NX

    def strip_to(d):
        peer = lax.rem(x + d, NX)
        return remote(
            s.quarter.at[columns(peer, strip)], s.xin.at[d - 1], m.qx_s.at[d - 1], m.qx_r.at[d - 1], {"x": peer}
        )

    for d in (2, 1, 3):
        strip_to(d).start()

    own_dx.wait()
    for d in range(1, NX):
        dxo_to(d).wait_recv()

    @when(x_last)
    def _():
        for n in range(NX):
            edges_out(n)[2].wait_recv()
        at = slice(BLOCK - EDGE, BLOCK)
        o.dxo[at, :] = (o.dxo[at, :].astype(f32) + s.exn[...].astype(f32)).astype(bf16)

    @when(x_first)
    def _():
        for n in range(NX):
            edges_out(n)[3].wait_recv()
        o.dxo[0:EDGE, :] = (o.dxo[0:EDGE, :].astype(f32) + s.exp[...].astype(f32)).astype(bf16)

    strips = s.quarter[columns(x, strip)]
    for d in range(1, NX):
        strip_to(d).wait_recv()
        strips = strips + s.xin[d - 1]
    for i in range(NZ):
        s.piece[i] = strips[8 * (i // 2) : 8 * (i // 2) + 8, 256 * (i % 2) : 256 * (i % 2) + 256]

    def piece_to(d):
        peer = lax.rem(z + d, NZ)
        return remote(s.piece.at[peer], s.zin.at[d - 1], m.qz_s.at[d - 1], m.qz_r.at[d - 1], {"z": peer})

    for d in (4, 3, 5, 2, 6, 1, 7):
        piece_to(d).start()

    met = s.right[NX, 0] * s.left[NX - 1, 1] + s.right[NX, 1] * s.left[NX - 1, 0]
    picks = jnp.concatenate([s.gather[...]] * 2, axis=1)
    crossing_end = dot_nt(picks, jnp.concatenate(parts_of(met, 2), axis=1).astype(bf16))
    after = -jnp.sum(crossing_end, axis=1, keepdims=True)
    for k in range(NX - 1, -1, -1):
        d_rate = jnp.dot(s.dl[k], lower, precision=highest, preferred_element_type=f32) + after
        after = d_rate[:, 0:1]
        d_dt = d_rate * jnp.exp(s.prm[:, 10, :]) + s.dvu[k]
        s.ddt[k] = d_dt / (1.0 + jnp.exp(-(s.dth[k] + s.prm[:, 9, :])))
    for d in range(1, NX):
        dto_to(d).start()
    own_ddt = pltpu.make_async_copy(s.ddt.at[x], s.dto.at[x], m.own.at[8])
    own_ddt.start()

    value = s.piece[z]
    for d in range(1, NZ):
        piece_to(d).wait_recv()
        value = value + s.zin[d - 1]
    s.held[z] = value

    def piece_back(d):
        return remote(s.held.at[z], s.held.at[z], m.gz_s.at[d - 1], m.gz_r.at[d - 1], {"z": lax.rem(z + d, NZ)})

    def piece_from(d):
        source = lax.rem(z - d + NZ, NZ)
        return remote(s.held.at[z], s.held.at[source], m.gz_s.at[d - 1], m.gz_r.at[d - 1], {"z": source})

    for d in (4, 3, 5, 2, 6, 1, 7):
        piece_back(d).start()
    own_ddt.wait()
    for d in range(1, NX):
        dto_to(d).wait_recv()
    for n in range(NX):
        o.dts[8 * n : 8 * n + 8] = s.dto[n]
    for d in range(1, NZ):
        piece_from(d).wait_recv()
    own_strip = columns(x, strip)
    o.total[own_strip] = jnp.concatenate(
        [jnp.concatenate([s.held[2 * i], s.held[2 * i + 1]], axis=1) for i in range(NZ // 2)], axis=0
    )

    def strip_back(d):
        at = o.total.at[own_strip]
        return remote(at, at, m.gx_s.at[d - 1], m.gx_r.at[d - 1], {"x": lax.rem(x + d, NX)})

    def strip_from(d):
        source = lax.rem(x - d + NX, NX)
        at = o.total.at[columns(source, strip)]
        return remote(at, at, m.gx_s.at[d - 1], m.gx_r.at[d - 1], {"x": source})

    for d in (2, 1, 3):
        strip_back(d).start()

    for step, h, way in w_steps:
        w_ring(step, h, way).wait_send()
    for h in range(2):
        for n in range(8):
            w_across(n, h).wait_send()
    for d in range(1, NX):
        for copy in (x_to(d), dt_to(d), dy_to(d), bc_to(d), bco_to(d), dto_to(d), dxo_to(d), strip_to(d)):
            copy.wait_send()
    for i in range(NZ):

        @unless(jnp.logical_and(mine, z == i))
        def _():
            message(i).wait_send()

    for copy in edges_out(x):
        copy.wait_send()

    def sent(n, carry):
        @unless(last)
        def _():
            going_up(n).wait_send()

        @unless(first)
        def _():
            going_down(n).wait_send()

        return carry

    lax.fori_loop(0, PIECES, sent, 0)
    for n in range(NY):
        swap(n).wait_send()
    for step in range(4):
        for h in range(2):
            for way in (1, -1):
                if step > 0 or (h == 0) == (way == 1):
                    reduced(step, h, way).wait_send()
    for d in range(1, NZ):
        piece_to(d).wait_send()
        piece_back(d).wait_send()
    for d in range(1, NX):
        strip_from(d).wait_recv()
    for d in range(1, NX):
        strip_back(d).wait_send()


def whole(w, act, x, switch, saved, final, gain, dt, msg, taps):
    shapes = (
        jax.ShapeDtypeStruct((BLOCK, INNER), bf16),
        jax.ShapeDtypeStruct((BLOCK, INNER), bf16),
        jax.ShapeDtypeStruct((BLOCK, INNER), bf16),
        jax.ShapeDtypeStruct((HEADS, BLOCK), f32),
        jax.ShapeDtypeStruct((BLOCK, 2 * GROUPS * STATE), f32),
    )
    scratch = [pltpu.VMEM(shape, dtype) for shape, dtype in BUFFERS.values()]
    scratch += [DMA(shape) for shape in SEMAPHORES.values()]
    return pl.pallas_call(
        kernel,
        out_shape=shapes,
        in_specs=[vmem()] * len(INPUTS),
        out_specs=tuple(vmem() for _ in shapes),
        scratch_shapes=scratch,
        compiler_params=pltpu.CompilerParams(
            collective_id=0, has_side_effects=True, vmem_limit_bytes=VMEM_LIMIT
        ),
        name="mixer_backward",
    )(w, act, x, switch, saved, final, gain, dt, msg, taps)


def interleaved(first, second):
    return jnp.concatenate(
        [first[..., :STATE], second[..., :STATE], first[..., STATE:], second[..., STATE:]], axis=-1
    )


def local(
    layer_activity, writer_matrix, reader_matrix, source_unfiltered, switch_raw_signal, saved_result,
    final_adjoint, delta_raw, extra_logdrop, source_filter_coefs, writer_filter_coefs, reader_filter_coefs,
    delta_offset, fading_exponents, direct_factor, rescale_factor,
):
    tokens = layer_activity.shape[1]
    shard = interleaved(writer_matrix, reader_matrix)
    taps = jnp.concatenate([source_filter_coefs, source_filter_coefs], axis=1)
    scalars = jnp.broadcast_to(
        jnp.concatenate([delta_offset, fading_exponents, direct_factor])[:, None], (3, BLOCK)
    )
    params = jnp.concatenate([taps, scalars, jnp.zeros((4, BLOCK), f32)], axis=0)
    drops = extra_logdrop.reshape(NZ, NX, BLOCK)
    message = jnp.concatenate([drops, jnp.broadcast_to(params[None], (NZ, 12, BLOCK))], axis=1)
    delta = delta_raw.reshape(tokens, HEADS).T.astype(f32)
    group = lax.axis_index("x") // 2
    all_taps = interleaved(writer_filter_coefs, reader_filter_coefs)
    map_taps = jnp.where(group == 0, all_taps[:, : 2 * STATE], all_taps[:, 2 * STATE :])
    d_gate, d_x, d_hidden, d_dt, total = whole(
        shard,
        layer_activity.reshape(tokens, -1),
        source_unfiltered.reshape(tokens, INNER),
        switch_raw_signal.reshape(tokens, INNER),
        saved_result.reshape(tokens, INNER),
        final_adjoint.reshape(tokens, INNER),
        rescale_factor.reshape(1, INNER),
        delta,
        message,
        map_taps,
    )
    return (
        d_hidden.reshape(1, tokens, -1),
        d_x.reshape(1, tokens, INNER),
        d_gate.reshape(1, tokens, INNER),
        d_dt.T.astype(bf16).reshape(1, tokens, HEADS),
        jnp.concatenate([total[:, :STATE], total[:, 2 * STATE : 3 * STATE]], axis=1),
        jnp.concatenate([total[:, STATE : 2 * STATE], total[:, 3 * STATE :]], axis=1),
    )


def solution(mesh):
    split = Mesh(mesh.devices.reshape(NZ, NX, NY, NC), ("z", "x", "y", "c"))
    sp, dp = ("z", "x"), ("y", "c")
    in_specs = (
        P(dp, sp, None),
        P(dp, None),
        P(dp, None),
        P(dp, sp, None),
        P(dp, sp, None),
        P(dp, sp, None),
        P(dp, sp, None),
        P(dp, sp, None),
        P(dp, None, sp),
        P(None, sp),
        P(),
        P(),
        P(sp),
        P(sp),
        P(sp),
        P(),
    )
    out_specs = (
        P(dp, sp, None),
        P(dp, sp, None),
        P(dp, sp, None),
        P(dp, sp, None),
        P(dp, None),
        P(dp, None),
    )
    return jax.shard_map(local, mesh=split, in_specs=in_specs, out_specs=out_specs, check_vma=False)
```

```python
import functools

import jax
import jax.numpy as jnp
from jax import lax
from jax.experimental import pallas as pl
from jax.experimental.pallas import tpu as pltpu
from jax.sharding import Mesh
from jax.sharding import PartitionSpec as P

HEADS = 32
HEAD_DIM = 64
STATE = 128
GROUPS = 2
NORM_GROUPS = 8
CONV_K = 5
BLOCK = 128
INNER = 2048
NZ, NX, NY, NC = 8, 4, 8, 2
LH = HEADS // NX
LW = LH * HEAD_DIM
CHUNK = NX * BLOCK
EDGE = 16
EPSILON = 1e-06
VMEM_LIMIT = 60 * 1024 * 1024

f32 = jnp.float32
bf16 = jnp.bfloat16
highest = lax.Precision.HIGHEST
MESH = pl.DeviceIdType.MESH
DMA = pltpu.SemaphoreType.DMA


def vmem():
    return pl.BlockSpec(memory_space=pltpu.VMEM)


def remote(src, dst, send, recv, device):
    return pltpu.make_async_remote_copy(
        src_ref=src, dst_ref=dst, send_sem=send, recv_sem=recv, device_id=device, device_id_type=MESH
    )


def greet(barrier, device):
    pl.semaphore_signal(barrier, inc=1, device_id=device, device_id_type=MESH)


def columns(start, size):
    return pl.ds(pl.multiple_of(start * size, size), size)


def dot(a, b):
    return jnp.dot(a, b, preferred_element_type=f32)


def dot_nt(a, b):
    return lax.dot_general(a, b, (((1,), (1,)), ((), ())), preferred_element_type=f32)


def dot_tn(a, b):
    return lax.dot_general(a, b, (((0,), (0,)), ((), ())), preferred_element_type=f32)


def iota2(shape, dim):
    return lax.broadcasted_iota(jnp.int32, shape, dim)


def parts_of(value, count):
    out = []
    for _ in range(count):
        top = value.astype(bf16).astype(f32)
        out.append(top)
        value = value - top
    return out


def silu_parts(pre):
    gate = 1.0 / (1.0 + jnp.exp(-pre))
    return pre * gate, gate * (1.0 + pre * (1.0 - gate))


def norm_group(group, saved_ref, switch_ref, final_ref, gain_ref, dy_ref, dgate_ref):
    width = INNER // NORM_GROUPS
    cols = slice(group * width, (group + 1) * width)
    saved = saved_ref[:, cols].astype(f32)
    switch = switch_ref[:, cols].astype(f32)
    final = final_ref[:, cols].astype(f32)
    gate = 1.0 / (1.0 + jnp.exp(-switch))
    act = switch * gate
    mixed = saved * act
    scale = lax.rsqrt(jnp.mean(mixed * mixed, axis=-1, keepdims=True) + EPSILON)
    d_normed = final * gain_ref[:, cols]
    inner = jnp.mean(d_normed * mixed, axis=-1, keepdims=True)
    d_mixed = d_normed * scale - mixed * (scale * scale * scale * inner)
    dy_ref[:, cols] = (d_mixed * act).astype(bf16)
    slope = gate * (1.0 + switch * (1.0 - gate))
    dgate_ref[:, cols] = (d_mixed * saved * slope).astype(bf16)


def pair_row(prm_ref, row, j):
    lane = iota2((1, 128), 1)
    return jnp.where(lane < HEAD_DIM, prm_ref[2 * j, row : row + 1, :], prm_ref[2 * j + 1, row : row + 1, :])


def fill_padded(pad_ref, body_ref, prev_ref, next_ref, z):
    pad_ref[pl.ds(0, EDGE)] = jnp.where(z == 0, 0.0, prev_ref[...].astype(f32))
    for k in range(NX):
        pad_ref[pl.ds(EDGE + k * BLOCK, BLOCK)] = body_ref[k].astype(f32)
    pad_ref[pl.ds(EDGE + CHUNK, EDGE)] = jnp.where(z == NZ - 1, 0.0, next_ref[...].astype(f32))


def unconvolved(pad_ref, start, size, lanes, tap_of):
    total = jnp.zeros((size, 128), f32)
    for tap in range(CONV_K):
        total = total + tap_of(tap) * pad_ref[pl.ds(start + 2 * EDGE + 2 - tap, size), lanes]
    return total


BUFFERS = dict(
    w=((BLOCK, 2 * GROUPS * STATE), bf16),
    dt=((HEADS, BLOCK), f32),
    msg=((NZ, 16, BLOCK), f32),
    taps=((8, 2 * STATE), f32),
    dy=((BLOCK, INNER), bf16),
    xh=((NX, BLOCK, LW), bf16),
    dyh=((NX, BLOCK, LW), bf16),
    dth=((NX, LH, BLOCK), f32),
    prm=((LH, 16, BLOCK), f32),
    xp=((EDGE, LW), bf16),
    xn=((EDGE, LW), bf16),
    wf=((NY * NC, BLOCK, 2 * GROUPS * STATE), bf16),
    bc=((BLOCK, 2 * GROUPS * STATE), bf16),
    bch=((NX, BLOCK, 2 * STATE), bf16),
    bp=((EDGE, 2 * STATE), bf16),
    bn=((EDGE, 2 * STATE), bf16),
    three=((48, 3 * LW), bf16),
    wide=((24, LH * BLOCK), bf16),
    gather=((LH, LW), bf16),
    xpad=((CHUNK + 2 * EDGE, LW), f32),
    bcpad=((CHUNK + 2 * EDGE, 2 * STATE), f32),
    v16=((CHUNK, LW), bf16),
    pv16=((CHUNK, LW), bf16),
    qv16=((CHUNK, LW), bf16),
    pdy16=((CHUNK, LW), bf16),
    qdy16=((CHUNK, LW), bf16),
    b16=((CHUNK, STATE), bf16),
    c16=((CHUNK, STATE), bf16),
    u=((CHUNK, LW), f32),
    slope=((CHUNK, LW), f32),
    spread=((CHUNK, 3 * LW), f32),
    bs=((CHUNK, STATE), f32),
    cs=((CHUNK, STATE), f32),
    level=((NX, LH, BLOCK), f32),
    gamma=((NX, 8, LW), f32),
    signed=((NX, BLOCK, BLOCK), f32),
    grid_t=((NX, BLOCK, BLOCK), f32),
    weights=((NX, BLOCK, BLOCK), f32),
    right=((NX + 1, 2, STATE, LW), f32),
    left=((NX, 2, STATE, LW), f32),
    sr=((2, STATE, LW), f32),
    sl=((2, STATE, LW), f32),
    decay=((8, LW), f32),
    outr=((2, STATE, LW), bf16),
    outl=((2, STATE, LW), bf16),
    cr=((2, STATE, LW), bf16),
    cl=((2, STATE, LW), bf16),
    dv=((CHUNK, LW), f32),
    dl=((NX, LH, BLOCK), f32),
    dvu=((NX, LH, BLOCK), f32),
    dxpad=((CHUNK + 4 * EDGE, LW), f32),
    dbcpad=((CHUNK + 4 * EDGE, 2 * STATE), f32),
    dx=((NX, BLOCK, LW), bf16),
    dxp=((EDGE, LW), bf16),
    dxn=((EDGE, LW), bf16),
    dbc=((NX, BLOCK, 2 * STATE), bf16),
    dbp=((EDGE, 2 * STATE), bf16),
    dbn=((EDGE, 2 * STATE), bf16),
    ddt=((NX, LH, BLOCK), f32),
    dto=((NX, LH, BLOCK), f32),
    exp=((EDGE, INNER), bf16),
    exn=((EDGE, INNER), bf16),
    bco=((NX, BLOCK, 2 * STATE), bf16),
    ebp=((NX, EDGE, 2 * STATE), bf16),
    ebn=((NX, EDGE, 2 * STATE), bf16),
    dmaps=((BLOCK, 2 * GROUPS * STATE), bf16),
    part=((NY, BLOCK, 2 * GROUPS * STATE), bf16),
    kept=((NY, BLOCK, 2 * GROUPS * STATE), f32),
    pair=((NY, BLOCK, 2 * GROUPS * STATE), bf16),
    inr=((4, BLOCK, 2 * GROUPS * STATE), bf16),
    inl=((4, BLOCK, 2 * GROUPS * STATE), bf16),
    outwr=((4, BLOCK, 2 * GROUPS * STATE), bf16),
    outwl=((4, BLOCK, 2 * GROUPS * STATE), bf16),
    quarter=((BLOCK, 2 * GROUPS * STATE), f32),
    piece=((NZ, 8, 256), f32),
    xin=((NX - 1, BLOCK // NX, 2 * GROUPS * STATE), f32),
    zin=((NZ - 1, 8, 256), f32),
    held=((NZ, 8, 256), f32),
)
PIECES = 16
LAG = 5
CUTS = 4
UNITS = NX * LH // 2
SEMAPHORES = dict(
    own=(12,), x_s=(3,), x_r=(3,), y_s=(3,), y_r=(3,), t_s=(3,), t_r=(3,), m_s=(8,), m_r=(8,),
    h_s=(4, NX), h_r=(4,), wr_s=(4, CUTS), wr_r=(4, CUTS), wl_s=(4, CUTS), wl_r=(4, CUTS),
    wp_s=(8, CUTS), wp_r=(8, CUTS),
    b_s=(3,), b_r=(3,), up_s=(PIECES,), up_r=(PIECES,), dn_s=(PIECES,), dn_r=(PIECES,),
    ox_s=(3,), ox_r=(3,), ob_s=(3,), ob_r=(3,), ot_s=(3,), ot_r=(3,), e_s=(4,), e_r=(4, NX),
    sw_s=(8,), sw_r=(8,), rr_s=(4, CUTS), rr_r=(4, CUTS), rl_s=(4, CUTS), rl_r=(4, CUTS),
    qx_s=(3,), qx_r=(3,), qz_s=(7,), qz_r=(7,), gz_s=(7,), gz_r=(7,), gx_s=(2, 3), gx_r=(2, 3),
)


class Named:
    def __init__(self, names, refs):
        for name, ref in zip(names, refs, strict=True):
            setattr(self, name, ref)


INPUTS = (
    "wb", "wc", "act", "x", "switch", "saved", "final", "gain", "delta", "drops",
    "source_taps", "writer_taps", "reader_taps", "offset", "fading", "skip",
)
OUTPUTS = ("dgate", "dxo", "dhid", "dts", "dwb", "dwc")


def kernel(*refs):
    n_in, n_out, n_buf = len(INPUTS), len(OUTPUTS), len(BUFFERS)
    a = Named(INPUTS, refs[:n_in])
    o = Named(OUTPUTS, refs[n_in : n_in + n_out])
    s = Named(BUFFERS, refs[n_in + n_out : n_in + n_out + n_buf])
    m = Named(SEMAPHORES, refs[n_in + n_out + n_buf :])
    z, x, y, c = (lax.axis_index(name) for name in ("z", "x", "y", "c"))
    cut = BLOCK // CUTS
    up, down = lax.rem(z + 1, NZ), lax.rem(z + NZ - 1, NZ)
    north, south = lax.rem(y + 1, NY), lax.rem(y + NY - 1, NY)
    other = 1 - c
    head = z * NX + x
    dest = z // 2
    slot = lax.rem(head, LH)
    mine = dest == x
    first, last = z == 0, z == NZ - 1
    x_first, x_last = x == 0, x == NX - 1

    def when(condition):
        return pl.when(condition)

    def unless(condition):
        return pl.when(jnp.logical_not(condition))

    def sender_of(i):
        return 2 * x + i // NX, i % NX

    def is_me(i):
        sz, sx = sender_of(i)
        return jnp.logical_and(sz == z, sx == x)

    @when(first)
    def _():
        s.cr[...] = jnp.zeros_like(s.cr)

    @when(last)
    def _():
        s.cl[...] = jnp.zeros_like(s.cl)

    @unless(x_first)
    def _():
        s.exp[...] = jnp.zeros_like(s.exp)
        s.ebp[...] = jnp.zeros_like(s.ebp)

    @unless(x_last)
    def _():
        s.exn[...] = jnp.zeros_like(s.exn)
        s.ebn[...] = jnp.zeros_like(s.ebn)

    gather_w = []
    for g in range(GROUPS):
        lanes = slice(STATE * g, STATE * (g + 1))
        for n, ref in enumerate((a.wb, a.wc)):
            to = slice(STATE * (2 * g + n), STATE * (2 * g + n + 1))
            gather_w.append(pltpu.make_async_copy(ref.at[:, lanes], s.w.at[:, to], m.own.at[2 * g + n]))
    for copy in gather_w:
        copy.start()
    s.dt[...] = a.delta[...].astype(f32)
    row_taps = jnp.concatenate([a.source_taps[...]] * 2, axis=1)
    for i in range(NZ):
        s.msg[i, 0:4] = a.drops[i]
        s.msg[i, 4:9] = row_taps
        for n, ref in enumerate((a.offset, a.fading, a.skip)):
            s.msg[i, 9 + n : 10 + n] = jnp.full((1, BLOCK), ref[0], f32)
    low_group = x < NX // 2
    for n, ref in enumerate((a.writer_taps, a.reader_taps)):
        s.taps[0:CONV_K, STATE * n : STATE * (n + 1)] = jnp.where(low_group, ref[:, :STATE], ref[:, STATE:])
    for copy in gather_w:
        copy.wait()

    barrier = pltpu.get_barrier_semaphore()
    for d in range(1, NX):
        greet(barrier, {"x": lax.rem(x + d, NX)})
    for d in range(1, NZ):
        greet(barrier, {"z": lax.rem(z + d, NZ)})
    greet(barrier, {"y": north})
    greet(barrier, {"y": south})
    greet(barrier, {"c": other})
    for i in range(LH):

        @unless(is_me(i))
        def _():
            sz, sx = sender_of(i)
            greet(barrier, {"z": sz, "x": sx})

    greet(barrier, {"z": down, "x": jnp.int32(NX - 1)})
    greet(barrier, {"z": up, "x": jnp.int32(0)})

    @when(x_first)
    def _():
        for n in range(NX):
            greet(barrier, {"z": down, "x": jnp.int32(n)})

    @when(x_last)
    def _():
        for n in range(NX):
            greet(barrier, {"z": up, "x": jnp.int32(n)})

    pl.semaphore_wait(
        barrier,
        NX - 1 + NZ - 1 + 3 + NZ + 2
        - mine.astype(jnp.int32) + NX * x_first.astype(jnp.int32) + NX * x_last.astype(jnp.int32),
    )

    def rows(h):
        return pl.ds(h * cut, cut)

    def w_ring(step, h, way):
        block = lax.rem(y - way * step + NY, NY) * NC + c
        src = s.w.at[rows(h)] if step == 0 else s.wf.at[block, rows(h)]
        send, recv, to = (m.wr_s, m.wr_r, north) if way > 0 else (m.wl_s, m.wl_r, south)
        return remote(src, s.wf.at[block, rows(h)], send.at[step, h], recv.at[step, h], {"y": to})

    def w_offset(n):
        return 0 if n == 0 else (-n if n < 5 else n - 4)

    def w_across(n, h):
        block = lax.rem(y + w_offset(n) + NY, NY) * NC + c
        src = s.w.at[rows(h)] if n == 0 else s.wf.at[block, rows(h)]
        return remote(src, s.wf.at[block, rows(h)], m.wp_s.at[n, h], m.wp_r.at[n, h], {"c": other})

    def near_side(h, way):
        return (h < CUTS // 2) == (way == 1)

    w_steps = [
        (step, h, way) for step in range(4) for h in range(CUTS) for way in (1, -1) if step < 3 or near_side(h, way)
    ]
    for step, h, way in w_steps[: 2 * CUTS]:
        w_ring(step, h, way).start()
    own = [
        pltpu.make_async_copy(s.w, s.wf.at[y * NC + c], m.own.at[0]),
        pltpu.make_async_copy(a.x.at[:, columns(x, LW)], s.xh.at[x], m.own.at[1]),
        pltpu.make_async_copy(s.dt.at[columns(x, LH)], s.dth.at[x], m.own.at[2]),
    ]
    for copy in own:
        copy.start()
    for h in range(CUTS):
        w_across(0, h).start()

    def edge_in(which, n):
        tail, lead = pl.ds(BLOCK - EDGE, EDGE), pl.ds(0, EDGE)
        lanes, pair_lanes = columns(n, LW), columns(n // 2, 2 * STATE)
        src, dst, to = (
            (a.x.at[tail, lanes], s.xp, up),
            (a.x.at[lead, lanes], s.xn, down),
            (s.bc.at[tail, pair_lanes], s.bp, up),
            (s.bc.at[lead, pair_lanes], s.bn, down),
        )[which]
        return remote(src, dst, m.h_s.at[which, n], m.h_r.at[which], {"z": to, "x": jnp.int32(n)})

    def edges_start(pair):
        for n in range(NX):

            @when(x_last)
            def _():
                edge_in(2 * pair, n).start()

            @when(x_first)
            def _():
                edge_in(2 * pair + 1, n).start()

    edges_start(0)

    def x_to(d):
        peer = lax.rem(x + d, NX)
        return remote(
            a.x.at[:, columns(peer, LW)], s.xh.at[x], m.x_s.at[d - 1], m.x_r.at[d - 1], {"x": peer}
        )

    def dt_to(d):
        peer = lax.rem(x + d, NX)
        return remote(
            s.dt.at[columns(peer, LH)], s.dth.at[x], m.t_s.at[d - 1], m.t_r.at[d - 1], {"x": peer}
        )

    def dy_to(d):
        peer = lax.rem(x + d, NX)
        return remote(
            s.dy.at[:, columns(peer, LW)], s.dyh.at[x], m.y_s.at[d - 1], m.y_r.at[d - 1], {"x": peer}
        )

    def message(i):
        return remote(
            s.msg.at[i], s.prm.at[slot], m.m_s.at[i], m.m_r.at[slot], {"z": jnp.int32(i), "x": dest}
        )

    for d in range(1, NX):
        x_to(d).start()
        dt_to(d).start()
    keep = pltpu.make_async_copy(s.msg.at[z], s.prm.at[slot], m.own.at[3])
    for i in range(NZ):

        @unless(jnp.logical_and(mine, z == i))
        def _():
            message(i).start()

    @when(mine)
    def _():
        keep.start()

    for group in range(NORM_GROUPS):
        norm_group(group, a.saved, a.switch, a.final, a.gain, s.dy, o.dgate)
    for d in range(1, NX):
        dy_to(d).start()
    own_dy = pltpu.make_async_copy(s.dy.at[:, columns(x, LW)], s.dyh.at[x], m.own.at[4])
    own_dy.start()

    def projected(n, core):
        block = lax.rem(y + w_offset(n) + NY, NY) * NC + core
        return dot(a.act[:, columns(block, BLOCK)], s.wf[block])

    def inputs_of(k):
        for j in range(LH // 2):
            lanes = slice(128 * j, 128 * (j + 1))
            pre = jnp.zeros((BLOCK, 128), f32)
            for tap in range(CONV_K):
                pre = pre + pair_row(s.prm, 4 + tap, j) * s.xpad[pl.ds(k * BLOCK + EDGE - 2 + tap, BLOCK), lanes]
            at = pl.ds(k * BLOCK, BLOCK)
            s.u[at, lanes], s.slope[at, lanes] = silu_parts(pre)

    own[0].wait()
    maps = projected(0, c)
    for step in range(4):
        for h in range(CUTS):
            for way in (1, -1):
                if step == 3 and not near_side(h, way):
                    continue
                w_ring(step, h, way).wait_recv()
                following = (step + 1, h, way)
                if following in w_steps:
                    w_ring(*following).start()
                w_across(1 + step if way == 1 or step == 3 else 5 + step, h).start()
        if step < 3:
            maps = maps + projected(1 + step, c) + projected(5 + step, c)
        for n in ((0,), (1, 5), (2, 6), (3, 7))[step]:
            for h in range(CUTS):
                w_across(n, h).wait_recv()
            maps = maps + projected(n, other)
        if step == 2:
            for d in range(1, NX):
                x_to(d).wait_recv()
            own[1].wait()
            edge_in(0, x).wait_recv()
            edge_in(1, x).wait_recv()
            for i in range(LH):

                @unless(is_me(i))
                def _():
                    sz, sx = sender_of(i)
                    remote(s.msg.at[i], s.prm.at[i], m.m_s.at[i], m.m_r.at[i], {"z": sz, "x": sx}).wait_recv()

            @when(mine)
            def _():
                keep.wait()

            fill_padded(s.xpad, s.xh, s.xp, s.xn, z)
            for k in range(NX):
                inputs_of(k)
    maps = maps + projected(4, c)
    for h in range(CUTS):
        w_across(4, h).wait_recv()
    maps = maps + projected(4, other)
    s.bc[...] = maps.astype(bf16)

    def bc_to(d):
        peer = lax.rem(x + d, NX)
        return remote(
            s.bc.at[:, columns(peer // 2, 2 * STATE)], s.bch.at[x], m.b_s.at[d - 1], m.b_r.at[d - 1], {"x": peer}
        )

    for d in range(1, NX):
        bc_to(d).start()
    own_bc = pltpu.make_async_copy(s.bc.at[:, columns(x // 2, 2 * STATE)], s.bch.at[x], m.own.at[5])
    own_bc.start()
    edges_start(1)

    r, cc = iota2((48, 3 * LW), 0), iota2((48, 3 * LW), 1)
    s.three[...] = jnp.logical_and(
        r // 16 == cc // LW, jnp.bitwise_and(r, 7) == jnp.bitwise_and(cc, LW - 1) // HEAD_DIM
    ).astype(bf16)
    r, cc = iota2((24, LH * BLOCK), 0), iota2((24, LH * BLOCK), 1)
    s.wide[...] = (jnp.bitwise_and(r, 7) == cc // BLOCK).astype(bf16)
    s.gather[...] = (iota2((LH, LW), 1) // HEAD_DIM == iota2((LH, LW), 0)).astype(bf16)
    for pad in (s.dxpad, s.dbcpad):
        pad[pl.ds(0, 2 * EDGE)] = jnp.zeros((2 * EDGE, pad.shape[1]), f32)
        pad[pl.ds(2 * EDGE + CHUNK, 2 * EDGE)] = jnp.zeros((2 * EDGE, pad.shape[1]), f32)

    for d in range(1, NX):
        dt_to(d).wait_recv()
        dy_to(d).wait_recv()
    own[2].wait()
    own_dy.wait()
    row, col = iota2((BLOCK, BLOCK), 0), iota2((BLOCK, BLOCK), 1)
    upper = (row <= col).astype(f32)
    lower = (row >= col).astype(f32)
    sign = (row > col).astype(f32) - (row < col).astype(f32)
    low_half = iota2((BLOCK, 128), 1) < HEAD_DIM
    head_row = iota2((8, BLOCK), 0)

    for k in range(NX):
        at = pl.ds(k * BLOCK, BLOCK)
        dt = jax.nn.softplus(s.dth[k] + s.prm[:, 9, :])
        rate = dt * jnp.exp(s.prm[:, 10, :]) + s.prm[:, k, :]
        level = jnp.dot(rate, upper, precision=highest, preferred_element_type=f32)
        total = level[:, BLOCK - 1 : BLOCK]
        s.level[k] = level
        stack = jnp.concatenate(
            parts_of(dt, 2) + parts_of(jnp.exp(-level), 2) + parts_of(jnp.exp(level - total), 2), axis=0
        )
        spread = dot_tn(stack.astype(bf16), s.three[...])
        s.spread[at] = spread
        s.gamma[k] = jnp.broadcast_to(spread[BLOCK - 1 : BLOCK, LW : 2 * LW], (8, LW))
        for j in range(LH // 2):
            lanes = slice(128 * j, 128 * (j + 1))
            pe = spread[:, LW + 128 * j : LW + 128 * (j + 1)]
            qe = spread[:, 2 * LW + 128 * j : 2 * LW + 128 * (j + 1)]
            v = s.u[at, lanes] * spread[:, lanes]
            dy = s.dyh[k, :, lanes].astype(f32)
            s.v16[at, lanes] = v.astype(bf16)
            s.pv16[at, lanes], s.qv16[at, lanes] = (pe * v).astype(bf16), (qe * v).astype(bf16)
            s.pdy16[at, lanes], s.qdy16[at, lanes] = (pe * dy).astype(bf16), (qe * dy).astype(bf16)

    own_bc.wait()
    for d in range(1, NX):
        bc_to(d).wait_recv()
    edge_in(2, x).wait_recv()
    edge_in(3, x).wait_recv()
    fill_padded(s.bcpad, s.bch, s.bp, s.bn, z)
    s.decay[...] = jnp.ones_like(s.decay)
    for k in range(NX):
        at = pl.ds(k * BLOCK, BLOCK)
        for which, held, slopes in ((0, s.b16, s.bs), (1, s.c16, s.cs)):
            lanes = slice(which * STATE, (which + 1) * STATE)
            pre = jnp.zeros((BLOCK, STATE), f32)
            for tap in range(CONV_K):
                pre = pre + s.taps[tap : tap + 1, lanes] * s.bcpad[pl.ds(k * BLOCK + EDGE - 2 + tap, BLOCK), lanes]
            value, slopes[at] = silu_parts(pre)
            held[at] = value.astype(bf16)
        b, cc = s.b16[at], s.c16[at]
        kvr, cdr = dot_tn(b, s.qv16[at]), dot_tn(cc, s.qdy16[at])
        kvl, cdl = dot_tn(b, s.pv16[at]), dot_tn(cc, s.pdy16[at])
        s.right[k + 1, 0], s.right[k + 1, 1] = kvr, cdr
        if k > 0:
            s.left[k - 1, 0], s.left[k - 1, 1] = kvl, cdl
        if k == 0:
            s.sr[0], s.sr[1], s.sl[0], s.sl[1] = kvr, cdr, kvl, cdl
        else:
            g, before = s.gamma[k, 0:1], s.decay[0:1]
            s.sr[0] = s.sr[0] * g + kvr
            s.sr[1] = s.sr[1] * g + cdr
            s.sl[0] = s.sl[0] + before * kvl
            s.sl[1] = s.sl[1] + before * cdl
        s.decay[...] = s.decay[...] * s.gamma[k]

    def piece(n):
        return n // 8, pl.ds(pl.multiple_of(lax.rem(n // 4, 2) * 64, 64), 64), columns(lax.rem(n, 4), 128)

    def going_up(n):
        return remote(s.outr.at[piece(n)], s.cr.at[piece(n)], m.up_s.at[n], m.up_r.at[n], {"z": up})

    def going_down(n):
        return remote(s.outl.at[piece(n)], s.cl.at[piece(n)], m.dn_s.at[n], m.dn_r.at[n], {"z": down})

    def scan_step(t):
        n = t - LAG * z

        @when(jnp.logical_and(n >= 0, n < PIECES))
        def _():
            @unless(first)
            def _():
                going_up(n).wait_recv()

            @unless(last)
            def _():
                at = piece(n)
                s.outr[at] = (s.cr[at].astype(f32) * s.decay[0:1, at[2]] + s.sr[at]).astype(bf16)
                going_up(n).start()

        i = t - LAG * (NZ - 1 - z)

        @when(jnp.logical_and(i >= 0, i < PIECES))
        def _():
            @unless(last)
            def _():
                going_down(i).wait_recv()

            @unless(first)
            def _():
                at = piece(i)
                s.outl[at] = (s.cl[at].astype(f32) * s.decay[0:1, at[2]] + s.sl[at]).astype(bf16)
                going_down(i).start()

    def within(k, j):
        at = pl.ds(pl.multiple_of(k * BLOCK, BLOCK), BLOCK)
        lanes = columns(j, 128)
        parts = jnp.concatenate(parts_of(s.level[k], 3), axis=0).astype(bf16)
        level_cols = dot_tn(parts, s.wide[:, columns(j, 256)])
        vj, dyj = s.v16[at, lanes], s.dyh[k, :, lanes]
        signed, grid_t = s.signed[k], s.grid_t[k]
        halves = []
        weights = s.weights[k]
        dl = s.dl[k]
        for i in range(2):
            h = 2 * j + i
            near = jnp.exp(-jnp.abs(level_cols[:, 128 * i : 128 * (i + 1)] - s.level[k, pl.ds(h, 1), :]))
            keep_half = low_half if i == 0 else jnp.logical_not(low_half)
            shared = dot_nt(jnp.where(keep_half, dyj, jnp.zeros_like(dyj)), vj) * near
            weights = weights + shared
            crossing = (shared * signed).astype(bf16)
            pick = (head_row == h).astype(bf16)
            dl = dl + dot(pick, crossing) - dot_nt(pick, crossing)
            halves.append(dot((grid_t * near).astype(bf16), dyj))
        s.weights[k] = weights
        s.dl[k] = dl
        s.dv[at, lanes] = jnp.where(low_half, halves[0], halves[1])

    s.weights[...] = jnp.zeros_like(s.weights)
    s.dl[...] = jnp.zeros_like(s.dl)
    for k in range(NX):
        at = pl.ds(k * BLOCK, BLOCK)
        b, cc = s.b16[at], s.c16[at]
        s.signed[k] = dot_nt(cc, b) * sign
        s.grid_t[k] = dot_nt(b, cc)

    far = z // (NZ // 2)
    near_end = z * (1 - far) + (NZ - 1 - z) * far
    before = LAG * near_end
    between = before + PIECES
    until = LAG * (NZ - 1 - near_end)

    def unit(n):
        within(n // (LH // 2), lax.rem(n, LH // 2))

    def steps(t, carry):
        scan_step(t)

        @when(t < before)
        def _():
            unit(t)

        @when(jnp.logical_and(t >= between, t < until))
        def _():
            def two(i, inner):
                n = before + 2 * (t - between) + i

                @when(n < UNITS)
                def _():
                    unit(n)

                return inner

            lax.fori_loop(0, 2, two, 0)

        return carry

    lax.fori_loop(0, PIECES + LAG * (NZ - 1), steps, 0)

    def rest(n, carry):
        done = jnp.where(until > between, before + 2 * (until - between), before)

        @when(n >= done)
        def _():
            unit(n)

        return carry

    lax.fori_loop(0, UNITS, rest, 0)

    s.right[0, 0], s.right[0, 1] = s.cr[0].astype(f32), s.cr[1].astype(f32)
    s.left[NX - 1, 0], s.left[NX - 1, 1] = s.cl[0].astype(f32), s.cl[1].astype(f32)
    for k in range(NX):
        g = s.gamma[k, 0:1]
        s.right[k + 1, 0] = s.right[k + 1, 0] + s.right[k, 0] * g
        s.right[k + 1, 1] = s.right[k + 1, 1] + s.right[k, 1] * g
    for k in range(NX - 2, -1, -1):
        g = s.gamma[k + 1, 0:1]
        s.left[k, 0] = s.left[k, 0] + g * s.left[k + 1, 0]
        s.left[k, 1] = s.left[k, 1] + g * s.left[k + 1, 1]

    def map_gradients(k, carry):
        at = pl.ds(pl.multiple_of(k * BLOCK, BLOCK), BLOCK)
        padded = pl.ds(pl.multiple_of(2 * EDGE + k * BLOCK, EDGE), BLOCK)
        weights = s.weights[k].astype(bf16)
        dc = dot(weights, s.b16[at])
        db = dot_tn(weights, s.c16[at])
        dc = dc + dot_nt(s.pdy16[at], s.right[k, 0].astype(bf16)) + dot_nt(s.qdy16[at], s.left[k, 0].astype(bf16))
        db = db + dot_nt(s.qv16[at], s.left[k, 1].astype(bf16)) + dot_nt(s.pv16[at], s.right[k, 1].astype(bf16))
        s.dbcpad[padded, 0:STATE] = db * s.bs[at]
        s.dbcpad[padded, STATE : 2 * STATE] = dc * s.cs[at]
        return carry

    lax.fori_loop(0, NX, map_gradients, 0)

    def input_gradients(k, carry):
        at = pl.ds(pl.multiple_of(k * BLOCK, BLOCK), BLOCK)
        padded = pl.ds(pl.multiple_of(2 * EDGE + k * BLOCK, EDGE), BLOCK)
        b, cc = s.b16[at], s.c16[at]
        dl = s.dl[k]
        dvu = jnp.zeros((8, BLOCK), f32)
        for j in range(LH // 2):
            lanes = slice(128 * j, 128 * (j + 1))
            kvr, cdr = s.right[k, 0, :, lanes].astype(bf16), s.right[k, 1, :, lanes].astype(bf16)
            kvl, cdl = s.left[k, 0, :, lanes].astype(bf16), s.left[k, 1, :, lanes].astype(bf16)
            pe = s.spread[at, LW + 128 * j : LW + 128 * (j + 1)]
            qe = s.spread[at, 2 * LW + 128 * j : 2 * LW + 128 * (j + 1)]
            from_later, from_earlier = dot(b, cdl), dot(b, cdr)
            pv, qv, pdy, qdy = s.pv16[at, lanes], s.qv16[at, lanes], s.pdy16[at, lanes], s.qdy16[at, lanes]
            dv = s.dv[at, lanes] + qe * from_later + pe * from_earlier
            cross = (
                qv.astype(f32) * from_later - pv.astype(f32) * from_earlier
                + qdy.astype(f32) * dot(cc, kvl) - pdy.astype(f32) * dot(cc, kvr)
            )
            picks = jnp.concatenate([s.gather[:, lanes]] * 2, axis=1)
            dl = dl + dot_nt(picks, jnp.concatenate(parts_of(cross, 2), axis=1).astype(bf16))
            dvu = dvu + dot_nt(picks, jnp.concatenate(parts_of(dv * s.u[at, lanes], 2), axis=1).astype(bf16))
            du = dv * s.spread[at, lanes] + pair_row(s.prm, 11, j) * s.dyh[k, :, lanes].astype(f32)
            s.dxpad[padded, lanes] = du * s.slope[at, lanes]
        s.dl[k], s.dvu[k] = dl, dvu
        return carry

    def masked_edges(pad, width, tap_for, before_ref, behind_ref):
        for w in range(width // 128):
            lanes = slice(128 * w, 128 * (w + 1))
            before = unconvolved(pad, -EDGE, EDGE, lanes, tap_for(w))
            behind = unconvolved(pad, CHUNK, EDGE, lanes, tap_for(w))
            before_ref[:, lanes] = jnp.where(first, 0.0, before).astype(bf16)
            behind_ref[:, lanes] = jnp.where(last, 0.0, behind).astype(bf16)

    def map_tap(w):
        return lambda tap: s.taps[tap : tap + 1, 128 * w : 128 * (w + 1)]

    def input_tap(j):
        return lambda tap: pair_row(s.prm, 4 + tap, j)

    def bco_to(d):
        peer = lax.rem(x + d, NX)
        return remote(s.dbc.at[peer], s.bco.at[x], m.ob_s.at[d - 1], m.ob_r.at[d - 1], {"x": peer})

    def dto_to(d):
        peer = lax.rem(x + d, NX)
        return remote(s.ddt.at[peer], s.dto.at[x], m.ot_s.at[d - 1], m.ot_r.at[d - 1], {"x": peer})

    def dxo_to(d):
        peer = lax.rem(x + d, NX)
        return remote(
            s.dx.at[peer], o.dxo.at[:, columns(x, LW)], m.ox_s.at[d - 1], m.ox_r.at[d - 1], {"x": peer}
        )

    def edges_out(n):
        before, behind = {"z": down, "x": jnp.int32(NX - 1)}, {"z": up, "x": jnp.int32(0)}
        return (
            remote(s.dbp, s.ebn.at[n], m.e_s.at[0], m.e_r.at[0, n], before),
            remote(s.dbn, s.ebp.at[n], m.e_s.at[1], m.e_r.at[1, n], behind),
            remote(s.dxp, s.exn.at[:, columns(n, LW)], m.e_s.at[2], m.e_r.at[2, n], before),
            remote(s.dxn, s.exp.at[:, columns(n, LW)], m.e_s.at[3], m.e_r.at[3, n], behind),
        )

    masked_edges(s.dbcpad, 2 * STATE, map_tap, s.dbp, s.dbn)
    for copy in edges_out(x)[:2]:
        copy.start()
    for k in range(NX):
        for w in range(2):
            lanes = slice(STATE * w, STATE * (w + 1))
            s.dbc[k, :, lanes] = unconvolved(s.dbcpad, k * BLOCK, BLOCK, lanes, map_tap(w)).astype(bf16)
    for d in (2, 1, 3):
        bco_to(d).start()
    own_bco = pltpu.make_async_copy(s.dbc.at[x], s.bco.at[x], m.own.at[6])
    own_bco.start()

    lax.fori_loop(0, NX, input_gradients, 0)
    masked_edges(s.dxpad, LW, input_tap, s.dxp, s.dxn)
    for copy in edges_out(x)[2:]:
        copy.start()
    for k in range(NX):
        for j in range(LH // 2):
            lanes = slice(128 * j, 128 * (j + 1))
            s.dx[k, :, lanes] = unconvolved(s.dxpad, k * BLOCK, BLOCK, lanes, input_tap(j)).astype(bf16)
    for d in (2, 1, 3):
        dxo_to(d).start()
    own_dx = pltpu.make_async_copy(s.dx.at[x], o.dxo.at[:, columns(x, LW)], m.own.at[7])
    own_dx.start()

    own_bco.wait()
    for d in range(1, NX):
        bco_to(d).wait_recv()

    @when(x_last)
    def _():
        for n in range(NX):
            edges_out(n)[0].wait_recv()

    @when(x_first)
    def _():
        for n in range(NX):
            edges_out(n)[1].wait_recv()

    for g in range(GROUPS):
        lanes = slice(2 * STATE * g, 2 * STATE * (g + 1))
        both = s.bco[2 * g].astype(f32) + s.bco[2 * g + 1].astype(f32)
        edge = s.ebp[2 * g].astype(f32) + s.ebp[2 * g + 1].astype(f32)
        s.dmaps[0:EDGE, lanes] = (both[0:EDGE] + edge).astype(bf16)
        s.dmaps[EDGE : BLOCK - EDGE, lanes] = both[EDGE : BLOCK - EDGE].astype(bf16)
        edge = s.ebn[2 * g].astype(f32) + s.ebn[2 * g + 1].astype(f32)
        s.dmaps[BLOCK - EDGE :, lanes] = (both[BLOCK - EDGE :] + edge).astype(bf16)

    order = [4, 3, 5, 2, 6, 1, 7, 0]

    def weight_part(n, core):
        block = lax.rem(y + order[n], NY) * NC + core
        return dot_tn(a.act[:, columns(block, BLOCK)], s.dmaps[...])

    def swap(n):
        return remote(s.part.at[n], s.pair.at[n], m.sw_s.at[n], m.sw_r.at[n], {"c": other})

    for n in range(NY):
        s.part[n] = weight_part(n, other).astype(bf16)
        swap(n).start()
    s.kept[0] = weight_part(0, c)

    def reduced(step, h, way):
        send, recv, to = (m.rr_s, m.rr_r, north) if way > 0 else (m.rl_s, m.rl_r, south)
        out, into = (s.outwr, s.inr) if way > 0 else (s.outwl, s.inl)
        return remote(out.at[step, rows(h)], into.at[step, rows(h)], send.at[step, h], recv.at[step, h], {"y": to})

    def both_cores(n, h):
        return s.kept[n, rows(h)] + s.pair[n, rows(h)].astype(f32)

    def hidden_part(n):
        s_block = n
        o.dhid[:, 128 * n : 128 * (n + 1)] = dot_nt(s.dmaps[...], s.wf[s_block]).astype(bf16)

    for step in range(4):
        for n in ((0,), (1, 2), (3, 4), (5, 6))[step]:
            swap(n).wait_recv()
        for h in range(CUTS):
            for way in (1, -1):
                if step == 0 and not near_side(h, way):
                    continue
                n = order.index((way * (4 - step)) % NY)
                value = both_cores(n, h)
                if step > 1 or (step == 1 and near_side(h, way)):
                    reduced(step - 1, h, way).wait_recv()
                    value = value + (s.inr if way > 0 else s.inl)[step - 1, rows(h)].astype(f32)
                (s.outwr if way > 0 else s.outwl)[step, rows(h)] = value.astype(bf16)
                reduced(step, h, way).start()
        for n in ((1, 2), (3, 4), (5, 6), (7,))[step]:
            s.kept[n] = weight_part(n, c)
        for n in range(4 * step, 4 * step + 4):
            hidden_part(n)
    swap(7).wait_recv()
    for h in range(CUTS):
        value = both_cores(7, h)
        for way in (1, -1):
            reduced(3, h, way).wait_recv()
            value = value + (s.inr if way > 0 else s.inl)[3, rows(h)].astype(f32)
        s.quarter[rows(h)] = value

    strip = BLOCK // NX

    def strip_to(d):
        peer = lax.rem(x + d, NX)
        return remote(
            s.quarter.at[columns(peer, strip)], s.xin.at[d - 1], m.qx_s.at[d - 1], m.qx_r.at[d - 1], {"x": peer}
        )

    for d in (2, 1, 3):
        strip_to(d).start()

    own_dx.wait()
    for d in range(1, NX):
        dxo_to(d).wait_recv()

    @when(x_last)
    def _():
        for n in range(NX):
            edges_out(n)[2].wait_recv()
        at = slice(BLOCK - EDGE, BLOCK)
        o.dxo[at, :] = (o.dxo[at, :].astype(f32) + s.exn[...].astype(f32)).astype(bf16)

    @when(x_first)
    def _():
        for n in range(NX):
            edges_out(n)[3].wait_recv()
        o.dxo[0:EDGE, :] = (o.dxo[0:EDGE, :].astype(f32) + s.exp[...].astype(f32)).astype(bf16)

    strips = s.quarter[columns(x, strip)]
    for d in range(1, NX):
        strip_to(d).wait_recv()
        strips = strips + s.xin[d - 1]
    for i in range(NZ):
        s.piece[i] = strips[8 * (i // 2) : 8 * (i // 2) + 8, 256 * (i % 2) : 256 * (i % 2) + 256]

    def piece_to(d):
        peer = lax.rem(z + d, NZ)
        return remote(s.piece.at[peer], s.zin.at[d - 1], m.qz_s.at[d - 1], m.qz_r.at[d - 1], {"z": peer})

    for d in (4, 3, 5, 2, 6, 1, 7):
        piece_to(d).start()

    met = s.right[NX, 0] * s.left[NX - 1, 1] + s.right[NX, 1] * s.left[NX - 1, 0]
    picks = jnp.concatenate([s.gather[...]] * 2, axis=1)
    crossing_end = dot_nt(picks, jnp.concatenate(parts_of(met, 2), axis=1).astype(bf16))
    after = -jnp.sum(crossing_end, axis=1, keepdims=True)
    for k in range(NX - 1, -1, -1):
        d_rate = jnp.dot(s.dl[k], lower, precision=highest, preferred_element_type=f32) + after
        after = d_rate[:, 0:1]
        d_dt = d_rate * jnp.exp(s.prm[:, 10, :]) + s.dvu[k]
        s.ddt[k] = d_dt / (1.0 + jnp.exp(-(s.dth[k] + s.prm[:, 9, :])))
    for d in range(1, NX):
        dto_to(d).start()
    own_ddt = pltpu.make_async_copy(s.ddt.at[x], s.dto.at[x], m.own.at[8])
    own_ddt.start()

    value = s.piece[z]
    for d in range(1, NZ):
        piece_to(d).wait_recv()
        value = value + s.zin[d - 1]
    s.held[z] = value

    def piece_back(d):
        return remote(s.held.at[z], s.held.at[z], m.gz_s.at[d - 1], m.gz_r.at[d - 1], {"z": lax.rem(z + d, NZ)})

    def piece_from(d):
        source = lax.rem(z - d + NZ, NZ)
        return remote(s.held.at[z], s.held.at[source], m.gz_s.at[d - 1], m.gz_r.at[d - 1], {"z": source})

    for d in (4, 3, 5, 2, 6, 1, 7):
        piece_back(d).start()
    own_ddt.wait()
    for d in range(1, NX):
        dto_to(d).wait_recv()
    for n in range(NX // 2):
        o.dts[16 * n : 16 * n + 16] = jnp.concatenate([s.dto[2 * n], s.dto[2 * n + 1]], axis=0).astype(bf16)
    for d in range(1, NZ):
        piece_from(d).wait_recv()
    own_strip = columns(x, strip)
    strip_total = jnp.concatenate(
        [jnp.concatenate([s.held[2 * i], s.held[2 * i + 1]], axis=1) for i in range(NZ // 2)], axis=0
    )
    for n, out in enumerate((o.dwb, o.dwc)):
        for g in range(GROUPS):
            lane = STATE * (2 * g + n)
            out[own_strip, STATE * g : STATE * (g + 1)] = strip_total[:, lane : lane + STATE]

    def strip_back(n, d):
        at = (o.dwb, o.dwc)[n].at[own_strip]
        return remote(at, at, m.gx_s.at[n, d - 1], m.gx_r.at[n, d - 1], {"x": lax.rem(x + d, NX)})

    def strip_from(n, d):
        source = lax.rem(x - d + NX, NX)
        at = (o.dwb, o.dwc)[n].at[columns(source, strip)]
        return remote(at, at, m.gx_s.at[n, d - 1], m.gx_r.at[n, d - 1], {"x": source})

    for d in (2, 1, 3):
        for n in range(2):
            strip_back(n, d).start()

    for step, h, way in w_steps:
        w_ring(step, h, way).wait_send()
    for h in range(CUTS):
        for n in range(8):
            w_across(n, h).wait_send()
    for which in range(4):
        for n in range(NX):

            @when((x_last, x_first)[which % 2])
            def _():
                edge_in(which, n).wait_send()

    for d in range(1, NX):
        for copy in (x_to(d), dt_to(d), dy_to(d), bc_to(d), bco_to(d), dto_to(d), dxo_to(d), strip_to(d)):
            copy.wait_send()
    for i in range(NZ):

        @unless(jnp.logical_and(mine, z == i))
        def _():
            message(i).wait_send()

    for copy in edges_out(x):
        copy.wait_send()

    def sent(n, carry):
        @unless(last)
        def _():
            going_up(n).wait_send()

        @unless(first)
        def _():
            going_down(n).wait_send()

        return carry

    lax.fori_loop(0, PIECES, sent, 0)
    for n in range(NY):
        swap(n).wait_send()
    for step in range(4):
        for h in range(CUTS):
            for way in (1, -1):
                if step > 0 or near_side(h, way):
                    reduced(step, h, way).wait_send()
    for d in range(1, NZ):
        piece_to(d).wait_send()
        piece_back(d).wait_send()
    for d in range(1, NX):
        for n in range(2):
            strip_from(n, d).wait_recv()
    for d in range(1, NX):
        for n in range(2):
            strip_back(n, d).wait_send()


def whole(*args):
    shapes = (
        jax.ShapeDtypeStruct((BLOCK, INNER), bf16),
        jax.ShapeDtypeStruct((BLOCK, INNER), bf16),
        jax.ShapeDtypeStruct((BLOCK, INNER), bf16),
        jax.ShapeDtypeStruct((HEADS, BLOCK), bf16),
        jax.ShapeDtypeStruct((BLOCK, GROUPS * STATE), f32),
        jax.ShapeDtypeStruct((BLOCK, GROUPS * STATE), f32),
    )
    scratch = [pltpu.VMEM(shape, dtype) for shape, dtype in BUFFERS.values()]
    scratch += [DMA(shape) for shape in SEMAPHORES.values()]
    scalar = pl.BlockSpec(memory_space=pltpu.SMEM)
    return pl.pallas_call(
        kernel,
        out_shape=shapes,
        in_specs=[vmem()] * (len(INPUTS) - 3) + [scalar] * 3,
        out_specs=tuple(vmem() for _ in shapes),
        scratch_shapes=scratch,
        compiler_params=pltpu.CompilerParams(
            collective_id=0, has_side_effects=True, vmem_limit_bytes=VMEM_LIMIT
        ),
        name="mixer_backward",
    )(*args)


def local(
    layer_activity, writer_matrix, reader_matrix, source_unfiltered, switch_raw_signal, saved_result,
    final_adjoint, delta_raw, extra_logdrop, source_filter_coefs, writer_filter_coefs, reader_filter_coefs,
    delta_offset, fading_exponents, direct_factor, rescale_factor,
):
    tokens = layer_activity.shape[1]
    d_gate, d_x, d_hidden, d_dt, d_w_b, d_w_c = whole(
        writer_matrix,
        reader_matrix,
        layer_activity.reshape(tokens, -1),
        source_unfiltered.reshape(tokens, INNER),
        switch_raw_signal.reshape(tokens, INNER),
        saved_result.reshape(tokens, INNER),
        final_adjoint.reshape(tokens, INNER),
        rescale_factor.reshape(1, INNER),
        delta_raw.reshape(tokens, HEADS).T,
        extra_logdrop.reshape(NZ, NX, BLOCK),
        source_filter_coefs,
        writer_filter_coefs,
        reader_filter_coefs,
        delta_offset,
        fading_exponents,
        direct_factor,
    )
    return (
        d_hidden.reshape(1, tokens, -1),
        d_x.reshape(1, tokens, INNER),
        d_gate.reshape(1, tokens, INNER),
        d_dt.T.reshape(1, tokens, HEADS),
        d_w_b,
        d_w_c,
    )


def solution(mesh):
    split = Mesh(mesh.devices.reshape(NZ, NX, NY, NC), ("z", "x", "y", "c"))
    sp, dp = ("z", "x"), ("y", "c")
    in_specs = (
        P(dp, sp, None),
        P(dp, None),
        P(dp, None),
        P(dp, sp, None),
        P(dp, sp, None),
        P(dp, sp, None),
        P(dp, sp, None),
        P(dp, sp, None),
        P(dp, None, sp),
        P(None, sp),
        P(),
        P(),
        P(sp),
        P(sp),
        P(sp),
        P(),
    )
    out_specs = (
        P(dp, sp, None),
        P(dp, sp, None),
        P(dp, sp, None),
        P(dp, sp, None),
        P(dp, None),
        P(dp, None),
    )
    return jax.shard_map(local, mesh=split, in_specs=in_specs, out_specs=out_specs, check_vma=False)
```

```python
import functools

import jax
import jax.numpy as jnp
from jax import lax
from jax.experimental import pallas as pl
from jax.experimental.pallas import tpu as pltpu
from jax.sharding import Mesh
from jax.sharding import PartitionSpec as P

HEADS = 32
HEAD_DIM = 64
STATE = 128
GROUPS = 2
NORM_GROUPS = 8
CONV_K = 5
BLOCK = 128
INNER = 2048
NZ, NX, NY, NC = 8, 4, 8, 2
LH = HEADS // NX
LW = LH * HEAD_DIM
CHUNK = NX * BLOCK
EDGE = 16
EPSILON = 1e-06
VMEM_LIMIT = 60 * 1024 * 1024

f32 = jnp.float32
bf16 = jnp.bfloat16
highest = lax.Precision.HIGHEST
MESH = pl.DeviceIdType.MESH
DMA = pltpu.SemaphoreType.DMA


def vmem():
    return pl.BlockSpec(memory_space=pltpu.VMEM)


def remote(src, dst, send, recv, device):
    return pltpu.make_async_remote_copy(
        src_ref=src, dst_ref=dst, send_sem=send, recv_sem=recv, device_id=device, device_id_type=MESH
    )


def greet(barrier, device):
    pl.semaphore_signal(barrier, inc=1, device_id=device, device_id_type=MESH)


def columns(start, size):
    return pl.ds(pl.multiple_of(start * size, size), size)


def dot(a, b):
    return jnp.dot(a, b, preferred_element_type=f32)


def dot_nt(a, b):
    return lax.dot_general(a, b, (((1,), (1,)), ((), ())), preferred_element_type=f32)


def dot_tn(a, b):
    return lax.dot_general(a, b, (((0,), (0,)), ((), ())), preferred_element_type=f32)


def iota2(shape, dim):
    return lax.broadcasted_iota(jnp.int32, shape, dim)


def parts_of(value, count):
    out = []
    for _ in range(count):
        top = value.astype(bf16).astype(f32)
        out.append(top)
        value = value - top
    return out


def silu_parts(pre):
    gate = 1.0 / (1.0 + jnp.exp(-pre))
    return pre * gate, gate * (1.0 + pre * (1.0 - gate))


def norm_group(group, saved_ref, switch_ref, final_ref, gain_ref, dy_ref, dgate_ref):
    width = INNER // NORM_GROUPS
    cols = slice(group * width, (group + 1) * width)
    saved = saved_ref[:, cols].astype(f32)
    switch = switch_ref[:, cols].astype(f32)
    final = final_ref[:, cols].astype(f32)
    gate = 1.0 / (1.0 + jnp.exp(-switch))
    act = switch * gate
    mixed = saved * act
    scale = lax.rsqrt(jnp.mean(mixed * mixed, axis=-1, keepdims=True) + EPSILON)
    d_normed = final * gain_ref[:, cols]
    inner = jnp.mean(d_normed * mixed, axis=-1, keepdims=True)
    d_mixed = d_normed * scale - mixed * (scale * scale * scale * inner)
    dy_ref[:, cols] = (d_mixed * act).astype(bf16)
    slope = gate * (1.0 + switch * (1.0 - gate))
    dgate_ref[:, cols] = (d_mixed * saved * slope).astype(bf16)


def pair_row(prm_ref, row, j):
    lane = iota2((1, 128), 1)
    return jnp.where(lane < HEAD_DIM, prm_ref[2 * j, row : row + 1, :], prm_ref[2 * j + 1, row : row + 1, :])


def fill_padded(pad_ref, body_ref, prev_ref, next_ref, z):
    pad_ref[pl.ds(0, EDGE)] = jnp.where(z == 0, 0.0, prev_ref[...].astype(f32))
    for k in range(NX):
        pad_ref[pl.ds(EDGE + k * BLOCK, BLOCK)] = body_ref[k].astype(f32)
    pad_ref[pl.ds(EDGE + CHUNK, EDGE)] = jnp.where(z == NZ - 1, 0.0, next_ref[...].astype(f32))


def unconvolved(pad_ref, start, size, lanes, tap_of):
    total = jnp.zeros((size, 128), f32)
    for tap in range(CONV_K):
        total = total + tap_of(tap) * pad_ref[pl.ds(start + 2 * EDGE + 2 - tap, size), lanes]
    return total


BUFFERS = dict(
    w=((BLOCK, 2 * GROUPS * STATE), bf16),
    dt=((HEADS, BLOCK), f32),
    msg=((NZ, 16, BLOCK), f32),
    taps=((8, 2 * STATE), f32),
    dy=((BLOCK, INNER), bf16),
    xh=((NX, BLOCK, LW), bf16),
    dyh=((NX, BLOCK, LW), bf16),
    dth=((NX, LH, BLOCK), f32),
    prm=((LH, 16, BLOCK), f32),
    xp=((EDGE, LW), bf16),
    xn=((EDGE, LW), bf16),
    wf=((NY * NC, BLOCK, 2 * GROUPS * STATE), bf16),
    bc=((BLOCK, 2 * GROUPS * STATE), bf16),
    bch=((NX, BLOCK, 2 * STATE), bf16),
    bp=((EDGE, 2 * STATE), bf16),
    bn=((EDGE, 2 * STATE), bf16),
    three=((48, 3 * LW), bf16),
    wide=((24, LH * BLOCK), bf16),
    gather=((LH, LW), bf16),
    xpad=((CHUNK + 2 * EDGE, LW), f32),
    bcpad=((CHUNK + 2 * EDGE, 2 * STATE), f32),
    v16=((CHUNK, LW), bf16),
    pv16=((CHUNK, LW), bf16),
    qv16=((CHUNK, LW), bf16),
    pdy16=((CHUNK, LW), bf16),
    qdy16=((CHUNK, LW), bf16),
    b16=((CHUNK, STATE), bf16),
    c16=((CHUNK, STATE), bf16),
    u=((CHUNK, LW), f32),
    slope=((CHUNK, LW), f32),
    spread=((CHUNK, 3 * LW), f32),
    bs=((CHUNK, STATE), f32),
    cs=((CHUNK, STATE), f32),
    level=((NX, LH, BLOCK), f32),
    gamma=((NX, 8, LW), f32),
    signed=((NX, BLOCK, BLOCK), f32),
    grid_t=((NX, BLOCK, BLOCK), f32),
    weights=((NX, BLOCK, BLOCK), f32),
    right=((NX + 1, 2, STATE, LW), f32),
    left=((NX, 2, STATE, LW), f32),
    sr=((2, STATE, LW), f32),
    sl=((2, STATE, LW), f32),
    decay=((8, LW), f32),
    outr=((2, STATE, LW), bf16),
    outl=((2, STATE, LW), bf16),
    cr=((2, STATE, LW), bf16),
    cl=((2, STATE, LW), bf16),
    dv=((CHUNK, LW), f32),
    dl=((NX, LH, BLOCK), f32),
    dvu=((NX, LH, BLOCK), f32),
    dxpad=((CHUNK + 4 * EDGE, LW), f32),
    dbcpad=((CHUNK + 4 * EDGE, 2 * STATE), f32),
    dx=((NX, BLOCK, LW), bf16),
    dxp=((EDGE, LW), bf16),
    dxn=((EDGE, LW), bf16),
    dbc=((NX, BLOCK, 2 * STATE), bf16),
    dbp=((EDGE, 2 * STATE), bf16),
    dbn=((EDGE, 2 * STATE), bf16),
    ddt=((NX, LH, BLOCK), f32),
    dto=((NX, LH, BLOCK), f32),
    exp=((EDGE, INNER), bf16),
    exn=((EDGE, INNER), bf16),
    bco=((NX, BLOCK, 2 * STATE), bf16),
    ebp=((NX, EDGE, 2 * STATE), bf16),
    ebn=((NX, EDGE, 2 * STATE), bf16),
    dmaps=((BLOCK, 2 * GROUPS * STATE), bf16),
    part=((NY, BLOCK, 2 * GROUPS * STATE), bf16),
    kept=((NY, BLOCK, 2 * GROUPS * STATE), f32),
    pair=((NY, BLOCK, 2 * GROUPS * STATE), bf16),
    inr=((4, BLOCK, 2 * GROUPS * STATE), bf16),
    inl=((4, BLOCK, 2 * GROUPS * STATE), bf16),
    outwr=((4, BLOCK, 2 * GROUPS * STATE), bf16),
    outwl=((4, BLOCK, 2 * GROUPS * STATE), bf16),
    quarter=((BLOCK, 2 * GROUPS * STATE), f32),
    quarter16=((BLOCK, 2 * GROUPS * STATE), bf16),
    piece=((NZ, 16, 128), f32),
    piece16=((NZ, 16, 128), bf16),
    xin=((NX - 1, BLOCK // NX, 2 * GROUPS * STATE), bf16),
    zin=((NZ - 1, 16, 128), bf16),
    held=((NZ, 16, 128), bf16),
    summed=((BLOCK, 2 * GROUPS * STATE), bf16),
)
PIECES = 16
EARLY = 6
LAG = 8
CUTS = 4
UNITS = NX * LH // 2
SEMAPHORES = dict(
    own=(12,), x_s=(3,), x_r=(3,), y_s=(3,), y_r=(3,), t_s=(3,), t_r=(3,), m_s=(8,), m_r=(8,),
    h_s=(4, NX), h_r=(4,), wr_s=(4, CUTS), wr_r=(4, CUTS), wl_s=(4, CUTS), wl_r=(4, CUTS),
    wp_s=(8, CUTS), wp_r=(8, CUTS),
    b_s=(3,), b_r=(3,), up_s=(PIECES,), up_r=(PIECES,), dn_s=(PIECES,), dn_r=(PIECES,),
    ox_s=(3,), ox_r=(3,), ob_s=(3,), ob_r=(3,), ot_s=(3,), ot_r=(3,), e_s=(4,), e_r=(4, NX),
    sw_s=(8,), sw_r=(8,), rr_s=(4, CUTS), rr_r=(4, CUTS), rl_s=(4, CUTS), rl_r=(4, CUTS),
    qx_s=(3,), qx_r=(3,), qz_s=(7,), qz_r=(7,), gz_s=(7,), gz_r=(7,), gx_s=(3,), gx_r=(3,),
)


class Named:
    def __init__(self, names, refs):
        for name, ref in zip(names, refs, strict=True):
            setattr(self, name, ref)


INPUTS = (
    "wb", "wc", "act", "x", "switch", "saved", "final", "gain", "delta", "drops",
    "source_taps", "writer_taps", "reader_taps", "offset", "fading", "skip",
)
OUTPUTS = ("dgate", "dxo", "dhid", "dts", "dwb", "dwc")


def kernel(*refs):
    n_in, n_out, n_buf = len(INPUTS), len(OUTPUTS), len(BUFFERS)
    a = Named(INPUTS, refs[:n_in])
    o = Named(OUTPUTS, refs[n_in : n_in + n_out])
    s = Named(BUFFERS, refs[n_in + n_out : n_in + n_out + n_buf])
    m = Named(SEMAPHORES, refs[n_in + n_out + n_buf :])
    z, x, y, c = (lax.axis_index(name) for name in ("z", "x", "y", "c"))
    cut = BLOCK // CUTS
    up, down = lax.rem(z + 1, NZ), lax.rem(z + NZ - 1, NZ)
    north, south = lax.rem(y + 1, NY), lax.rem(y + NY - 1, NY)
    other = 1 - c
    head = z * NX + x
    dest = z // 2
    slot = lax.rem(head, LH)
    mine = dest == x
    first, last = z == 0, z == NZ - 1
    x_first, x_last = x == 0, x == NX - 1

    def when(condition):
        return pl.when(condition)

    def unless(condition):
        return pl.when(jnp.logical_not(condition))

    def sender_of(i):
        return 2 * x + i // NX, i % NX

    def is_me(i):
        sz, sx = sender_of(i)
        return jnp.logical_and(sz == z, sx == x)

    @when(first)
    def _():
        s.cr[...] = jnp.zeros_like(s.cr)

    @when(last)
    def _():
        s.cl[...] = jnp.zeros_like(s.cl)

    @unless(x_first)
    def _():
        s.exp[...] = jnp.zeros_like(s.exp)
        s.ebp[...] = jnp.zeros_like(s.ebp)

    @unless(x_last)
    def _():
        s.exn[...] = jnp.zeros_like(s.exn)
        s.ebn[...] = jnp.zeros_like(s.ebn)

    gather_w = []
    for g in range(GROUPS):
        lanes = slice(STATE * g, STATE * (g + 1))
        for n, ref in enumerate((a.wb, a.wc)):
            to = slice(STATE * (2 * g + n), STATE * (2 * g + n + 1))
            gather_w.append(pltpu.make_async_copy(ref.at[:, lanes], s.w.at[:, to], m.own.at[2 * g + n]))
    for copy in gather_w:
        copy.start()
    s.dt[...] = a.delta[...].astype(f32)
    row_taps = jnp.concatenate([a.source_taps[...]] * 2, axis=1)
    for i in range(NZ):
        s.msg[i, 0:4] = a.drops[i]
        s.msg[i, 4:9] = row_taps
        for n, ref in enumerate((a.offset, a.fading, a.skip)):
            s.msg[i, 9 + n : 10 + n] = jnp.full((1, BLOCK), ref[0], f32)
    low_group = x < NX // 2
    for n, ref in enumerate((a.writer_taps, a.reader_taps)):
        s.taps[0:CONV_K, STATE * n : STATE * (n + 1)] = jnp.where(low_group, ref[:, :STATE], ref[:, STATE:])
    for copy in gather_w:
        copy.wait()

    barrier = pltpu.get_barrier_semaphore()
    for d in range(1, NX):
        greet(barrier, {"x": lax.rem(x + d, NX)})
    for d in range(1, NZ):
        greet(barrier, {"z": lax.rem(z + d, NZ)})
    greet(barrier, {"y": north})
    greet(barrier, {"y": south})
    greet(barrier, {"c": other})
    for i in range(LH):

        @unless(is_me(i))
        def _():
            sz, sx = sender_of(i)
            greet(barrier, {"z": sz, "x": sx})

    greet(barrier, {"z": down, "x": jnp.int32(NX - 1)})
    greet(barrier, {"z": up, "x": jnp.int32(0)})

    @when(x_first)
    def _():
        for n in range(NX):
            greet(barrier, {"z": down, "x": jnp.int32(n)})

    @when(x_last)
    def _():
        for n in range(NX):
            greet(barrier, {"z": up, "x": jnp.int32(n)})

    pl.semaphore_wait(
        barrier,
        NX - 1 + NZ - 1 + 3 + NZ + 2
        - mine.astype(jnp.int32) + NX * x_first.astype(jnp.int32) + NX * x_last.astype(jnp.int32),
    )

    def rows(h):
        return pl.ds(h * cut, cut)

    def w_ring(step, h, way):
        block = lax.rem(y - way * step + NY, NY) * NC + c
        src = s.w.at[rows(h)] if step == 0 else s.wf.at[block, rows(h)]
        send, recv, to = (m.wr_s, m.wr_r, north) if way > 0 else (m.wl_s, m.wl_r, south)
        return remote(src, s.wf.at[block, rows(h)], send.at[step, h], recv.at[step, h], {"y": to})

    def w_offset(n):
        return 0 if n == 0 else (-n if n < 5 else n - 4)

    def w_across(n, h):
        block = lax.rem(y + w_offset(n) + NY, NY) * NC + c
        src = s.w.at[rows(h)] if n == 0 else s.wf.at[block, rows(h)]
        return remote(src, s.wf.at[block, rows(h)], m.wp_s.at[n, h], m.wp_r.at[n, h], {"c": other})

    def near_side(h, way):
        return (h < CUTS // 2) == (way == 1)

    w_steps = [
        (step, h, way) for step in range(4) for h in range(CUTS) for way in (1, -1) if step < 3 or near_side(h, way)
    ]
    for step, h, way in w_steps[: 2 * CUTS]:
        w_ring(step, h, way).start()
    own = [
        pltpu.make_async_copy(s.w, s.wf.at[y * NC + c], m.own.at[0]),
        pltpu.make_async_copy(a.x.at[:, columns(x, LW)], s.xh.at[x], m.own.at[1]),
        pltpu.make_async_copy(s.dt.at[columns(x, LH)], s.dth.at[x], m.own.at[2]),
    ]
    for copy in own:
        copy.start()
    for h in range(CUTS):
        w_across(0, h).start()

    def edge_in(which, n):
        tail, lead = pl.ds(BLOCK - EDGE, EDGE), pl.ds(0, EDGE)
        lanes, pair_lanes = columns(n, LW), columns(n // 2, 2 * STATE)
        src, dst, to = (
            (a.x.at[tail, lanes], s.xp, up),
            (a.x.at[lead, lanes], s.xn, down),
            (s.bc.at[tail, pair_lanes], s.bp, up),
            (s.bc.at[lead, pair_lanes], s.bn, down),
        )[which]
        return remote(src, dst, m.h_s.at[which, n], m.h_r.at[which], {"z": to, "x": jnp.int32(n)})

    def edges_start(pair):
        for n in range(NX):

            @when(x_last)
            def _():
                edge_in(2 * pair, n).start()

            @when(x_first)
            def _():
                edge_in(2 * pair + 1, n).start()

    edges_start(0)

    def x_to(d):
        peer = lax.rem(x + d, NX)
        return remote(
            a.x.at[:, columns(peer, LW)], s.xh.at[x], m.x_s.at[d - 1], m.x_r.at[d - 1], {"x": peer}
        )

    def dt_to(d):
        peer = lax.rem(x + d, NX)
        return remote(
            s.dt.at[columns(peer, LH)], s.dth.at[x], m.t_s.at[d - 1], m.t_r.at[d - 1], {"x": peer}
        )

    def dy_to(d):
        peer = lax.rem(x + d, NX)
        return remote(
            s.dy.at[:, columns(peer, LW)], s.dyh.at[x], m.y_s.at[d - 1], m.y_r.at[d - 1], {"x": peer}
        )

    def message(i):
        return remote(
            s.msg.at[i], s.prm.at[slot], m.m_s.at[i], m.m_r.at[slot], {"z": jnp.int32(i), "x": dest}
        )

    for d in range(1, NX):
        x_to(d).start()
        dt_to(d).start()
    keep = pltpu.make_async_copy(s.msg.at[z], s.prm.at[slot], m.own.at[3])
    for i in range(NZ):

        @unless(jnp.logical_and(mine, z == i))
        def _():
            message(i).start()

    @when(mine)
    def _():
        keep.start()

    for group in range(NORM_GROUPS):
        norm_group(group, a.saved, a.switch, a.final, a.gain, s.dy, o.dgate)
    for d in range(1, NX):
        dy_to(d).start()
    own_dy = pltpu.make_async_copy(s.dy.at[:, columns(x, LW)], s.dyh.at[x], m.own.at[4])
    own_dy.start()

    def projected(n, core):
        block = lax.rem(y + w_offset(n) + NY, NY) * NC + core
        return dot(a.act[:, columns(block, BLOCK)], s.wf[block])

    def inputs_of(k):
        for j in range(LH // 2):
            lanes = slice(128 * j, 128 * (j + 1))
            pre = jnp.zeros((BLOCK, 128), f32)
            for tap in range(CONV_K):
                pre = pre + pair_row(s.prm, 4 + tap, j) * s.xpad[pl.ds(k * BLOCK + EDGE - 2 + tap, BLOCK), lanes]
            at = pl.ds(k * BLOCK, BLOCK)
            s.u[at, lanes], s.slope[at, lanes] = silu_parts(pre)

    own[0].wait()
    maps = projected(0, c)
    for step in range(4):
        for h in range(CUTS):
            for way in (1, -1):
                if step == 3 and not near_side(h, way):
                    continue
                w_ring(step, h, way).wait_recv()
                following = (step + 1, h, way)
                if following in w_steps:
                    w_ring(*following).start()
                w_across(1 + step if way == 1 or step == 3 else 5 + step, h).start()
        if step < 3:
            maps = maps + projected(1 + step, c) + projected(5 + step, c)
        for n in ((0,), (1, 5), (2, 6), (3, 7))[step]:
            for h in range(CUTS):
                w_across(n, h).wait_recv()
            maps = maps + projected(n, other)
        if step == 2:
            for d in range(1, NX):
                x_to(d).wait_recv()
            own[1].wait()
            edge_in(0, x).wait_recv()
            edge_in(1, x).wait_recv()
            for i in range(LH):

                @unless(is_me(i))
                def _():
                    sz, sx = sender_of(i)
                    remote(s.msg.at[i], s.prm.at[i], m.m_s.at[i], m.m_r.at[i], {"z": sz, "x": sx}).wait_recv()

            @when(mine)
            def _():
                keep.wait()

            fill_padded(s.xpad, s.xh, s.xp, s.xn, z)
            for k in range(NX):
                inputs_of(k)
    maps = maps + projected(4, c)
    for h in range(CUTS):
        w_across(4, h).wait_recv()
    maps = maps + projected(4, other)
    s.bc[...] = maps.astype(bf16)

    def bc_to(d):
        peer = lax.rem(x + d, NX)
        return remote(
            s.bc.at[:, columns(peer // 2, 2 * STATE)], s.bch.at[x], m.b_s.at[d - 1], m.b_r.at[d - 1], {"x": peer}
        )

    for d in range(1, NX):
        bc_to(d).start()
    own_bc = pltpu.make_async_copy(s.bc.at[:, columns(x // 2, 2 * STATE)], s.bch.at[x], m.own.at[5])
    own_bc.start()
    edges_start(1)

    r, cc = iota2((48, 3 * LW), 0), iota2((48, 3 * LW), 1)
    s.three[...] = jnp.logical_and(
        r // 16 == cc // LW, jnp.bitwise_and(r, 7) == jnp.bitwise_and(cc, LW - 1) // HEAD_DIM
    ).astype(bf16)
    r, cc = iota2((24, LH * BLOCK), 0), iota2((24, LH * BLOCK), 1)
    s.wide[...] = (jnp.bitwise_and(r, 7) == cc // BLOCK).astype(bf16)
    s.gather[...] = (iota2((LH, LW), 1) // HEAD_DIM == iota2((LH, LW), 0)).astype(bf16)
    for pad in (s.dxpad, s.dbcpad):
        pad[pl.ds(0, 2 * EDGE)] = jnp.zeros((2 * EDGE, pad.shape[1]), f32)
        pad[pl.ds(2 * EDGE + CHUNK, 2 * EDGE)] = jnp.zeros((2 * EDGE, pad.shape[1]), f32)

    for d in range(1, NX):
        dt_to(d).wait_recv()
        dy_to(d).wait_recv()
    own[2].wait()
    own_dy.wait()
    row, col = iota2((BLOCK, BLOCK), 0), iota2((BLOCK, BLOCK), 1)
    upper = (row <= col).astype(f32)
    lower = (row >= col).astype(f32)
    sign = (row > col).astype(f32) - (row < col).astype(f32)
    low_half = iota2((BLOCK, 128), 1) < HEAD_DIM
    head_row = iota2((8, BLOCK), 0)

    for k in range(NX):
        at = pl.ds(k * BLOCK, BLOCK)
        dt = jax.nn.softplus(s.dth[k] + s.prm[:, 9, :])
        rate = dt * jnp.exp(s.prm[:, 10, :]) + s.prm[:, k, :]
        level = jnp.dot(rate, upper, precision=highest, preferred_element_type=f32)
        total = level[:, BLOCK - 1 : BLOCK]
        s.level[k] = level
        stack = jnp.concatenate(
            parts_of(dt, 2) + parts_of(jnp.exp(-level), 2) + parts_of(jnp.exp(level - total), 2), axis=0
        )
        spread = dot_tn(stack.astype(bf16), s.three[...])
        s.spread[at] = spread
        s.gamma[k] = jnp.broadcast_to(spread[BLOCK - 1 : BLOCK, LW : 2 * LW], (8, LW))
        for j in range(LH // 2):
            lanes = slice(128 * j, 128 * (j + 1))
            pe = spread[:, LW + 128 * j : LW + 128 * (j + 1)]
            qe = spread[:, 2 * LW + 128 * j : 2 * LW + 128 * (j + 1)]
            v = s.u[at, lanes] * spread[:, lanes]
            dy = s.dyh[k, :, lanes].astype(f32)
            s.v16[at, lanes] = v.astype(bf16)
            s.pv16[at, lanes], s.qv16[at, lanes] = (pe * v).astype(bf16), (qe * v).astype(bf16)
            s.pdy16[at, lanes], s.qdy16[at, lanes] = (pe * dy).astype(bf16), (qe * dy).astype(bf16)

    own_bc.wait()
    for d in range(1, NX):
        bc_to(d).wait_recv()
    edge_in(2, x).wait_recv()
    edge_in(3, x).wait_recv()
    fill_padded(s.bcpad, s.bch, s.bp, s.bn, z)
    s.decay[...] = jnp.ones_like(s.decay)
    for k in range(NX):
        at = pl.ds(k * BLOCK, BLOCK)
        for which, held, slopes in ((0, s.b16, s.bs), (1, s.c16, s.cs)):
            lanes = slice(which * STATE, (which + 1) * STATE)
            pre = jnp.zeros((BLOCK, STATE), f32)
            for tap in range(CONV_K):
                pre = pre + s.taps[tap : tap + 1, lanes] * s.bcpad[pl.ds(k * BLOCK + EDGE - 2 + tap, BLOCK), lanes]
            value, slopes[at] = silu_parts(pre)
            held[at] = value.astype(bf16)
        b, cc = s.b16[at], s.c16[at]
        kvr, cdr = dot_tn(b, s.qv16[at]), dot_tn(cc, s.qdy16[at])
        kvl, cdl = dot_tn(b, s.pv16[at]), dot_tn(cc, s.pdy16[at])
        s.right[k + 1, 0], s.right[k + 1, 1] = kvr, cdr
        if k > 0:
            s.left[k - 1, 0], s.left[k - 1, 1] = kvl, cdl
        if k == 0:
            s.sr[0], s.sr[1], s.sl[0], s.sl[1] = kvr, cdr, kvl, cdl
        else:
            g, before = s.gamma[k, 0:1], s.decay[0:1]
            s.sr[0] = s.sr[0] * g + kvr
            s.sr[1] = s.sr[1] * g + cdr
            s.sl[0] = s.sl[0] + before * kvl
            s.sl[1] = s.sl[1] + before * cdl
        s.decay[...] = s.decay[...] * s.gamma[k]

    def piece(n):
        return n // 8, pl.ds(pl.multiple_of(lax.rem(n // 4, 2) * 64, 64), 64), columns(lax.rem(n, 4), 128)

    def going_up(n):
        return remote(s.outr.at[piece(n)], s.cr.at[piece(n)], m.up_s.at[n], m.up_r.at[n], {"z": up})

    def going_down(n):
        return remote(s.outl.at[piece(n)], s.cl.at[piece(n)], m.dn_s.at[n], m.dn_r.at[n], {"z": down})

    def scan_step(t):
        n = t - LAG * z

        @when(jnp.logical_and(n >= 0, n < PIECES))
        def _():
            @unless(first)
            def _():
                going_up(n).wait_recv()

            @unless(last)
            def _():
                at = piece(n)
                s.outr[at] = (s.cr[at].astype(f32) * s.decay[0:1, at[2]] + s.sr[at]).astype(bf16)
                going_up(n).start()

        i = t - LAG * (NZ - 1 - z)

        @when(jnp.logical_and(i >= 0, i < PIECES))
        def _():
            @unless(last)
            def _():
                going_down(i).wait_recv()

            @unless(first)
            def _():
                at = piece(i)
                s.outl[at] = (s.cl[at].astype(f32) * s.decay[0:1, at[2]] + s.sl[at]).astype(bf16)
                going_down(i).start()

    def within(k, j):
        at = pl.ds(pl.multiple_of(k * BLOCK, BLOCK), BLOCK)
        lanes = columns(j, 128)
        parts = jnp.concatenate(parts_of(s.level[k], 3), axis=0).astype(bf16)
        level_cols = dot_tn(parts, s.wide[:, columns(j, 256)])
        vj, dyj = s.v16[at, lanes], s.dyh[k, :, lanes]
        signed, grid_t = s.signed[k], s.grid_t[k]
        halves = []
        weights = s.weights[k]
        dl = s.dl[k]
        for i in range(2):
            h = 2 * j + i
            near = jnp.exp(-jnp.abs(level_cols[:, 128 * i : 128 * (i + 1)] - s.level[k, pl.ds(h, 1), :]))
            keep_half = low_half if i == 0 else jnp.logical_not(low_half)
            shared = dot_nt(jnp.where(keep_half, dyj, jnp.zeros_like(dyj)), vj) * near
            weights = weights + shared
            crossing = (shared * signed).astype(bf16)
            pick = (head_row == h).astype(bf16)
            dl = dl + dot(pick, crossing) - dot_nt(pick, crossing)
            halves.append(dot((grid_t * near).astype(bf16), dyj))
        s.weights[k] = weights
        s.dl[k] = dl
        s.dv[at, lanes] = jnp.where(low_half, halves[0], halves[1])

    s.weights[...] = jnp.zeros_like(s.weights)
    s.dl[...] = jnp.zeros_like(s.dl)
    for k in range(NX):
        at = pl.ds(k * BLOCK, BLOCK)
        b, cc = s.b16[at], s.c16[at]
        s.signed[k] = dot_nt(cc, b) * sign
        s.grid_t[k] = dot_nt(b, cc)

    far = z // (NZ // 2)
    near_end = z * (1 - far) + (NZ - 1 - z) * far
    early = EARLY * near_end
    between = LAG * near_end + PIECES
    until = LAG * (NZ - 1 - near_end)

    def unit(n):
        within(n // (LH // 2), lax.rem(n, LH // 2))

    def steps(t, carry):
        scan_step(t)

        @when(jnp.logical_and(t < early, t < UNITS))
        def _():
            unit(t)

        @when(jnp.logical_and(t >= between, t < until))
        def _():
            def two(i, inner):
                n = early + 2 * (t - between) + i

                @when(n < UNITS)
                def _():
                    unit(n)

                return inner

            lax.fori_loop(0, 2, two, 0)

        return carry

    lax.fori_loop(0, PIECES + LAG * (NZ - 1), steps, 0)

    def rest(n, carry):
        done = jnp.where(until > between, early + 2 * (until - between), early)

        @when(n >= done)
        def _():
            unit(n)

        return carry

    lax.fori_loop(0, UNITS, rest, 0)

    s.right[0, 0], s.right[0, 1] = s.cr[0].astype(f32), s.cr[1].astype(f32)
    s.left[NX - 1, 0], s.left[NX - 1, 1] = s.cl[0].astype(f32), s.cl[1].astype(f32)
    for k in range(NX):
        g = s.gamma[k, 0:1]
        s.right[k + 1, 0] = s.right[k + 1, 0] + s.right[k, 0] * g
        s.right[k + 1, 1] = s.right[k + 1, 1] + s.right[k, 1] * g
    for k in range(NX - 2, -1, -1):
        g = s.gamma[k + 1, 0:1]
        s.left[k, 0] = s.left[k, 0] + g * s.left[k + 1, 0]
        s.left[k, 1] = s.left[k, 1] + g * s.left[k + 1, 1]

    def map_gradients(k, carry):
        at = pl.ds(pl.multiple_of(k * BLOCK, BLOCK), BLOCK)
        padded = pl.ds(pl.multiple_of(2 * EDGE + k * BLOCK, EDGE), BLOCK)
        weights = s.weights[k].astype(bf16)
        dc = dot(weights, s.b16[at])
        db = dot_tn(weights, s.c16[at])
        dc = dc + dot_nt(s.pdy16[at], s.right[k, 0].astype(bf16)) + dot_nt(s.qdy16[at], s.left[k, 0].astype(bf16))
        db = db + dot_nt(s.qv16[at], s.left[k, 1].astype(bf16)) + dot_nt(s.pv16[at], s.right[k, 1].astype(bf16))
        s.dbcpad[padded, 0:STATE] = db * s.bs[at]
        s.dbcpad[padded, STATE : 2 * STATE] = dc * s.cs[at]
        return carry

    lax.fori_loop(0, NX, map_gradients, 0)

    def input_gradients(k, carry):
        at = pl.ds(pl.multiple_of(k * BLOCK, BLOCK), BLOCK)
        padded = pl.ds(pl.multiple_of(2 * EDGE + k * BLOCK, EDGE), BLOCK)
        b, cc = s.b16[at], s.c16[at]
        dl = s.dl[k]
        dvu = jnp.zeros((8, BLOCK), f32)
        for j in range(LH // 2):
            lanes = slice(128 * j, 128 * (j + 1))
            kvr, cdr = s.right[k, 0, :, lanes].astype(bf16), s.right[k, 1, :, lanes].astype(bf16)
            kvl, cdl = s.left[k, 0, :, lanes].astype(bf16), s.left[k, 1, :, lanes].astype(bf16)
            pe = s.spread[at, LW + 128 * j : LW + 128 * (j + 1)]
            qe = s.spread[at, 2 * LW + 128 * j : 2 * LW + 128 * (j + 1)]
            from_later, from_earlier = dot(b, cdl), dot(b, cdr)
            pv, qv, pdy, qdy = s.pv16[at, lanes], s.qv16[at, lanes], s.pdy16[at, lanes], s.qdy16[at, lanes]
            dv = s.dv[at, lanes] + qe * from_later + pe * from_earlier
            cross = (
                qv.astype(f32) * from_later - pv.astype(f32) * from_earlier
                + qdy.astype(f32) * dot(cc, kvl) - pdy.astype(f32) * dot(cc, kvr)
            )
            picks = jnp.concatenate([s.gather[:, lanes]] * 2, axis=1)
            dl = dl + dot_nt(picks, jnp.concatenate(parts_of(cross, 2), axis=1).astype(bf16))
            dvu = dvu + dot_nt(picks, jnp.concatenate(parts_of(dv * s.u[at, lanes], 2), axis=1).astype(bf16))
            du = dv * s.spread[at, lanes] + pair_row(s.prm, 11, j) * s.dyh[k, :, lanes].astype(f32)
            s.dxpad[padded, lanes] = du * s.slope[at, lanes]
        s.dl[k], s.dvu[k] = dl, dvu
        return carry

    def masked_edges(pad, width, tap_for, before_ref, behind_ref):
        for w in range(width // 128):
            lanes = slice(128 * w, 128 * (w + 1))
            before = unconvolved(pad, -EDGE, EDGE, lanes, tap_for(w))
            behind = unconvolved(pad, CHUNK, EDGE, lanes, tap_for(w))
            before_ref[:, lanes] = jnp.where(first, 0.0, before).astype(bf16)
            behind_ref[:, lanes] = jnp.where(last, 0.0, behind).astype(bf16)

    def map_tap(w):
        return lambda tap: s.taps[tap : tap + 1, 128 * w : 128 * (w + 1)]

    def input_tap(j):
        return lambda tap: pair_row(s.prm, 4 + tap, j)

    def bco_to(d):
        peer = lax.rem(x + d, NX)
        return remote(s.dbc.at[peer], s.bco.at[x], m.ob_s.at[d - 1], m.ob_r.at[d - 1], {"x": peer})

    def dto_to(d):
        peer = lax.rem(x + d, NX)
        return remote(s.ddt.at[peer], s.dto.at[x], m.ot_s.at[d - 1], m.ot_r.at[d - 1], {"x": peer})

    def dxo_to(d):
        peer = lax.rem(x + d, NX)
        return remote(
            s.dx.at[peer], o.dxo.at[:, columns(x, LW)], m.ox_s.at[d - 1], m.ox_r.at[d - 1], {"x": peer}
        )

    def edges_out(n):
        before, behind = {"z": down, "x": jnp.int32(NX - 1)}, {"z": up, "x": jnp.int32(0)}
        return (
            remote(s.dbp, s.ebn.at[n], m.e_s.at[0], m.e_r.at[0, n], before),
            remote(s.dbn, s.ebp.at[n], m.e_s.at[1], m.e_r.at[1, n], behind),
            remote(s.dxp, s.exn.at[:, columns(n, LW)], m.e_s.at[2], m.e_r.at[2, n], before),
            remote(s.dxn, s.exp.at[:, columns(n, LW)], m.e_s.at[3], m.e_r.at[3, n], behind),
        )

    masked_edges(s.dbcpad, 2 * STATE, map_tap, s.dbp, s.dbn)
    for copy in edges_out(x)[:2]:
        copy.start()
    for k in range(NX):
        for w in range(2):
            lanes = slice(STATE * w, STATE * (w + 1))
            s.dbc[k, :, lanes] = unconvolved(s.dbcpad, k * BLOCK, BLOCK, lanes, map_tap(w)).astype(bf16)
    for d in (2, 1, 3):
        bco_to(d).start()
    own_bco = pltpu.make_async_copy(s.dbc.at[x], s.bco.at[x], m.own.at[6])
    own_bco.start()

    lax.fori_loop(0, NX, input_gradients, 0)
    masked_edges(s.dxpad, LW, input_tap, s.dxp, s.dxn)
    for copy in edges_out(x)[2:]:
        copy.start()
    for k in range(NX):
        for j in range(LH // 2):
            lanes = slice(128 * j, 128 * (j + 1))
            s.dx[k, :, lanes] = unconvolved(s.dxpad, k * BLOCK, BLOCK, lanes, input_tap(j)).astype(bf16)
    for d in (2, 1, 3):
        dxo_to(d).start()
    own_dx = pltpu.make_async_copy(s.dx.at[x], o.dxo.at[:, columns(x, LW)], m.own.at[7])
    own_dx.start()

    own_bco.wait()
    for d in range(1, NX):
        bco_to(d).wait_recv()

    @when(x_last)
    def _():
        for n in range(NX):
            edges_out(n)[0].wait_recv()

    @when(x_first)
    def _():
        for n in range(NX):
            edges_out(n)[1].wait_recv()

    for g in range(GROUPS):
        lanes = slice(2 * STATE * g, 2 * STATE * (g + 1))
        both = s.bco[2 * g].astype(f32) + s.bco[2 * g + 1].astype(f32)
        edge = s.ebp[2 * g].astype(f32) + s.ebp[2 * g + 1].astype(f32)
        s.dmaps[0:EDGE, lanes] = (both[0:EDGE] + edge).astype(bf16)
        s.dmaps[EDGE : BLOCK - EDGE, lanes] = both[EDGE : BLOCK - EDGE].astype(bf16)
        edge = s.ebn[2 * g].astype(f32) + s.ebn[2 * g + 1].astype(f32)
        s.dmaps[BLOCK - EDGE :, lanes] = (both[BLOCK - EDGE :] + edge).astype(bf16)

    order = [4, 3, 5, 2, 6, 1, 7, 0]

    def weight_part(n, core):
        block = lax.rem(y + order[n], NY) * NC + core
        return dot_tn(a.act[:, columns(block, BLOCK)], s.dmaps[...])

    def swap(n):
        return remote(s.part.at[n], s.pair.at[n], m.sw_s.at[n], m.sw_r.at[n], {"c": other})

    for n in range(NY):
        s.part[n] = weight_part(n, other).astype(bf16)
        swap(n).start()
    s.kept[0] = weight_part(0, c)

    def reduced(step, h, way):
        send, recv, to = (m.rr_s, m.rr_r, north) if way > 0 else (m.rl_s, m.rl_r, south)
        out, into = (s.outwr, s.inr) if way > 0 else (s.outwl, s.inl)
        return remote(out.at[step, rows(h)], into.at[step, rows(h)], send.at[step, h], recv.at[step, h], {"y": to})

    def both_cores(n, h):
        return s.kept[n, rows(h)] + s.pair[n, rows(h)].astype(f32)

    def hidden_part(n):
        s_block = n
        o.dhid[:, 128 * n : 128 * (n + 1)] = dot_nt(s.dmaps[...], s.wf[s_block]).astype(bf16)

    for step in range(4):
        for n in ((0,), (1, 2), (3, 4), (5, 6))[step]:
            swap(n).wait_recv()
        for h in range(CUTS):
            for way in (1, -1):
                if step == 0 and not near_side(h, way):
                    continue
                n = order.index((way * (4 - step)) % NY)
                value = both_cores(n, h)
                if step > 1 or (step == 1 and near_side(h, way)):
                    reduced(step - 1, h, way).wait_recv()
                    value = value + (s.inr if way > 0 else s.inl)[step - 1, rows(h)].astype(f32)
                (s.outwr if way > 0 else s.outwl)[step, rows(h)] = value.astype(bf16)
                reduced(step, h, way).start()
        for n in ((1, 2), (3, 4), (5, 6), (7,))[step]:
            s.kept[n] = weight_part(n, c)
        for n in range(4 * step, 4 * step + 4):
            hidden_part(n)
    swap(7).wait_recv()
    for h in range(CUTS):
        value = both_cores(7, h)
        for way in (1, -1):
            reduced(3, h, way).wait_recv()
            value = value + (s.inr if way > 0 else s.inl)[3, rows(h)].astype(f32)
        s.quarter[rows(h)] = value
        s.quarter16[rows(h)] = value.astype(bf16)

    strip = BLOCK // NX

    def strip_to(d):
        peer = lax.rem(x + d, NX)
        return remote(
            s.quarter16.at[columns(peer, strip)], s.xin.at[d - 1], m.qx_s.at[d - 1], m.qx_r.at[d - 1], {"x": peer}
        )

    for d in (2, 1, 3):
        strip_to(d).start()

    own_dx.wait()
    for d in range(1, NX):
        dxo_to(d).wait_recv()

    @when(x_last)
    def _():
        for n in range(NX):
            edges_out(n)[2].wait_recv()
        at = slice(BLOCK - EDGE, BLOCK)
        o.dxo[at, :] = (o.dxo[at, :].astype(f32) + s.exn[...].astype(f32)).astype(bf16)

    @when(x_first)
    def _():
        for n in range(NX):
            edges_out(n)[3].wait_recv()
        o.dxo[0:EDGE, :] = (o.dxo[0:EDGE, :].astype(f32) + s.exp[...].astype(f32)).astype(bf16)

    strips = s.quarter[columns(x, strip)]
    for d in range(1, NX):
        strip_to(d).wait_recv()
        strips = strips + s.xin[d - 1].astype(f32)
    for i in range(NZ):
        part = strips[16 * (i // 4) : 16 * (i // 4) + 16, 128 * (i % 4) : 128 * (i % 4) + 128]
        s.piece[i], s.piece16[i] = part, part.astype(bf16)

    def piece_to(d):
        peer = lax.rem(z + d, NZ)
        return remote(s.piece16.at[peer], s.zin.at[d - 1], m.qz_s.at[d - 1], m.qz_r.at[d - 1], {"z": peer})

    for d in (4, 3, 5, 2, 6, 1, 7):
        piece_to(d).start()

    met = s.right[NX, 0] * s.left[NX - 1, 1] + s.right[NX, 1] * s.left[NX - 1, 0]
    picks = jnp.concatenate([s.gather[...]] * 2, axis=1)
    crossing_end = dot_nt(picks, jnp.concatenate(parts_of(met, 2), axis=1).astype(bf16))
    after = -jnp.sum(crossing_end, axis=1, keepdims=True)
    for k in range(NX - 1, -1, -1):
        d_rate = jnp.dot(s.dl[k], lower, precision=highest, preferred_element_type=f32) + after
        after = d_rate[:, 0:1]
        d_dt = d_rate * jnp.exp(s.prm[:, 10, :]) + s.dvu[k]
        s.ddt[k] = d_dt / (1.0 + jnp.exp(-(s.dth[k] + s.prm[:, 9, :])))
    for d in range(1, NX):
        dto_to(d).start()
    own_ddt = pltpu.make_async_copy(s.ddt.at[x], s.dto.at[x], m.own.at[8])
    own_ddt.start()

    value = s.piece[z]
    for d in range(1, NZ):
        piece_to(d).wait_recv()
        value = value + s.zin[d - 1].astype(f32)
    s.held[z] = value.astype(bf16)

    def piece_back(d):
        return remote(s.held.at[z], s.held.at[z], m.gz_s.at[d - 1], m.gz_r.at[d - 1], {"z": lax.rem(z + d, NZ)})

    def piece_from(d):
        source = lax.rem(z - d + NZ, NZ)
        return remote(s.held.at[z], s.held.at[source], m.gz_s.at[d - 1], m.gz_r.at[d - 1], {"z": source})

    for d in (4, 3, 5, 2, 6, 1, 7):
        piece_back(d).start()
    own_ddt.wait()
    for d in range(1, NX):
        dto_to(d).wait_recv()
    for n in range(NX // 2):
        o.dts[16 * n : 16 * n + 16] = jnp.concatenate([s.dto[2 * n], s.dto[2 * n + 1]], axis=0).astype(bf16)
    for d in range(1, NZ):
        piece_from(d).wait_recv()
    own_strip = columns(x, strip)
    for i in range(NZ):
        at = pl.ds(pl.multiple_of(x * strip + 16 * (i // 4), 16), 16)
        s.summed[at, 128 * (i % 4) : 128 * (i % 4) + 128] = s.held[i]

    def strip_back(d):
        at = s.summed.at[own_strip]
        return remote(at, at, m.gx_s.at[d - 1], m.gx_r.at[d - 1], {"x": lax.rem(x + d, NX)})

    def strip_from(d):
        source = lax.rem(x - d + NX, NX)
        at = s.summed.at[columns(source, strip)]
        return remote(at, at, m.gx_s.at[d - 1], m.gx_r.at[d - 1], {"x": source})

    for d in (2, 1, 3):
        strip_back(d).start()

    for step, h, way in w_steps:
        w_ring(step, h, way).wait_send()
    for h in range(CUTS):
        for n in range(8):
            w_across(n, h).wait_send()
    for which in range(4):
        for n in range(NX):

            @when((x_last, x_first)[which % 2])
            def _():
                edge_in(which, n).wait_send()

    for d in range(1, NX):
        for copy in (x_to(d), dt_to(d), dy_to(d), bc_to(d), bco_to(d), dto_to(d), dxo_to(d), strip_to(d)):
            copy.wait_send()
    for i in range(NZ):

        @unless(jnp.logical_and(mine, z == i))
        def _():
            message(i).wait_send()

    for copy in edges_out(x):
        copy.wait_send()

    def sent(n, carry):
        @unless(last)
        def _():
            going_up(n).wait_send()

        @unless(first)
        def _():
            going_down(n).wait_send()

        return carry

    lax.fori_loop(0, PIECES, sent, 0)
    for n in range(NY):
        swap(n).wait_send()
    for step in range(4):
        for h in range(CUTS):
            for way in (1, -1):
                if step > 0 or near_side(h, way):
                    reduced(step, h, way).wait_send()
    for d in range(1, NZ):
        piece_to(d).wait_send()
        piece_back(d).wait_send()
    for d in range(1, NX):
        strip_from(d).wait_recv()
    for n, out in enumerate((o.dwb, o.dwc)):
        for g in range(GROUPS):
            lane = STATE * (2 * g + n)
            out[:, STATE * g : STATE * (g + 1)] = s.summed[:, lane : lane + STATE].astype(f32)
    for d in range(1, NX):
        strip_back(d).wait_send()


def whole(*args):
    shapes = (
        jax.ShapeDtypeStruct((BLOCK, INNER), bf16),
        jax.ShapeDtypeStruct((BLOCK, INNER), bf16),
        jax.ShapeDtypeStruct((BLOCK, INNER), bf16),
        jax.ShapeDtypeStruct((HEADS, BLOCK), bf16),
        jax.ShapeDtypeStruct((BLOCK, GROUPS * STATE), f32),
        jax.ShapeDtypeStruct((BLOCK, GROUPS * STATE), f32),
    )
    scratch = [pltpu.VMEM(shape, dtype) for shape, dtype in BUFFERS.values()]
    scratch += [DMA(shape) for shape in SEMAPHORES.values()]
    scalar = pl.BlockSpec(memory_space=pltpu.SMEM)
    return pl.pallas_call(
        kernel,
        out_shape=shapes,
        in_specs=[vmem()] * (len(INPUTS) - 3) + [scalar] * 3,
        out_specs=tuple(vmem() for _ in shapes),
        scratch_shapes=scratch,
        compiler_params=pltpu.CompilerParams(
            collective_id=0, has_side_effects=True, vmem_limit_bytes=VMEM_LIMIT
        ),
        name="mixer_backward",
    )(*args)


def deliver_kernel(*refs):
    half = len(refs) // 2
    for given, out in zip(refs[:half], refs[half:], strict=True):
        out[...] = given[...]


def delivered(arrays):
    return pl.pallas_call(
        deliver_kernel,
        out_shape=tuple(jax.ShapeDtypeStruct(v.shape, v.dtype) for v in arrays),
        in_specs=[vmem()] * len(arrays),
        out_specs=tuple(vmem() for _ in arrays),
        name="deliver",
    )(*arrays)


def local(
    layer_activity, writer_matrix, reader_matrix, source_unfiltered, switch_raw_signal, saved_result,
    final_adjoint, delta_raw, extra_logdrop, source_filter_coefs, writer_filter_coefs, reader_filter_coefs,
    delta_offset, fading_exponents, direct_factor, rescale_factor,
):
    tokens = layer_activity.shape[1]
    outputs = whole(
        writer_matrix,
        reader_matrix,
        layer_activity.reshape(tokens, -1),
        source_unfiltered.reshape(tokens, INNER),
        switch_raw_signal.reshape(tokens, INNER),
        saved_result.reshape(tokens, INNER),
        final_adjoint.reshape(tokens, INNER),
        rescale_factor.reshape(1, INNER),
        delta_raw.reshape(tokens, HEADS).T,
        extra_logdrop.reshape(NZ, NX, BLOCK),
        source_filter_coefs,
        writer_filter_coefs,
        reader_filter_coefs,
        delta_offset,
        fading_exponents,
        direct_factor,
    )
    d_gate, d_x, d_hidden, d_dt, d_w_b, d_w_c = delivered(outputs)
    return (
        d_hidden.reshape(1, tokens, -1),
        d_x.reshape(1, tokens, INNER),
        d_gate.reshape(1, tokens, INNER),
        d_dt.T.reshape(1, tokens, HEADS),
        d_w_b,
        d_w_c,
    )


def solution(mesh):
    split = Mesh(mesh.devices.reshape(NZ, NX, NY, NC), ("z", "x", "y", "c"))
    sp, dp = ("z", "x"), ("y", "c")
    in_specs = (
        P(dp, sp, None),
        P(dp, None),
        P(dp, None),
        P(dp, sp, None),
        P(dp, sp, None),
        P(dp, sp, None),
        P(dp, sp, None),
        P(dp, sp, None),
        P(dp, None, sp),
        P(None, sp),
        P(),
        P(),
        P(sp),
        P(sp),
        P(sp),
        P(),
    )
    out_specs = (
        P(dp, sp, None),
        P(dp, sp, None),
        P(dp, sp, None),
        P(dp, sp, None),
        P(dp, None),
        P(dp, None),
    )
    return jax.shard_map(local, mesh=split, in_specs=in_specs, out_specs=out_specs, check_vma=False)
```

```python
import functools

import jax
import jax.numpy as jnp
from jax import lax
from jax.experimental import pallas as pl
from jax.experimental.pallas import tpu as pltpu
from jax.sharding import Mesh
from jax.sharding import PartitionSpec as P

HEADS = 32
HEAD_DIM = 64
STATE = 128
GROUPS = 2
NORM_GROUPS = 8
CONV_K = 5
BLOCK = 128
INNER = 2048
NZ, NX, NY, NC = 8, 4, 8, 2
LH = HEADS // NX
LW = LH * HEAD_DIM
CHUNK = NX * BLOCK
EDGE = 16
EPSILON = 1e-06
VMEM_LIMIT = 60 * 1024 * 1024

f32 = jnp.float32
bf16 = jnp.bfloat16
highest = lax.Precision.HIGHEST
MESH = pl.DeviceIdType.MESH
DMA = pltpu.SemaphoreType.DMA


def vmem():
    return pl.BlockSpec(memory_space=pltpu.VMEM)


def remote(src, dst, send, recv, device):
    return pltpu.make_async_remote_copy(
        src_ref=src, dst_ref=dst, send_sem=send, recv_sem=recv, device_id=device, device_id_type=MESH
    )


def greet(barrier, device):
    pl.semaphore_signal(barrier, inc=1, device_id=device, device_id_type=MESH)


def columns(start, size):
    return pl.ds(pl.multiple_of(start * size, size), size)


def dot(a, b):
    return jnp.dot(a, b, preferred_element_type=f32)


def dot_nt(a, b):
    return lax.dot_general(a, b, (((1,), (1,)), ((), ())), preferred_element_type=f32)


def dot_tn(a, b):
    return lax.dot_general(a, b, (((0,), (0,)), ((), ())), preferred_element_type=f32)


def iota2(shape, dim):
    return lax.broadcasted_iota(jnp.int32, shape, dim)


def parts_of(value, count):
    out = []
    for _ in range(count):
        top = value.astype(bf16).astype(f32)
        out.append(top)
        value = value - top
    return out


def silu_parts(pre):
    gate = 1.0 / (1.0 + jnp.exp(-pre))
    return pre * gate, gate * (1.0 + pre * (1.0 - gate))


def norm_group(group, saved_ref, switch_ref, final_ref, gain_ref, dy_ref, dgate_ref):
    width = INNER // NORM_GROUPS
    cols = slice(group * width, (group + 1) * width)
    saved = saved_ref[:, cols].astype(f32)
    switch = switch_ref[:, cols].astype(f32)
    final = final_ref[:, cols].astype(f32)
    gate = 1.0 / (1.0 + jnp.exp(-switch))
    act = switch * gate
    mixed = saved * act
    scale = lax.rsqrt(jnp.mean(mixed * mixed, axis=-1, keepdims=True) + EPSILON)
    d_normed = final * gain_ref[:, cols]
    inner = jnp.mean(d_normed * mixed, axis=-1, keepdims=True)
    d_mixed = d_normed * scale - mixed * (scale * scale * scale * inner)
    dy_ref[:, cols] = (d_mixed * act).astype(bf16)
    slope = gate * (1.0 + switch * (1.0 - gate))
    dgate_ref[:, cols] = (d_mixed * saved * slope).astype(bf16)


def pair_row(prm_ref, row, j):
    lane = iota2((1, 128), 1)
    return jnp.where(lane < HEAD_DIM, prm_ref[2 * j, row : row + 1, :], prm_ref[2 * j + 1, row : row + 1, :])


def fill_padded(pad_ref, body_ref, prev_ref, next_ref, z):
    pad_ref[pl.ds(0, EDGE)] = jnp.where(z == 0, 0.0, prev_ref[...].astype(f32))
    for k in range(NX):
        pad_ref[pl.ds(EDGE + k * BLOCK, BLOCK)] = body_ref[k].astype(f32)
    pad_ref[pl.ds(EDGE + CHUNK, EDGE)] = jnp.where(z == NZ - 1, 0.0, next_ref[...].astype(f32))


def unconvolved(pad_ref, start, size, lanes, tap_of):
    total = jnp.zeros((size, 128), f32)
    for tap in range(CONV_K):
        total = total + tap_of(tap) * pad_ref[pl.ds(start + 2 * EDGE + 2 - tap, size), lanes]
    return total


STREAMED = ("x", "saved", "switch", "final", "act")
BUFFERS = dict(
    **{f"{name}_in": ((BLOCK, INNER), bf16) for name in STREAMED},
    dgate_out=((BLOCK, INNER), bf16),
    dxo_out=((BLOCK, INNER), bf16),
    dhid_out=((BLOCK, INNER), bf16),
    w=((BLOCK, 2 * GROUPS * STATE), bf16),
    dt=((HEADS, BLOCK), f32),
    msg=((NZ, 16, BLOCK), f32),
    taps=((8, 2 * STATE), f32),
    dy=((BLOCK, INNER), bf16),
    xh=((NX, BLOCK, LW), bf16),
    dyh=((NX, BLOCK, LW), bf16),
    dth=((NX, LH, BLOCK), f32),
    prm=((LH, 16, BLOCK), f32),
    xp=((EDGE, LW), bf16),
    xn=((EDGE, LW), bf16),
    wf=((NY * NC, BLOCK, 2 * GROUPS * STATE), bf16),
    bc=((BLOCK, 2 * GROUPS * STATE), bf16),
    bch=((NX, BLOCK, 2 * STATE), bf16),
    bp=((EDGE, 2 * STATE), bf16),
    bn=((EDGE, 2 * STATE), bf16),
    three=((48, 3 * LW), bf16),
    wide=((24, LH * BLOCK), bf16),
    gather=((LH, LW), bf16),
    xpad=((CHUNK + 2 * EDGE, LW), f32),
    bcpad=((CHUNK + 2 * EDGE, 2 * STATE), f32),
    v16=((CHUNK, LW), bf16),
    pv16=((CHUNK, LW), bf16),
    qv16=((CHUNK, LW), bf16),
    pdy16=((CHUNK, LW), bf16),
    qdy16=((CHUNK, LW), bf16),
    b16=((CHUNK, STATE), bf16),
    c16=((CHUNK, STATE), bf16),
    u=((CHUNK, LW), f32),
    slope=((CHUNK, LW), f32),
    spread=((CHUNK, 3 * LW), f32),
    bs=((CHUNK, STATE), f32),
    cs=((CHUNK, STATE), f32),
    level=((NX, LH, BLOCK), f32),
    gamma=((NX, 8, LW), f32),
    signed=((NX, BLOCK, BLOCK), f32),
    grid_t=((NX, BLOCK, BLOCK), f32),
    weights=((NX, BLOCK, BLOCK), f32),
    right=((NX + 1, 2, STATE, LW), f32),
    left=((NX, 2, STATE, LW), f32),
    sr=((2, STATE, LW), f32),
    sl=((2, STATE, LW), f32),
    decay=((8, LW), f32),
    outr=((2, STATE, LW), bf16),
    outl=((2, STATE, LW), bf16),
    cr=((2, STATE, LW), bf16),
    cl=((2, STATE, LW), bf16),
    dv=((CHUNK, LW), f32),
    dl=((NX, LH, BLOCK), f32),
    dvu=((NX, LH, BLOCK), f32),
    dxpad=((CHUNK + 4 * EDGE, LW), f32),
    dbcpad=((CHUNK + 4 * EDGE, 2 * STATE), f32),
    dx=((NX, BLOCK, LW), bf16),
    dxp=((EDGE, LW), bf16),
    dxn=((EDGE, LW), bf16),
    dbc=((NX, BLOCK, 2 * STATE), bf16),
    dbp=((EDGE, 2 * STATE), bf16),
    dbn=((EDGE, 2 * STATE), bf16),
    ddt=((NX, LH, BLOCK), f32),
    dto=((NX, LH, BLOCK), f32),
    exp=((EDGE, INNER), bf16),
    exn=((EDGE, INNER), bf16),
    bco=((NX, BLOCK, 2 * STATE), bf16),
    ebp=((NX, EDGE, 2 * STATE), bf16),
    ebn=((NX, EDGE, 2 * STATE), bf16),
    dmaps=((BLOCK, 2 * GROUPS * STATE), bf16),
    part=((NY, BLOCK, 2 * GROUPS * STATE), bf16),
    kept=((NY, BLOCK, 2 * GROUPS * STATE), f32),
    pair=((NY, BLOCK, 2 * GROUPS * STATE), bf16),
    inr=((4, BLOCK, 2 * GROUPS * STATE), bf16),
    inl=((4, BLOCK, 2 * GROUPS * STATE), bf16),
    outwr=((4, BLOCK, 2 * GROUPS * STATE), bf16),
    outwl=((4, BLOCK, 2 * GROUPS * STATE), bf16),
    quarter=((BLOCK, 2 * GROUPS * STATE), f32),
    quarter16=((BLOCK, 2 * GROUPS * STATE), bf16),
    piece=((NZ, 16, 128), f32),
    piece16=((NZ, 16, 128), bf16),
    xin=((NX - 1, BLOCK // NX, 2 * GROUPS * STATE), bf16),
    zin=((NZ - 1, 16, 128), bf16),
    held=((NZ, 16, 128), bf16),
    summed=((BLOCK, 2 * GROUPS * STATE), bf16),
)
PIECES = 16
EARLY = 6
LAG = 8
CUTS = 4
UNITS = NX * LH // 2
SEMAPHORES = dict(
    own=(12,), big=(8,), x_s=(3,), x_r=(3,), y_s=(3,), y_r=(3,), t_s=(3,), t_r=(3,), m_s=(8,), m_r=(8,),
    h_s=(4, NX), h_r=(4,), wr_s=(4, CUTS), wr_r=(4, CUTS), wl_s=(4, CUTS), wl_r=(4, CUTS),
    wp_s=(8, CUTS), wp_r=(8, CUTS),
    b_s=(3,), b_r=(3,), up_s=(PIECES,), up_r=(PIECES,), dn_s=(PIECES,), dn_r=(PIECES,),
    ox_s=(3,), ox_r=(3,), ob_s=(3,), ob_r=(3,), ot_s=(3,), ot_r=(3,), e_s=(4,), e_r=(4, NX),
    sw_s=(8,), sw_r=(8,), rr_s=(4, CUTS), rr_r=(4, CUTS), rl_s=(4, CUTS), rl_r=(4, CUTS),
    qx_s=(3,), qx_r=(3,), qz_s=(7,), qz_r=(7,), gz_s=(7,), gz_r=(7,), gx_s=(3,), gx_r=(3,),
)


class Named:
    def __init__(self, names, refs):
        for name, ref in zip(names, refs, strict=True):
            setattr(self, name, ref)


INPUTS = (
    "wb", "wc", "act", "x", "switch", "saved", "final", "gain", "delta", "drops",
    "source_taps", "writer_taps", "reader_taps", "offset", "fading", "skip",
)
OUTPUTS = ("dgate", "dxo", "dhid", "dts", "dwb", "dwc")


def kernel(*refs):
    n_in, n_out, n_buf = len(INPUTS), len(OUTPUTS), len(BUFFERS)
    a = Named(INPUTS, refs[:n_in])
    o = Named(OUTPUTS, refs[n_in : n_in + n_out])
    s = Named(BUFFERS, refs[n_in + n_out : n_in + n_out + n_buf])
    m = Named(SEMAPHORES, refs[n_in + n_out + n_buf :])
    z, x, y, c = (lax.axis_index(name) for name in ("z", "x", "y", "c"))
    cut = BLOCK // CUTS
    up, down = lax.rem(z + 1, NZ), lax.rem(z + NZ - 1, NZ)
    north, south = lax.rem(y + 1, NY), lax.rem(y + NY - 1, NY)
    other = 1 - c
    head = z * NX + x
    dest = z // 2
    slot = lax.rem(head, LH)
    mine = dest == x
    first, last = z == 0, z == NZ - 1
    x_first, x_last = x == 0, x == NX - 1

    def when(condition):
        return pl.when(condition)

    def unless(condition):
        return pl.when(jnp.logical_not(condition))

    def sender_of(i):
        return 2 * x + i // NX, i % NX

    def is_me(i):
        sz, sx = sender_of(i)
        return jnp.logical_and(sz == z, sx == x)

    @when(first)
    def _():
        s.cr[...] = jnp.zeros_like(s.cr)

    @when(last)
    def _():
        s.cl[...] = jnp.zeros_like(s.cl)

    @unless(x_first)
    def _():
        s.exp[...] = jnp.zeros_like(s.exp)
        s.ebp[...] = jnp.zeros_like(s.ebp)

    @unless(x_last)
    def _():
        s.exn[...] = jnp.zeros_like(s.exn)
        s.ebn[...] = jnp.zeros_like(s.ebn)

    loads = {}
    for n, name in enumerate(STREAMED):
        held_here = getattr(s, f"{name}_in")
        loads[name] = pltpu.make_async_copy(getattr(a, name), held_here, m.big.at[n])
        loads[name].start()
        setattr(a, name, held_here)
    stores = [
        pltpu.make_async_copy(s.dgate_out, o.dgate, m.big.at[5]),
        pltpu.make_async_copy(s.dhid_out, o.dhid, m.big.at[6]),
        pltpu.make_async_copy(s.dxo_out, o.dxo, m.big.at[7]),
    ]

    gather_w = []
    for g in range(GROUPS):
        lanes = slice(STATE * g, STATE * (g + 1))
        for n, ref in enumerate((a.wb, a.wc)):
            to = slice(STATE * (2 * g + n), STATE * (2 * g + n + 1))
            gather_w.append(pltpu.make_async_copy(ref.at[:, lanes], s.w.at[:, to], m.own.at[2 * g + n]))
    for copy in gather_w:
        copy.start()
    s.dt[...] = a.delta[...].astype(f32)
    row_taps = jnp.concatenate([a.source_taps[...]] * 2, axis=1)
    for i in range(NZ):
        s.msg[i, 0:4] = a.drops[i]
        s.msg[i, 4:9] = row_taps
        for n, ref in enumerate((a.offset, a.fading, a.skip)):
            s.msg[i, 9 + n : 10 + n] = jnp.full((1, BLOCK), ref[0], f32)
    low_group = x < NX // 2
    for n, ref in enumerate((a.writer_taps, a.reader_taps)):
        s.taps[0:CONV_K, STATE * n : STATE * (n + 1)] = jnp.where(low_group, ref[:, :STATE], ref[:, STATE:])
    for copy in gather_w:
        copy.wait()

    barrier = pltpu.get_barrier_semaphore()
    for d in range(1, NX):
        greet(barrier, {"x": lax.rem(x + d, NX)})
    for d in range(1, NZ):
        greet(barrier, {"z": lax.rem(z + d, NZ)})
    greet(barrier, {"y": north})
    greet(barrier, {"y": south})
    greet(barrier, {"c": other})
    for i in range(LH):

        @unless(is_me(i))
        def _():
            sz, sx = sender_of(i)
            greet(barrier, {"z": sz, "x": sx})

    greet(barrier, {"z": down, "x": jnp.int32(NX - 1)})
    greet(barrier, {"z": up, "x": jnp.int32(0)})

    @when(x_first)
    def _():
        for n in range(NX):
            greet(barrier, {"z": down, "x": jnp.int32(n)})

    @when(x_last)
    def _():
        for n in range(NX):
            greet(barrier, {"z": up, "x": jnp.int32(n)})

    pl.semaphore_wait(
        barrier,
        NX - 1 + NZ - 1 + 3 + NZ + 2
        - mine.astype(jnp.int32) + NX * x_first.astype(jnp.int32) + NX * x_last.astype(jnp.int32),
    )

    def rows(h):
        return pl.ds(h * cut, cut)

    def w_ring(step, h, way):
        block = lax.rem(y - way * step + NY, NY) * NC + c
        src = s.w.at[rows(h)] if step == 0 else s.wf.at[block, rows(h)]
        send, recv, to = (m.wr_s, m.wr_r, north) if way > 0 else (m.wl_s, m.wl_r, south)
        return remote(src, s.wf.at[block, rows(h)], send.at[step, h], recv.at[step, h], {"y": to})

    def w_offset(n):
        return 0 if n == 0 else (-n if n < 5 else n - 4)

    def w_across(n, h):
        block = lax.rem(y + w_offset(n) + NY, NY) * NC + c
        src = s.w.at[rows(h)] if n == 0 else s.wf.at[block, rows(h)]
        return remote(src, s.wf.at[block, rows(h)], m.wp_s.at[n, h], m.wp_r.at[n, h], {"c": other})

    def near_side(h, way):
        return (h < CUTS // 2) == (way == 1)

    w_steps = [
        (step, h, way) for step in range(4) for h in range(CUTS) for way in (1, -1) if step < 3 or near_side(h, way)
    ]
    for step, h, way in w_steps[: 2 * CUTS]:
        w_ring(step, h, way).start()
    loads["x"].wait()
    own = [
        pltpu.make_async_copy(s.w, s.wf.at[y * NC + c], m.own.at[0]),
        pltpu.make_async_copy(a.x.at[:, columns(x, LW)], s.xh.at[x], m.own.at[1]),
        pltpu.make_async_copy(s.dt.at[columns(x, LH)], s.dth.at[x], m.own.at[2]),
    ]
    for copy in own:
        copy.start()
    for h in range(CUTS):
        w_across(0, h).start()

    def edge_in(which, n):
        tail, lead = pl.ds(BLOCK - EDGE, EDGE), pl.ds(0, EDGE)
        lanes, pair_lanes = columns(n, LW), columns(n // 2, 2 * STATE)
        src, dst, to = (
            (a.x.at[tail, lanes], s.xp, up),
            (a.x.at[lead, lanes], s.xn, down),
            (s.bc.at[tail, pair_lanes], s.bp, up),
            (s.bc.at[lead, pair_lanes], s.bn, down),
        )[which]
        return remote(src, dst, m.h_s.at[which, n], m.h_r.at[which], {"z": to, "x": jnp.int32(n)})

    def edges_start(pair):
        for n in range(NX):

            @when(x_last)
            def _():
                edge_in(2 * pair, n).start()

            @when(x_first)
            def _():
                edge_in(2 * pair + 1, n).start()

    edges_start(0)

    def x_to(d):
        peer = lax.rem(x + d, NX)
        return remote(
            a.x.at[:, columns(peer, LW)], s.xh.at[x], m.x_s.at[d - 1], m.x_r.at[d - 1], {"x": peer}
        )

    def dt_to(d):
        peer = lax.rem(x + d, NX)
        return remote(
            s.dt.at[columns(peer, LH)], s.dth.at[x], m.t_s.at[d - 1], m.t_r.at[d - 1], {"x": peer}
        )

    def dy_to(d):
        peer = lax.rem(x + d, NX)
        return remote(
            s.dy.at[:, columns(peer, LW)], s.dyh.at[x], m.y_s.at[d - 1], m.y_r.at[d - 1], {"x": peer}
        )

    def message(i):
        return remote(
            s.msg.at[i], s.prm.at[slot], m.m_s.at[i], m.m_r.at[slot], {"z": jnp.int32(i), "x": dest}
        )

    for d in range(1, NX):
        x_to(d).start()
        dt_to(d).start()
    keep = pltpu.make_async_copy(s.msg.at[z], s.prm.at[slot], m.own.at[3])
    for i in range(NZ):

        @unless(jnp.logical_and(mine, z == i))
        def _():
            message(i).start()

    @when(mine)
    def _():
        keep.start()

    for name in STREAMED[1:]:
        loads[name].wait()
    for group in range(NORM_GROUPS):
        norm_group(group, a.saved, a.switch, a.final, a.gain, s.dy, s.dgate_out)
    for d in range(1, NX):
        dy_to(d).start()
    own_dy = pltpu.make_async_copy(s.dy.at[:, columns(x, LW)], s.dyh.at[x], m.own.at[4])
    own_dy.start()
    stores[0].start()

    def projected(n, core):
        block = lax.rem(y + w_offset(n) + NY, NY) * NC + core
        return dot(a.act[:, columns(block, BLOCK)], s.wf[block])

    def inputs_of(k):
        for j in range(LH // 2):
            lanes = slice(128 * j, 128 * (j + 1))
            pre = jnp.zeros((BLOCK, 128), f32)
            for tap in range(CONV_K):
                pre = pre + pair_row(s.prm, 4 + tap, j) * s.xpad[pl.ds(k * BLOCK + EDGE - 2 + tap, BLOCK), lanes]
            at = pl.ds(k * BLOCK, BLOCK)
            s.u[at, lanes], s.slope[at, lanes] = silu_parts(pre)

    own[0].wait()
    maps = projected(0, c)
    for step in range(4):
        for h in range(CUTS):
            for way in (1, -1):
                if step == 3 and not near_side(h, way):
                    continue
                w_ring(step, h, way).wait_recv()
                following = (step + 1, h, way)
                if following in w_steps:
                    w_ring(*following).start()
                w_across(1 + step if way == 1 or step == 3 else 5 + step, h).start()
        if step < 3:
            maps = maps + projected(1 + step, c) + projected(5 + step, c)
        for n in ((0,), (1, 5), (2, 6), (3, 7))[step]:
            for h in range(CUTS):
                w_across(n, h).wait_recv()
            maps = maps + projected(n, other)
        if step == 2:
            for d in range(1, NX):
                x_to(d).wait_recv()
            own[1].wait()
            edge_in(0, x).wait_recv()
            edge_in(1, x).wait_recv()
            for i in range(LH):

                @unless(is_me(i))
                def _():
                    sz, sx = sender_of(i)
                    remote(s.msg.at[i], s.prm.at[i], m.m_s.at[i], m.m_r.at[i], {"z": sz, "x": sx}).wait_recv()

            @when(mine)
            def _():
                keep.wait()

            fill_padded(s.xpad, s.xh, s.xp, s.xn, z)
            for k in range(NX):
                inputs_of(k)
    maps = maps + projected(4, c)
    for h in range(CUTS):
        w_across(4, h).wait_recv()
    maps = maps + projected(4, other)
    s.bc[...] = maps.astype(bf16)

    def bc_to(d):
        peer = lax.rem(x + d, NX)
        return remote(
            s.bc.at[:, columns(peer // 2, 2 * STATE)], s.bch.at[x], m.b_s.at[d - 1], m.b_r.at[d - 1], {"x": peer}
        )

    for d in (2, 1, 3):
        bc_to(d).start()
    own_bc = pltpu.make_async_copy(s.bc.at[:, columns(x // 2, 2 * STATE)], s.bch.at[x], m.own.at[5])
    own_bc.start()
    edges_start(1)

    r, cc = iota2((48, 3 * LW), 0), iota2((48, 3 * LW), 1)
    s.three[...] = jnp.logical_and(
        r // 16 == cc // LW, jnp.bitwise_and(r, 7) == jnp.bitwise_and(cc, LW - 1) // HEAD_DIM
    ).astype(bf16)
    r, cc = iota2((24, LH * BLOCK), 0), iota2((24, LH * BLOCK), 1)
    s.wide[...] = (jnp.bitwise_and(r, 7) == cc // BLOCK).astype(bf16)
    s.gather[...] = (iota2((LH, LW), 1) // HEAD_DIM == iota2((LH, LW), 0)).astype(bf16)
    for pad in (s.dxpad, s.dbcpad):
        pad[pl.ds(0, 2 * EDGE)] = jnp.zeros((2 * EDGE, pad.shape[1]), f32)
        pad[pl.ds(2 * EDGE + CHUNK, 2 * EDGE)] = jnp.zeros((2 * EDGE, pad.shape[1]), f32)

    for d in range(1, NX):
        dt_to(d).wait_recv()
        dy_to(d).wait_recv()
    own[2].wait()
    own_dy.wait()
    row, col = iota2((BLOCK, BLOCK), 0), iota2((BLOCK, BLOCK), 1)
    upper = (row <= col).astype(f32)
    lower = (row >= col).astype(f32)
    sign = (row > col).astype(f32) - (row < col).astype(f32)
    low_half = iota2((BLOCK, 128), 1) < HEAD_DIM
    head_row = iota2((8, BLOCK), 0)

    for k in range(NX):
        at = pl.ds(k * BLOCK, BLOCK)
        dt = jax.nn.softplus(s.dth[k] + s.prm[:, 9, :])
        rate = dt * jnp.exp(s.prm[:, 10, :]) + s.prm[:, k, :]
        level = jnp.dot(rate, upper, precision=highest, preferred_element_type=f32)
        total = level[:, BLOCK - 1 : BLOCK]
        s.level[k] = level
        stack = jnp.concatenate(
            parts_of(dt, 2) + parts_of(jnp.exp(-level), 2) + parts_of(jnp.exp(level - total), 2), axis=0
        )
        spread = dot_tn(stack.astype(bf16), s.three[...])
        s.spread[at] = spread
        s.gamma[k] = jnp.broadcast_to(spread[BLOCK - 1 : BLOCK, LW : 2 * LW], (8, LW))
        for j in range(LH // 2):
            lanes = slice(128 * j, 128 * (j + 1))
            pe = spread[:, LW + 128 * j : LW + 128 * (j + 1)]
            qe = spread[:, 2 * LW + 128 * j : 2 * LW + 128 * (j + 1)]
            v = s.u[at, lanes] * spread[:, lanes]
            dy = s.dyh[k, :, lanes].astype(f32)
            s.v16[at, lanes] = v.astype(bf16)
            s.pv16[at, lanes], s.qv16[at, lanes] = (pe * v).astype(bf16), (qe * v).astype(bf16)
            s.pdy16[at, lanes], s.qdy16[at, lanes] = (pe * dy).astype(bf16), (qe * dy).astype(bf16)

    own_bc.wait()
    for d in range(1, NX):
        bc_to(d).wait_recv()
    edge_in(2, x).wait_recv()
    edge_in(3, x).wait_recv()
    fill_padded(s.bcpad, s.bch, s.bp, s.bn, z)
    s.decay[...] = jnp.ones_like(s.decay)
    for k in range(NX):
        at = pl.ds(k * BLOCK, BLOCK)
        for which, held, slopes in ((0, s.b16, s.bs), (1, s.c16, s.cs)):
            lanes = slice(which * STATE, (which + 1) * STATE)
            pre = jnp.zeros((BLOCK, STATE), f32)
            for tap in range(CONV_K):
                pre = pre + s.taps[tap : tap + 1, lanes] * s.bcpad[pl.ds(k * BLOCK + EDGE - 2 + tap, BLOCK), lanes]
            value, slopes[at] = silu_parts(pre)
            held[at] = value.astype(bf16)
        b, cc = s.b16[at], s.c16[at]
        kvr, cdr = dot_tn(b, s.qv16[at]), dot_tn(cc, s.qdy16[at])
        kvl, cdl = dot_tn(b, s.pv16[at]), dot_tn(cc, s.pdy16[at])
        s.right[k + 1, 0], s.right[k + 1, 1] = kvr, cdr
        if k > 0:
            s.left[k - 1, 0], s.left[k - 1, 1] = kvl, cdl
        if k == 0:
            s.sr[0], s.sr[1], s.sl[0], s.sl[1] = kvr, cdr, kvl, cdl
        else:
            g, before = s.gamma[k, 0:1], s.decay[0:1]
            s.sr[0] = s.sr[0] * g + kvr
            s.sr[1] = s.sr[1] * g + cdr
            s.sl[0] = s.sl[0] + before * kvl
            s.sl[1] = s.sl[1] + before * cdl
        s.decay[...] = s.decay[...] * s.gamma[k]

    def piece(n):
        return n // 8, pl.ds(pl.multiple_of(lax.rem(n // 4, 2) * 64, 64), 64), columns(lax.rem(n, 4), 128)

    def going_up(n):
        return remote(s.outr.at[piece(n)], s.cr.at[piece(n)], m.up_s.at[n], m.up_r.at[n], {"z": up})

    def going_down(n):
        return remote(s.outl.at[piece(n)], s.cl.at[piece(n)], m.dn_s.at[n], m.dn_r.at[n], {"z": down})

    def scan_step(t):
        n = t - LAG * z

        @when(jnp.logical_and(n >= 0, n < PIECES))
        def _():
            @unless(first)
            def _():
                going_up(n).wait_recv()

            @unless(last)
            def _():
                at = piece(n)
                s.outr[at] = (s.cr[at].astype(f32) * s.decay[0:1, at[2]] + s.sr[at]).astype(bf16)
                going_up(n).start()

        i = t - LAG * (NZ - 1 - z)

        @when(jnp.logical_and(i >= 0, i < PIECES))
        def _():
            @unless(last)
            def _():
                going_down(i).wait_recv()

            @unless(first)
            def _():
                at = piece(i)
                s.outl[at] = (s.cl[at].astype(f32) * s.decay[0:1, at[2]] + s.sl[at]).astype(bf16)
                going_down(i).start()

    def within(k, j):
        at = pl.ds(pl.multiple_of(k * BLOCK, BLOCK), BLOCK)
        lanes = columns(j, 128)
        parts = jnp.concatenate(parts_of(s.level[k], 3), axis=0).astype(bf16)
        level_cols = dot_tn(parts, s.wide[:, columns(j, 256)])
        vj, dyj = s.v16[at, lanes], s.dyh[k, :, lanes]
        signed, grid_t = s.signed[k], s.grid_t[k]
        halves = []
        weights = s.weights[k]
        dl = s.dl[k]
        for i in range(2):
            h = 2 * j + i
            near = jnp.exp(-jnp.abs(level_cols[:, 128 * i : 128 * (i + 1)] - s.level[k, pl.ds(h, 1), :]))
            keep_half = low_half if i == 0 else jnp.logical_not(low_half)
            shared = dot_nt(jnp.where(keep_half, dyj, jnp.zeros_like(dyj)), vj) * near
            weights = weights + shared
            crossing = (shared * signed).astype(bf16)
            pick = (head_row == h).astype(bf16)
            dl = dl + dot(pick, crossing) - dot_nt(pick, crossing)
            halves.append(dot((grid_t * near).astype(bf16), dyj))
        s.weights[k] = weights
        s.dl[k] = dl
        s.dv[at, lanes] = jnp.where(low_half, halves[0], halves[1])

    s.weights[...] = jnp.zeros_like(s.weights)
    s.dl[...] = jnp.zeros_like(s.dl)
    for k in range(NX):
        at = pl.ds(k * BLOCK, BLOCK)
        b, cc = s.b16[at], s.c16[at]
        s.signed[k] = dot_nt(cc, b) * sign
        s.grid_t[k] = dot_nt(b, cc)

    far = z // (NZ // 2)
    near_end = z * (1 - far) + (NZ - 1 - z) * far
    early = EARLY * near_end
    between = LAG * near_end + PIECES
    until = LAG * (NZ - 1 - near_end)

    def unit(n):
        within(n // (LH // 2), lax.rem(n, LH // 2))

    def steps(t, carry):
        scan_step(t)

        @when(jnp.logical_and(t < early, t < UNITS))
        def _():
            unit(t)

        @when(jnp.logical_and(t >= between, t < until))
        def _():
            def two(i, inner):
                n = early + 2 * (t - between) + i

                @when(n < UNITS)
                def _():
                    unit(n)

                return inner

            lax.fori_loop(0, 2, two, 0)

        return carry

    lax.fori_loop(0, PIECES + LAG * (NZ - 1), steps, 0)

    def rest(n, carry):
        done = jnp.where(until > between, early + 2 * (until - between), early)

        @when(n >= done)
        def _():
            unit(n)

        return carry

    lax.fori_loop(0, UNITS, rest, 0)

    s.right[0, 0], s.right[0, 1] = s.cr[0].astype(f32), s.cr[1].astype(f32)
    s.left[NX - 1, 0], s.left[NX - 1, 1] = s.cl[0].astype(f32), s.cl[1].astype(f32)
    for k in range(NX):
        g = s.gamma[k, 0:1]
        s.right[k + 1, 0] = s.right[k + 1, 0] + s.right[k, 0] * g
        s.right[k + 1, 1] = s.right[k + 1, 1] + s.right[k, 1] * g
    for k in range(NX - 2, -1, -1):
        g = s.gamma[k + 1, 0:1]
        s.left[k, 0] = s.left[k, 0] + g * s.left[k + 1, 0]
        s.left[k, 1] = s.left[k, 1] + g * s.left[k + 1, 1]

    def map_gradients(k, carry):
        at = pl.ds(pl.multiple_of(k * BLOCK, BLOCK), BLOCK)
        padded = pl.ds(pl.multiple_of(2 * EDGE + k * BLOCK, EDGE), BLOCK)
        weights = s.weights[k].astype(bf16)
        dc = dot(weights, s.b16[at])
        db = dot_tn(weights, s.c16[at])
        dc = dc + dot_nt(s.pdy16[at], s.right[k, 0].astype(bf16)) + dot_nt(s.qdy16[at], s.left[k, 0].astype(bf16))
        db = db + dot_nt(s.qv16[at], s.left[k, 1].astype(bf16)) + dot_nt(s.pv16[at], s.right[k, 1].astype(bf16))
        s.dbcpad[padded, 0:STATE] = db * s.bs[at]
        s.dbcpad[padded, STATE : 2 * STATE] = dc * s.cs[at]
        return carry

    lax.fori_loop(0, NX, map_gradients, 0)

    def input_gradients(k, carry):
        at = pl.ds(pl.multiple_of(k * BLOCK, BLOCK), BLOCK)
        padded = pl.ds(pl.multiple_of(2 * EDGE + k * BLOCK, EDGE), BLOCK)
        b, cc = s.b16[at], s.c16[at]
        dl = s.dl[k]
        dvu = jnp.zeros((8, BLOCK), f32)
        for j in range(LH // 2):
            lanes = slice(128 * j, 128 * (j + 1))
            kvr, cdr = s.right[k, 0, :, lanes].astype(bf16), s.right[k, 1, :, lanes].astype(bf16)
            kvl, cdl = s.left[k, 0, :, lanes].astype(bf16), s.left[k, 1, :, lanes].astype(bf16)
            pe = s.spread[at, LW + 128 * j : LW + 128 * (j + 1)]
            qe = s.spread[at, 2 * LW + 128 * j : 2 * LW + 128 * (j + 1)]
            from_later, from_earlier = dot(b, cdl), dot(b, cdr)
            pv, qv, pdy, qdy = s.pv16[at, lanes], s.qv16[at, lanes], s.pdy16[at, lanes], s.qdy16[at, lanes]
            dv = s.dv[at, lanes] + qe * from_later + pe * from_earlier
            cross = (
                qv.astype(f32) * from_later - pv.astype(f32) * from_earlier
                + qdy.astype(f32) * dot(cc, kvl) - pdy.astype(f32) * dot(cc, kvr)
            )
            picks = jnp.concatenate([s.gather[:, lanes]] * 2, axis=1)
            dl = dl + dot_nt(picks, jnp.concatenate(parts_of(cross, 2), axis=1).astype(bf16))
            dvu = dvu + dot_nt(picks, jnp.concatenate(parts_of(dv * s.u[at, lanes], 2), axis=1).astype(bf16))
            du = dv * s.spread[at, lanes] + pair_row(s.prm, 11, j) * s.dyh[k, :, lanes].astype(f32)
            s.dxpad[padded, lanes] = du * s.slope[at, lanes]
        s.dl[k], s.dvu[k] = dl, dvu
        return carry

    def masked_edges(pad, width, tap_for, before_ref, behind_ref):
        for w in range(width // 128):
            lanes = slice(128 * w, 128 * (w + 1))
            before = unconvolved(pad, -EDGE, EDGE, lanes, tap_for(w))
            behind = unconvolved(pad, CHUNK, EDGE, lanes, tap_for(w))
            before_ref[:, lanes] = jnp.where(first, 0.0, before).astype(bf16)
            behind_ref[:, lanes] = jnp.where(last, 0.0, behind).astype(bf16)

    def map_tap(w):
        return lambda tap: s.taps[tap : tap + 1, 128 * w : 128 * (w + 1)]

    def input_tap(j):
        return lambda tap: pair_row(s.prm, 4 + tap, j)

    def bco_to(d):
        peer = lax.rem(x + d, NX)
        return remote(s.dbc.at[peer], s.bco.at[x], m.ob_s.at[d - 1], m.ob_r.at[d - 1], {"x": peer})

    def dto_to(d):
        peer = lax.rem(x + d, NX)
        return remote(s.ddt.at[peer], s.dto.at[x], m.ot_s.at[d - 1], m.ot_r.at[d - 1], {"x": peer})

    def dxo_to(d):
        peer = lax.rem(x + d, NX)
        return remote(
            s.dx.at[peer], s.dxo_out.at[:, columns(x, LW)], m.ox_s.at[d - 1], m.ox_r.at[d - 1], {"x": peer}
        )

    def edges_out(n):
        before, behind = {"z": down, "x": jnp.int32(NX - 1)}, {"z": up, "x": jnp.int32(0)}
        return (
            remote(s.dbp, s.ebn.at[n], m.e_s.at[0], m.e_r.at[0, n], before),
            remote(s.dbn, s.ebp.at[n], m.e_s.at[1], m.e_r.at[1, n], behind),
            remote(s.dxp, s.exn.at[:, columns(n, LW)], m.e_s.at[2], m.e_r.at[2, n], before),
            remote(s.dxn, s.exp.at[:, columns(n, LW)], m.e_s.at[3], m.e_r.at[3, n], behind),
        )

    masked_edges(s.dbcpad, 2 * STATE, map_tap, s.dbp, s.dbn)
    for copy in edges_out(x)[:2]:
        copy.start()
    for k in range(NX):
        for w in range(2):
            lanes = slice(STATE * w, STATE * (w + 1))
            s.dbc[k, :, lanes] = unconvolved(s.dbcpad, k * BLOCK, BLOCK, lanes, map_tap(w)).astype(bf16)
    for d in (2, 1, 3):
        bco_to(d).start()
    own_bco = pltpu.make_async_copy(s.dbc.at[x], s.bco.at[x], m.own.at[6])
    own_bco.start()

    lax.fori_loop(0, NX, input_gradients, 0)
    masked_edges(s.dxpad, LW, input_tap, s.dxp, s.dxn)
    for copy in edges_out(x)[2:]:
        copy.start()
    for k in range(NX):
        for j in range(LH // 2):
            lanes = slice(128 * j, 128 * (j + 1))
            s.dx[k, :, lanes] = unconvolved(s.dxpad, k * BLOCK, BLOCK, lanes, input_tap(j)).astype(bf16)
    for d in (2, 1, 3):
        dxo_to(d).start()
    own_dx = pltpu.make_async_copy(s.dx.at[x], s.dxo_out.at[:, columns(x, LW)], m.own.at[7])
    own_dx.start()

    own_bco.wait()
    for d in range(1, NX):
        bco_to(d).wait_recv()

    @when(x_last)
    def _():
        for n in range(NX):
            edges_out(n)[0].wait_recv()

    @when(x_first)
    def _():
        for n in range(NX):
            edges_out(n)[1].wait_recv()

    for g in range(GROUPS):
        lanes = slice(2 * STATE * g, 2 * STATE * (g + 1))
        both = s.bco[2 * g].astype(f32) + s.bco[2 * g + 1].astype(f32)
        edge = s.ebp[2 * g].astype(f32) + s.ebp[2 * g + 1].astype(f32)
        s.dmaps[0:EDGE, lanes] = (both[0:EDGE] + edge).astype(bf16)
        s.dmaps[EDGE : BLOCK - EDGE, lanes] = both[EDGE : BLOCK - EDGE].astype(bf16)
        edge = s.ebn[2 * g].astype(f32) + s.ebn[2 * g + 1].astype(f32)
        s.dmaps[BLOCK - EDGE :, lanes] = (both[BLOCK - EDGE :] + edge).astype(bf16)

    order = [4, 3, 5, 2, 6, 1, 7, 0]

    def weight_part(n, core):
        block = lax.rem(y + order[n], NY) * NC + core
        return dot_tn(a.act[:, columns(block, BLOCK)], s.dmaps[...])

    def swap(n):
        return remote(s.part.at[n], s.pair.at[n], m.sw_s.at[n], m.sw_r.at[n], {"c": other})

    for n in range(NY):
        s.part[n] = weight_part(n, other).astype(bf16)
        swap(n).start()
    s.kept[0] = weight_part(0, c)

    def reduced(step, h, way):
        send, recv, to = (m.rr_s, m.rr_r, north) if way > 0 else (m.rl_s, m.rl_r, south)
        out, into = (s.outwr, s.inr) if way > 0 else (s.outwl, s.inl)
        return remote(out.at[step, rows(h)], into.at[step, rows(h)], send.at[step, h], recv.at[step, h], {"y": to})

    def both_cores(n, h):
        return s.kept[n, rows(h)] + s.pair[n, rows(h)].astype(f32)

    def hidden_part(n):
        s_block = n
        s.dhid_out[:, 128 * n : 128 * (n + 1)] = dot_nt(s.dmaps[...], s.wf[s_block]).astype(bf16)

    for step in range(4):
        for n in ((0,), (1, 2), (3, 4), (5, 6))[step]:
            swap(n).wait_recv()
        for h in range(CUTS):
            for way in (1, -1):
                if step == 0 and not near_side(h, way):
                    continue
                n = order.index((way * (4 - step)) % NY)
                value = both_cores(n, h)
                if step > 1 or (step == 1 and near_side(h, way)):
                    reduced(step - 1, h, way).wait_recv()
                    value = value + (s.inr if way > 0 else s.inl)[step - 1, rows(h)].astype(f32)
                (s.outwr if way > 0 else s.outwl)[step, rows(h)] = value.astype(bf16)
                reduced(step, h, way).start()
        for n in ((1, 2), (3, 4), (5, 6), (7,))[step]:
            s.kept[n] = weight_part(n, c)
        for n in range(4 * step, 4 * step + 4):
            hidden_part(n)
    swap(7).wait_recv()
    for h in range(CUTS):
        value = both_cores(7, h)
        for way in (1, -1):
            reduced(3, h, way).wait_recv()
            value = value + (s.inr if way > 0 else s.inl)[3, rows(h)].astype(f32)
        s.quarter[rows(h)] = value
        s.quarter16[rows(h)] = value.astype(bf16)

    strip = BLOCK // NX

    def strip_to(d):
        peer = lax.rem(x + d, NX)
        return remote(
            s.quarter16.at[columns(peer, strip)], s.xin.at[d - 1], m.qx_s.at[d - 1], m.qx_r.at[d - 1], {"x": peer}
        )

    for d in (2, 1, 3):
        strip_to(d).start()

    stores[1].start()

    own_dx.wait()
    for d in range(1, NX):
        dxo_to(d).wait_recv()

    @when(x_last)
    def _():
        for n in range(NX):
            edges_out(n)[2].wait_recv()
        at = slice(BLOCK - EDGE, BLOCK)
        s.dxo_out[at, :] = (s.dxo_out[at, :].astype(f32) + s.exn[...].astype(f32)).astype(bf16)

    @when(x_first)
    def _():
        for n in range(NX):
            edges_out(n)[3].wait_recv()
        s.dxo_out[0:EDGE, :] = (s.dxo_out[0:EDGE, :].astype(f32) + s.exp[...].astype(f32)).astype(bf16)

    stores[2].start()
    strips = s.quarter[columns(x, strip)]
    for d in range(1, NX):
        strip_to(d).wait_recv()
        strips = strips + s.xin[d - 1].astype(f32)
    for i in range(NZ):
        part = strips[16 * (i // 4) : 16 * (i // 4) + 16, 128 * (i % 4) : 128 * (i % 4) + 128]
        s.piece[i], s.piece16[i] = part, part.astype(bf16)

    def piece_to(d):
        peer = lax.rem(z + d, NZ)
        return remote(s.piece16.at[peer], s.zin.at[d - 1], m.qz_s.at[d - 1], m.qz_r.at[d - 1], {"z": peer})

    for d in (4, 3, 5, 2, 6, 1, 7):
        piece_to(d).start()

    met = s.right[NX, 0] * s.left[NX - 1, 1] + s.right[NX, 1] * s.left[NX - 1, 0]
    picks = jnp.concatenate([s.gather[...]] * 2, axis=1)
    crossing_end = dot_nt(picks, jnp.concatenate(parts_of(met, 2), axis=1).astype(bf16))
    after = -jnp.sum(crossing_end, axis=1, keepdims=True)
    for k in range(NX - 1, -1, -1):
        d_rate = jnp.dot(s.dl[k], lower, precision=highest, preferred_element_type=f32) + after
        after = d_rate[:, 0:1]
        d_dt = d_rate * jnp.exp(s.prm[:, 10, :]) + s.dvu[k]
        s.ddt[k] = d_dt / (1.0 + jnp.exp(-(s.dth[k] + s.prm[:, 9, :])))
    for d in range(1, NX):
        dto_to(d).start()
    own_ddt = pltpu.make_async_copy(s.ddt.at[x], s.dto.at[x], m.own.at[8])
    own_ddt.start()

    value = s.piece[z]
    for d in range(1, NZ):
        piece_to(d).wait_recv()
        value = value + s.zin[d - 1].astype(f32)
    s.held[z] = value.astype(bf16)

    def piece_back(d):
        return remote(s.held.at[z], s.held.at[z], m.gz_s.at[d - 1], m.gz_r.at[d - 1], {"z": lax.rem(z + d, NZ)})

    def piece_from(d):
        source = lax.rem(z - d + NZ, NZ)
        return remote(s.held.at[z], s.held.at[source], m.gz_s.at[d - 1], m.gz_r.at[d - 1], {"z": source})

    for d in (4, 3, 5, 2, 6, 1, 7):
        piece_back(d).start()
    own_ddt.wait()
    for d in range(1, NX):
        dto_to(d).wait_recv()
    for n in range(NX // 2):
        o.dts[16 * n : 16 * n + 16] = jnp.concatenate([s.dto[2 * n], s.dto[2 * n + 1]], axis=0).astype(bf16)
    for d in range(1, NZ):
        piece_from(d).wait_recv()
    own_strip = columns(x, strip)
    for i in range(NZ):
        at = pl.ds(pl.multiple_of(x * strip + 16 * (i // 4), 16), 16)
        s.summed[at, 128 * (i % 4) : 128 * (i % 4) + 128] = s.held[i]

    def strip_back(d):
        at = s.summed.at[own_strip]
        return remote(at, at, m.gx_s.at[d - 1], m.gx_r.at[d - 1], {"x": lax.rem(x + d, NX)})

    def strip_from(d):
        source = lax.rem(x - d + NX, NX)
        at = s.summed.at[columns(source, strip)]
        return remote(at, at, m.gx_s.at[d - 1], m.gx_r.at[d - 1], {"x": source})

    for d in (2, 1, 3):
        strip_back(d).start()

    for step, h, way in w_steps:
        w_ring(step, h, way).wait_send()
    for h in range(CUTS):
        for n in range(8):
            w_across(n, h).wait_send()
    for which in range(4):
        for n in range(NX):

            @when((x_last, x_first)[which % 2])
            def _():
                edge_in(which, n).wait_send()

    for d in range(1, NX):
        for copy in (x_to(d), dt_to(d), dy_to(d), bc_to(d), bco_to(d), dto_to(d), dxo_to(d), strip_to(d)):
            copy.wait_send()
    for i in range(NZ):

        @unless(jnp.logical_and(mine, z == i))
        def _():
            message(i).wait_send()

    for copy in edges_out(x):
        copy.wait_send()

    def sent(n, carry):
        @unless(last)
        def _():
            going_up(n).wait_send()

        @unless(first)
        def _():
            going_down(n).wait_send()

        return carry

    lax.fori_loop(0, PIECES, sent, 0)
    for n in range(NY):
        swap(n).wait_send()
    for step in range(4):
        for h in range(CUTS):
            for way in (1, -1):
                if step > 0 or near_side(h, way):
                    reduced(step, h, way).wait_send()
    for d in range(1, NZ):
        piece_to(d).wait_send()
        piece_back(d).wait_send()
    for copy in stores:
        copy.wait()
    for d in range(1, NX):
        strip_from(d).wait_recv()
    for n, out in enumerate((o.dwb, o.dwc)):
        for g in range(GROUPS):
            lane = STATE * (2 * g + n)
            out[:, STATE * g : STATE * (g + 1)] = s.summed[:, lane : lane + STATE].astype(f32)
    for d in range(1, NX):
        strip_back(d).wait_send()


def whole(*args):
    shapes = (
        jax.ShapeDtypeStruct((BLOCK, INNER), bf16),
        jax.ShapeDtypeStruct((BLOCK, INNER), bf16),
        jax.ShapeDtypeStruct((BLOCK, INNER), bf16),
        jax.ShapeDtypeStruct((HEADS, BLOCK), bf16),
        jax.ShapeDtypeStruct((BLOCK, GROUPS * STATE), f32),
        jax.ShapeDtypeStruct((BLOCK, GROUPS * STATE), f32),
    )
    scratch = [pltpu.VMEM(shape, dtype) for shape, dtype in BUFFERS.values()]
    scratch += [DMA(shape) for shape in SEMAPHORES.values()]
    scalar = pl.BlockSpec(memory_space=pltpu.SMEM)
    anywhere = pl.BlockSpec(memory_space=pl.ANY)
    return pl.pallas_call(
        kernel,
        out_shape=shapes,
        in_specs=[anywhere if name in STREAMED else vmem() for name in INPUTS[:-3]] + [scalar] * 3,
        out_specs=(anywhere,) * 3 + (vmem(),) * 3,
        scratch_shapes=scratch,
        compiler_params=pltpu.CompilerParams(
            collective_id=0, has_side_effects=True, vmem_limit_bytes=VMEM_LIMIT
        ),
        name="mixer_backward",
    )(*args)


def deliver_kernel(*refs):
    half = len(refs) // 2
    for given, out in zip(refs[:half], refs[half:], strict=True):
        out[...] = given[...]


def delivered(arrays):
    return pl.pallas_call(
        deliver_kernel,
        out_shape=tuple(jax.ShapeDtypeStruct(v.shape, v.dtype) for v in arrays),
        in_specs=[vmem()] * len(arrays),
        out_specs=tuple(vmem() for _ in arrays),
        name="deliver",
    )(*arrays)


def local(
    layer_activity, writer_matrix, reader_matrix, source_unfiltered, switch_raw_signal, saved_result,
    final_adjoint, delta_raw, extra_logdrop, source_filter_coefs, writer_filter_coefs, reader_filter_coefs,
    delta_offset, fading_exponents, direct_factor, rescale_factor,
):
    tokens = layer_activity.shape[1]
    outputs = whole(
        writer_matrix,
        reader_matrix,
        layer_activity.reshape(tokens, -1),
        source_unfiltered.reshape(tokens, INNER),
        switch_raw_signal.reshape(tokens, INNER),
        saved_result.reshape(tokens, INNER),
        final_adjoint.reshape(tokens, INNER),
        rescale_factor.reshape(1, INNER),
        delta_raw.reshape(tokens, HEADS).T,
        extra_logdrop.reshape(NZ, NX, BLOCK),
        source_filter_coefs,
        writer_filter_coefs,
        reader_filter_coefs,
        delta_offset,
        fading_exponents,
        direct_factor,
    )
    d_gate, d_x, d_hidden, d_dt, d_w_b, d_w_c = delivered(outputs)
    return (
        d_hidden.reshape(1, tokens, -1),
        d_x.reshape(1, tokens, INNER),
        d_gate.reshape(1, tokens, INNER),
        d_dt.T.reshape(1, tokens, HEADS),
        d_w_b,
        d_w_c,
    )


def solution(mesh):
    split = Mesh(mesh.devices.reshape(NZ, NX, NY, NC), ("z", "x", "y", "c"))
    sp, dp = ("z", "x"), ("y", "c")
    in_specs = (
        P(dp, sp, None),
        P(dp, None),
        P(dp, None),
        P(dp, sp, None),
        P(dp, sp, None),
        P(dp, sp, None),
        P(dp, sp, None),
        P(dp, sp, None),
        P(dp, None, sp),
        P(None, sp),
        P(),
        P(),
        P(sp),
        P(sp),
        P(sp),
        P(),
    )
    out_specs = (
        P(dp, sp, None),
        P(dp, sp, None),
        P(dp, sp, None),
        P(dp, sp, None),
        P(dp, None),
        P(dp, None),
    )
    return jax.shard_map(local, mesh=split, in_specs=in_specs, out_specs=out_specs, check_vma=False)
```
